32 devices in a mesh: rep: 2 (over x), fs: 8 (over z, y), tp: 2 (over core).
Axes of the slice: x: 2, y: 2, z: 4, core: 2. Of those that a mesh axis runs over, the one named last changes fastest.
Arguments:
- inputs: bfloat16 [6144, 2048], P(('rep', 'fs')), may hold values from -6 to 6
- w_up: bfloat16 [2048, 4096], P('fs', 'tp'), may hold values from -0.125 to 0.125
- w_down: bfloat16 [4096, 2048], P('tp', 'fs'), may hold values from -0.09375 to 0.09375
- cotangent: bfloat16 [6144, 2048], P(('rep', 'fs')), may hold values from -6 to 6
Outputs:
- d_inputs: bfloat16 [6144, 2048], P(('rep', 'fs'))
- d_w_up: float32 [2048, 4096], P('fs', 'tp')
The draws below stay inside these ranges and needn't reach their ends.
All inputs are finite; a program needn't handle non-finite values.
Results may differ from the reference program's by a relative error of at most 0.014.
Values may be sent and summed in bfloat16 or wider, within the bound.
A program may use at most 128 MiB of HBM per device.

```python
import jax
import jax.numpy as jnp

D = 2048
FF = 4096
TOKENS = 6144
N_TP = 2


def strengthened(result, own_key, source, target, shards_of, factor):
    def block_of(axis_at):
        return (jnp.arange(result.shape[axis_at]) // (result.shape[axis_at] // shards_of)).reshape((-1,) + (1,) * (result.ndim - 1 - axis_at))

    near = jax.random.permutation(own_key, shards_of)[block_of(target)]
    other_side = (block_of(target) + shards_of // 2) % shards_of
    return jnp.where((block_of(source) == near) | (block_of(source) == other_side), factor * result, result)


def block_levels(key, extent, pieces, low, top_value):
    def one(dim, blocks):
        draws = jax.random.uniform(jax.random.fold_in(jax.random.fold_in(key, 6), dim), (blocks,), jnp.float32, low / len(pieces), top_value / len(pieces))
        return jnp.repeat(jnp.exp(draws), extent[dim] // blocks).reshape((-1,) + (1,) * (len(extent) - dim - 1))

    loudness = one(*pieces[0])
    for cut in pieces[1:]:
        loudness = loudness * one(*cut)
    return loudness


def normal_values(stream_key, extent, spread, most, split=(), kind=jnp.bfloat16):
    result = jax.random.normal(stream_key, extent, jnp.float32) * spread
    if len(split) > 0:
        result = block_levels(stream_key, extent, split, -0.22, 0.18) * result
    return jnp.clip(result, min=-most, max=most).astype(kind)


def gaussian_with(own_key, shape, deviation, reach, pieces, heavy, kind=jnp.bfloat16):
    drawn = deviation * jax.random.normal(own_key, shape, jnp.float32)
    if pieces:
        drawn = drawn * block_levels(own_key, shape, pieces, -0.22, 0.18)
    return jnp.clip(strengthened(drawn, jax.random.fold_in(own_key, 3), *heavy), -reach, reach).astype(kind)


def setup_inputs(seed: int = 0) -> dict:
    key_of = jax.random.split(jax.random.key(seed), 5)
    inputs = gaussian_with(key_of[0], (TOKENS, D), 1.0, 6.0, ((0, 16),), (0, 1, 16, 2.0))
    w_up = normal_values(key_of[1], (D, FF), D ** -0.5, 0.125, ((0, 8), (1, 2)))
    w_down = normal_values(key_of[2], (FF, D), FF ** -0.5, 0.09375, ((0, 2), (1, 8)))
    cotangent = gaussian_with(key_of[3], (TOKENS, D), 1.0, 6.0, ((0, 16),), (0, 1, 16, 2.0))
    return {"inputs": inputs, "w_up": w_up, "w_down": w_down, "cotangent": cotangent}


def reference(inputs, w_up, w_down, cotangent):
    preact = jnp.dot(inputs, w_up, preferred_element_type=jnp.float32)
    grad_hidden = jnp.dot(cotangent, w_down.T, preferred_element_type=jnp.float32)
    grad_pre = (2.0 * jnp.maximum(preact, 0.0) * grad_hidden).astype(jnp.bfloat16)
    tp_cols = FF // N_TP
    accumulated = jnp.zeros(inputs.shape, jnp.float32)
    for shard_index in range(N_TP):
        lower = shard_index * tp_cols
        partial_sum = jnp.dot(grad_pre[:, lower:lower + tp_cols], w_up[:, lower:lower + tp_cols].T,
                              preferred_element_type=jnp.float32).astype(jnp.bfloat16)
        accumulated = accumulated + partial_sum.astype(jnp.float32)
    d_inputs = accumulated.astype(jnp.bfloat16)
    d_w_up = jnp.dot(inputs.T, grad_pre, preferred_element_type=jnp.float32)
    return d_inputs, d_w_up
```

```python
import functools

import jax
import jax.numpy as jnp
from jax import lax
from jax.experimental import pallas as pl
from jax.experimental.pallas import tpu as pltpu
from jax.sharding import PartitionSpec as P

MESH = pl.DeviceIdType.MESH
F32, BF16 = jnp.float32, jnp.bfloat16
CHUNKS = 2


def dot(a, b, da, db):
    return lax.dot_general(a, b, (((da,), (db,)), ((), ())), preferred_element_type=F32)


def kernel(line, n_tp, native, x_in, c_in, up_in, down_in, dw_out, din_out,
           xs, wu, wd, acc, g, dw, zin, fin, part_, tpin, q1, q2, fo,
           zs, zr, ys, yr, ts, tr, cs, cr, ls, os, orr, es, er, el, ps, pr, qs, qr, ds, dr, dl):
    r, f, c = lax.axis_index("rep"), lax.axis_index("fs"), lax.axis_index("tp")
    p, at = lax.rem(f, 2), lax.div(f, 2)
    core = lax.rem(c, 2)
    to_x, to_y = {"rep": 1 - r}, {"fs": f + 1 - 2 * p}
    to_core = {"tp": c + 1 - 2 * core}
    up, down = {"fs": f + 2}, {"fs": f - 2}
    has_up, has_down = at < line - 1, at > 0
    tokens, width = x_in.shape
    rows, cols = wu.shape[2:]
    level = 2 * rows
    quarter = 2 * r + p

    barrier = pltpu.get_barrier_semaphore()
    peers = [{"tp": lax.rem(c + k, n_tp)} for k in range(1, n_tp)]
    for dev in [to_x, to_y] + peers:
        pl.semaphore_signal(barrier, inc=1, device_id=dev, device_id_type=MESH)

    @pl.when(has_up)
    def _():
        pl.semaphore_signal(barrier, inc=1, device_id=up, device_id_type=MESH)

    @pl.when(has_down)
    def _():
        pl.semaphore_signal(barrier, inc=1, device_id=down, device_id_type=MESH)

    def remote(src, dst, send, recv, dev):
        return pltpu.make_async_remote_copy(
            src_ref=src, dst_ref=dst, send_sem=send, recv_sem=recv, device_id=dev, device_id_type=MESH
        )

    half = tokens // 2
    mine = pl.ds(pl.multiple_of(core * half, half), half)
    theirs = pl.ds(pl.multiple_of((1 - core) * half, half), half)
    ws = (wu, wd)

    def own_block(u, q):
        span = pl.ds(pl.multiple_of(q * cols, cols), cols)
        if u == 1 and native:
            return down_in.at[span, :]
        return (up_in, down_in)[u].at[:, span]

    own_x = pltpu.make_async_copy(x_in, xs.at[0, 0], ls.at[0])
    own_c = pltpu.make_async_copy(c_in, xs.at[1, 0], ls.at[1])
    own_w = [pltpu.make_async_copy(own_block(u, quarter), ws[u].at[at, p], ls.at[2 + u]) for u in (0, 1)]
    own_x.start()
    own_c.start()
    for copy in own_w:
        copy.start()
    acc[...] = jnp.zeros_like(acc)

    n_near = n_tp + 1
    inner = has_up & has_down

    @pl.when(inner)
    def _():
        pl.semaphore_wait(barrier, n_near + 2)

    @pl.when(jnp.logical_not(inner))
    def _():
        pl.semaphore_wait(barrier, n_near + 1 if line > 1 else n_near)

    y_copies = [
        remote(own_block(u, 2 * r + 1 - p), ws[u].at[at, p], ys.at[u], yr.at[u], to_y) for u in (0, 1)
    ]

    def y_arrival(u):
        blk = ws[u].at[at, 1 - p]
        return remote(blk, blk, ys.at[u], yr.at[u], to_y)

    for copy in y_copies:
        copy.start()

    def z_copy(go_up, s, j):
        u, own_pair = j % 2, j < 2
        lvl = at - s if go_up else at + s
        blk = ws[u].at[lvl, p if own_pair else 1 - p]
        src = own_block(u, quarter) if (s == 0 and own_pair) else blk
        d = 0 if go_up else 1
        return remote(src, blk, zs.at[d, s, j], zr.at[d, s, j], up if go_up else down)

    def z_valid(go_up, s):
        return ((at - s >= 0) & has_up) if go_up else ((at + s < line) & has_down)

    def z_step(s, j):
        for go_up in (True, False):
            d = 0 if go_up else 1
            if s > 0:
                lvl = at - s if go_up else at + s

                @pl.when((lvl >= 0) & (lvl < line))
                def _():
                    blk = ws[j % 2].at[lvl, p if j < 2 else 1 - p]
                    remote(blk, blk, zs.at[d, s - 1, j], zr.at[d, s - 1, j], to_x).wait_recv()
            if s < line - 1:
                @pl.when(z_valid(go_up, s))
                def _():
                    z_copy(go_up, s, j).start()

    z_step(0, 0)
    z_step(0, 1)

    own = (x_in, c_in)
    first = {}
    for slot, dev in ((1, to_x), (2, to_y)):
        for a in (0, 1):
            first[slot, a] = remote(
                own[a].at[mine], xs.at[a, slot, mine], ts.at[slot - 1, a], tr.at[slot - 1, a], dev
            )
    first[1, 0].start()
    first[2, 1].start()
    first[1, 1].start()
    first[2, 0].start()
    diag = [
        remote(xs.at[0, 1, mine], xs.at[0, 3, mine], ts.at[2, 0], tr.at[2, 0], to_y),
        remote(xs.at[1, 2, mine], xs.at[1, 3, mine], ts.at[2, 1], tr.at[2, 1], to_x),
    ]

    def swap(slot, a):
        return remote(
            xs.at[a, slot, mine], xs.at[a, slot, mine], cs.at[slot - 1, a], cr.at[slot - 1, a], to_core
        )

    def swapped(slot, a):
        blk = xs.at[a, slot, theirs]
        remote(blk, blk, cs.at[slot - 1, a], cr.at[slot - 1, a], to_core).wait_recv()

    def unit(u, slot, lvl):
        if u == 1 and native:
            total = acc[u, slot]
            for b in (0, 1):
                span = pl.ds(pl.multiple_of(lvl * level + b * rows, rows), rows)
                total = total + dot(xs[u, slot, :, span], wd[lvl, b], 1, 1)
            acc[u, slot] = total
        else:
            span = pl.ds(pl.multiple_of(lvl * level, level), level)
            acc[u, slot] += dot(xs[u, slot, :, span], ws[u][lvl].reshape(level, cols), 1, 0)

    done = [-1, -1]
    ready = [1, 1]

    def grow(u, s):
        done[u] = s
        n = ready[u]
        if s == 0:
            def body(slot, _):
                unit(u, slot, at)
                return 0

            lax.fori_loop(0, n, body, 0)
            return

        def body(i, _):
            lvl = at + s - 2 * s * lax.rem(i, 2)

            @pl.when((lvl >= 0) & (lvl < line))
            def _():
                unit(u, lax.div(i, 2), lvl)
            return 0

        lax.fori_loop(0, 2 * n, body, 0)

    order = ([0, 1, 2, 3], [0, 2, 1, 3])

    def join(slot, u):
        ready[u] += 1
        lo, hi = jnp.maximum(at - done[u], 0), jnp.minimum(at + done[u], line - 1)

        def body(lvl, _):
            unit(u, slot, lvl)
            return 0

        lax.fori_loop(lo, hi + 1, body, 0)

    own_x.wait()
    own_c.wait()
    for u in (0, 1):
        own_w[u].wait()
    for u in (0, 1):
        y_arrival(u).wait_recv()
        z_step(0, 2 + u)
    for u in (0, 1):
        grow(u, 0)

    def got(slot, a):
        def run():
            if slot < 3:
                first[slot, a].wait_recv()
                if (slot, a) == (1, 0):
                    diag[0].start()
                if (slot, a) == (2, 1):
                    diag[1].start()
            else:
                diag[a].wait_recv()
            swap(slot, a).start()
        return run

    def use(slot, a):
        def run():
            swapped(slot, a)
            join(slot, a)
        return run

    hooks = {
        (1, 2): [got(1, 0)],
        (1, 3): [use(1, 0)],
        (2, 0): [got(2, 1)],
        (2, 1): [got(1, 1), use(2, 1)],
        (2, 2): [use(1, 1)],
        (2, 3): [got(2, 0)],
        (3, 0): [use(2, 0), got(3, 1)],
        (3, 1): [use(3, 1)],
        (3, 2): [got(3, 0)],
    }
    last = [use(3, 0)]
    for s in range(1, line):
        for j in range(4):
            z_step(s, j)
            if j >= 2:
                grow(j - 2, s)
            for run in hooks.pop((s, j), []):
                run()
    for key in sorted(hooks):
        for run in hooks[key]:
            run()
    for run in last:
        run()

    def make_g(slot, _):
        g[slot] = (2.0 * jnp.maximum(acc[0, slot], 0.0) * acc[1, slot]).astype(BF16)
        return 0

    lax.fori_loop(0, 4, make_g, 0)

    low = at < line - at - 1
    sub = rows // CHUNKS

    def chunk(ch):
        return pl.ds(ch * sub, sub)

    def o_copy(go_up, o, ch):
        d = 0 if go_up else 1
        return remote(
            dw.at[o, :, chunk(ch)], zin.at[d, o, :, chunk(ch)],
            os.at[d, o, ch], orr.at[d, o, ch], up if go_up else down,
        )

    def make_dw(i):
        o = jnp.where(low, line - 1 - i, i)
        span = pl.ds(pl.multiple_of(o * level, level), level)
        lhs = xs[0, :, :, span].reshape(4 * tokens, level)
        value = dot(lhs, g[...].reshape(4 * tokens, cols), 0, 0)
        dw[o] = value.astype(BF16).reshape(2, rows, cols)

    def send_ends(i, ch):
        @pl.when((at == 0) & (line > 1))
        def _():
            o_copy(True, line - 1 - i, ch).start()

        @pl.when((at == line - 1) & (line > 1))
        def _():
            o_copy(False, i, ch).start()

    def p_copy(slot, k):
        there = lax.rem(c + k, n_tp)
        return remote(
            part_.at[slot, there], tpin.at[k - 1, slot], ps.at[k - 1, slot], pr.at[k - 1, slot], {"tp": there}
        )

    part = tokens // n_tp

    def make_part(slot):
        def body(lvl, _):
            span = pl.ds(pl.multiple_of(lvl * level, level), level)
            value = dot(g[slot], wu[lvl].reshape(level, cols), 1, 1)
            part_[slot, :, :, span] = value.astype(BF16).reshape(n_tp, part, level)
            return 0

        lax.fori_loop(0, line, body, 0)
        for k in range(1, n_tp):
            p_copy(slot, k).start()

    def tp_sum(slot):
        for k in range(1, n_tp):
            p_copy(slot, k).wait_recv()
        total = part_[slot, c].astype(F32)
        for k in range(1, n_tp):
            total = total + tpin[k - 1, slot].astype(F32)
        return total

    cut = (width * 3 // 8) // 128 * 128
    left, right = pl.ds(0, cut), pl.ds(cut, width - cut)
    q_copies = {
        "x3": remote(part_.at[3, c, :, left], q1.at[1, :, left], qs.at[0], qr.at[0], to_x),
        "y3": remote(part_.at[3, c, :, right], q1.at[1, :, right], qs.at[1], qr.at[1], to_y),
        "x1": remote(part_.at[1, c, :, left], q1.at[0, :, left], qs.at[2], qr.at[2], to_x),
        "y2": remote(part_.at[2, c, :, right], q1.at[0, :, right], qs.at[3], qr.at[3], to_y),
        "y2r": remote(part_.at[2, c, :, left], q2.at[:, left], qs.at[4], qr.at[4], to_y),
        "x1r": remote(part_.at[1, c, :, right], q2.at[:, right], qs.at[5], qr.at[5], to_x),
    }

    def store_sum(slot):
        part_[slot, c] = tp_sum(slot).astype(BF16)

    make_dw(0)
    send_ends(0, 0)
    make_part(3)
    make_part(1)
    make_part(2)
    store_sum(3)
    q_copies["x3"].start()
    q_copies["y3"].start()
    if line > 2:
        make_dw(1)
        send_ends(1, 0)
    store_sum(1)
    q_copies["x1"].start()
    store_sum(2)
    q_copies["y2"].start()
    for i in range(2, line - 1):
        make_dw(i)
        send_ends(i, 0)
    for ch in range(1, CHUNKS):
        for i in range(line - 1):
            send_ends(i, ch)
    if line > 1:
        make_dw(line - 1)
    make_part(0)

    def add_in(d, o, ch):
        dw[o, :, chunk(ch)] = (
            dw[o, :, chunk(ch)].astype(F32) + zin[d, o, :, chunk(ch)].astype(F32)
        ).astype(BF16)

    def o_step(t, ch):
        for go_up in (True, False):
            d = 0 if go_up else 1
            gap = at if go_up else line - 1 - at
            o = (line - 1 - t + at) if go_up else (t - line + 1 + at)

            @pl.when((gap > 0) & (gap <= t))
            def _():
                o_copy(go_up, o, ch).wait_recv()
                if t < line - 1:
                    add_in(d, o, ch)
                    o_copy(go_up, o, ch).start()

    def rows_of(ch):
        return pl.ds(ch * sub, sub)

    e_x = [remote(fin.at[ch, p], dw_out.at[quarter, rows_of(ch)], es.at[0, ch], er.at[0, ch], to_x) for ch in range(CHUNKS)]
    e_y = [remote(fin.at[ch, 1 - p], dw_out.at[quarter, rows_of(ch)], es.at[1, ch], er.at[1, ch], to_y) for ch in range(CHUNKS)]
    e_own = [pltpu.make_async_copy(fin.at[ch, p], dw_out.at[quarter, rows_of(ch)], el.at[ch]) for ch in range(CHUNKS)]
    e_r = []
    for ch in range(CHUNKS):
        blk = dw_out.at[2 * r + 1 - p, rows_of(ch)]
        e_r.append(remote(blk, blk, es.at[2, ch], er.at[2, ch], to_x))

    def finish(ch):
        fin[ch] = dw[at, :, chunk(ch)]

        for d, there in ((0, has_down), (1, has_up)):
            if line > 2:
                @pl.when(there & jnp.logical_not(has_up & has_down))
                def _():
                    fin[ch] = (dw[at, :, chunk(ch)].astype(F32) + zin[d, at, :, chunk(ch)].astype(F32)).astype(BF16)
            elif line == 2:
                @pl.when(there)
                def _():
                    fin[ch] = (dw[at, :, chunk(ch)].astype(F32) + zin[d, at, :, chunk(ch)].astype(F32)).astype(BF16)

        @pl.when(has_up & has_down)
        def _():
            fin[ch] = (
                dw[at, :, chunk(ch)].astype(F32)
                + zin[0, at, :, chunk(ch)].astype(F32)
                + zin[1, at, :, chunk(ch)].astype(F32)
            ).astype(BF16)

        e_x[ch].start()
        e_y[ch].start()
        e_own[ch].start()

    def relay(ch):
        blk = dw_out.at[2 * r + 1 - p, rows_of(ch)]
        remote(blk, blk, es.at[1, ch], er.at[1, ch], to_y).wait_recv()
        e_r[ch].start()

    def in_first():
        q_copies["x3"].wait_recv()
        part_[2, c, :, left] = (part_[2, c, :, left].astype(F32) + q1[1, :, left].astype(F32)).astype(BF16)
        q_copies["y2r"].start()
        q_copies["y3"].wait_recv()
        part_[1, c, :, right] = (part_[1, c, :, right].astype(F32) + q1[1, :, right].astype(F32)).astype(BF16)
        q_copies["x1r"].start()

    out_own = pltpu.make_async_copy(fo, din_out.at[c], dl.at[0])
    out_peers = [
        remote(fo, din_out.at[c], ds.at[k - 1], dr.at[k - 1], {"tp": lax.rem(c + k, n_tp)}) for k in range(1, n_tp)
    ]

    def in_last():
        total = tp_sum(0)
        for name in ("x1", "y2", "y2r", "x1r"):
            q_copies[name].wait_recv()
        fo[...] = (total + q1[0].astype(F32) + q2[...].astype(F32)).astype(BF16)
        out_own.start()
        for copy in out_peers:
            copy.start()

    late = {(0, min(2, line - 1)): [in_first], (CHUNKS - 1, min(2, line - 1)): [in_last]}
    for ch in range(CHUNKS):
        for t in range(1, line):
            o_step(t, ch)
            if t == line - 1:
                finish(ch)
            for run in late.pop((ch, t), []):
                run()
            if ch > 0 and t == 1:
                relay(ch - 1)
        if line == 1:
            finish(ch)
            if ch > 0:
                relay(ch - 1)
    for key in sorted(late):
        for run in late[key]:
            run()
    relay(CHUNKS - 1)

    for k in range(1, n_tp):
        out_peers[k - 1].wait_recv()
    for ch in range(CHUNKS):
        for q, col in ((2 * (1 - r) + p, 0), (2 * (1 - r) + 1 - p, 2)):
            blk = dw_out.at[q, rows_of(ch)]
            remote(blk, blk, es.at[col, ch], er.at[col, ch], to_x).wait_recv()
    out_own.wait()
    for copy in e_own:
        copy.wait()
    for copy in out_peers + e_x + e_y + e_r + list(q_copies.values()):
        copy.wait_send()
    for slot in range(4):
        for k in range(1, n_tp):
            p_copy(slot, k).wait_send()
    for ch in range(CHUNKS):
        for o in range(line):
            @pl.when((at < o) & has_up)
            def _():
                o_copy(True, o, ch).wait_send()

            @pl.when((at > o) & has_down)
            def _():
                o_copy(False, o, ch).wait_send()
    for slot in (1, 2, 3):
        for a in (0, 1):
            swap(slot, a).wait_send()
    for copy in list(first.values()) + diag + y_copies:
        copy.wait_send()
    for s in range(line - 1):
        for j in range(4):
            for go_up in (True, False):
                @pl.when(z_valid(go_up, s))
                def _():
                    z_copy(go_up, s, j).wait_send()


def fused(n_fs, n_tp, n_rep, x, c, w_up, w_down):
    line = n_fs // 2
    tokens, width = x.shape
    rows, block = w_up.shape
    cols = block // (2 * n_rep)
    native = rows % 128 == 0
    if not native:
        w_down = w_down.T
    part = tokens // n_tp
    dma = pltpu.SemaphoreType.DMA
    hbm = pl.BlockSpec(memory_space=pl.ANY)
    vmem = lambda *shape: pltpu.VMEM(shape, BF16)
    down_block = (cols, rows) if native else (rows, cols)
    others = max(n_tp - 1, 1)
    return pl.pallas_call(
        functools.partial(kernel, line, n_tp, native),
        out_shape=(
            jax.ShapeDtypeStruct((2 * n_rep, rows, cols), BF16),
            jax.ShapeDtypeStruct((n_tp, part, width), BF16),
        ),
        in_specs=[hbm] * 4,
        out_specs=(hbm,) * 2,
        scratch_shapes=[
            vmem(2, 4, tokens, width),
            vmem(line, 2, rows, cols),
            vmem(line, 2, *down_block),
            pltpu.VMEM((2, 4, tokens, cols), F32),
            vmem(4, tokens, cols),
            vmem(line, 2, rows, cols),
            vmem(2, line, 2, rows, cols),
            vmem(CHUNKS, 2, rows // CHUNKS, cols),
            vmem(4, n_tp, part, width),
            vmem(others, 4, part, width),
            vmem(2, part, width),
            vmem(part, width),
            vmem(part, width),
            dma((2, line, 4)), dma((2, line, 4)), dma((2,)), dma((2,)),
            dma((3, 2)), dma((3, 2)), dma((3, 2)), dma((3, 2)), dma((4,)),
            dma((2, line, CHUNKS)), dma((2, line, CHUNKS)),
            dma((3, CHUNKS)), dma((3, CHUNKS)), dma((CHUNKS,)),
            dma((others, 4)), dma((others, 4)), dma((6,)), dma((6,)),
            dma((others,)), dma((others,)), dma((1,)),
        ],
        compiler_params=pltpu.CompilerParams(
            collective_id=0, has_side_effects=True, vmem_limit_bytes=60 * 2**20
        ),
        name="fused",
    )(x, c, w_up, w_down)


def per_device(inputs, w_up, w_down, cotangent):
    n_rep, n_fs, n_tp = lax.axis_size("rep"), lax.axis_size("fs"), lax.axis_size("tp")
    rows, block = w_up.shape
    d_w, d_in = fused(n_fs, n_tp, n_rep, inputs, cotangent, w_up, w_down)
    d_w_up = d_w.transpose(1, 0, 2).reshape(rows, block).astype(F32)
    return d_in.reshape(inputs.shape), d_w_up


def solution(mesh):
    in_specs = (P(("rep", "fs"), None), P("fs", "tp"), P("tp", "fs"), P(("rep", "fs"), None))
    out_specs = (P(("rep", "fs"), None), P("fs", "tp"))
    return jax.shard_map(
        per_device, mesh=mesh, in_specs=in_specs, out_specs=out_specs, check_vma=False
    )
```

```python
import functools

import jax
import jax.numpy as jnp
from jax import lax
from jax.experimental import pallas as pl
from jax.experimental.pallas import tpu as pltpu
from jax.sharding import PartitionSpec as P

MESH = pl.DeviceIdType.MESH
F32, BF16 = jnp.float32, jnp.bfloat16


def dot(a, b, da, db):
    return lax.dot_general(a, b, (((da,), (db,)), ((), ())), preferred_element_type=F32)


def kernel(line, n_tp, native, parts, x_in, c_in, up_in, down_in, dw_out, din_out,
           xs, wu, wd, acc, g, dw, zin, fin, part_, tpin, q1, q2, fo,
           zs, zr, ys, yr, ts, tr, cs, cr, ls, os, orr, es, er, el, ps, pr, qs, qr, ds, dr, dl):
    r, f, c = lax.axis_index("rep"), lax.axis_index("fs"), lax.axis_index("tp")
    p, at = lax.rem(f, 2), lax.div(f, 2)
    core = lax.rem(c, 2)
    to_x, to_y = {"rep": 1 - r}, {"fs": f + 1 - 2 * p}
    to_core = {"tp": c + 1 - 2 * core}
    up, down = {"fs": f + 2}, {"fs": f - 2}
    has_up, has_down = at < line - 1, at > 0
    tokens, width = x_in.shape
    rows, cols = wu.shape[3:]
    level = 2 * rows
    final = parts - 1
    quarter = 2 * r + p

    barrier = pltpu.get_barrier_semaphore()
    peers = [{"tp": lax.rem(c + k, n_tp)} for k in range(1, n_tp)]
    for dev in [to_x, to_y] + peers:
        pl.semaphore_signal(barrier, inc=1, device_id=dev, device_id_type=MESH)

    @pl.when(has_up)
    def _():
        pl.semaphore_signal(barrier, inc=1, device_id=up, device_id_type=MESH)

    @pl.when(has_down)
    def _():
        pl.semaphore_signal(barrier, inc=1, device_id=down, device_id_type=MESH)

    def remote(src, dst, send, recv, dev):
        return pltpu.make_async_remote_copy(
            src_ref=src, dst_ref=dst, send_sem=send, recv_sem=recv, device_id=dev, device_id_type=MESH
        )

    half = tokens // 2
    mine = pl.ds(pl.multiple_of(core * half, half), half)
    theirs = pl.ds(pl.multiple_of((1 - core) * half, half), half)
    ws = (wu, wd)

    def own_block(u, q, h):
        span = pl.ds(pl.multiple_of((q * parts + h) * cols, cols), cols)
        if u == 1 and native:
            return down_in.at[span, :]
        return (up_in, down_in)[u].at[:, span]

    own_x = pltpu.make_async_copy(x_in, xs.at[0, 0], ls.at[0])
    own_c = pltpu.make_async_copy(c_in, xs.at[1, 0], ls.at[1])
    own_w = [
        pltpu.make_async_copy(own_block(u, quarter, h), ws[u].at[h, at, p], ls.at[2 + 2 * h + u])
        for h in range(parts) for u in (0, 1)
    ]
    own_x.start()
    own_c.start()
    for copy in own_w:
        copy.start()
    acc[...] = jnp.zeros_like(acc)

    n_near = n_tp + 1
    inner = has_up & has_down

    @pl.when(inner)
    def _():
        pl.semaphore_wait(barrier, n_near + 2)

    @pl.when(jnp.logical_not(inner))
    def _():
        pl.semaphore_wait(barrier, n_near + 1 if line > 1 else n_near)

    y_copies = [
        remote(own_block(u, 2 * r + 1 - p, h), ws[u].at[h, at, p], ys.at[h, u], yr.at[h, u], to_y)
        for h in range(parts) for u in (0, 1)
    ]

    def y_arrival(u, h):
        blk = ws[u].at[h, at, 1 - p]
        return remote(blk, blk, ys.at[h, u], yr.at[h, u], to_y)

    for copy in y_copies:
        copy.start()

    def z_copy(go_up, h, s, j):
        u, own_pair = j % 2, j < 2
        lvl = at - s if go_up else at + s
        blk = ws[u].at[h, lvl, p if own_pair else 1 - p]
        src = own_block(u, quarter, h) if (s == 0 and own_pair) else blk
        d = 0 if go_up else 1
        return remote(src, blk, zs.at[d, h, s, j], zr.at[d, h, s, j], up if go_up else down)

    def z_valid(go_up, s):
        return ((at - s >= 0) & has_up) if go_up else ((at + s < line) & has_down)

    def z_step(h, s, j):
        for go_up in (True, False):
            d = 0 if go_up else 1
            if s > 0:
                lvl = at - s if go_up else at + s

                @pl.when((lvl >= 0) & (lvl < line))
                def _():
                    blk = ws[j % 2].at[h, lvl, p if j < 2 else 1 - p]
                    remote(blk, blk, zs.at[d, h, s - 1, j], zr.at[d, h, s - 1, j], to_x).wait_recv()
            if s < line - 1:
                @pl.when(z_valid(go_up, s))
                def _():
                    z_copy(go_up, h, s, j).start()

    z_step(0, 0, 0)
    z_step(0, 0, 1)

    own = (x_in, c_in)
    first = {}
    for slot, dev in ((1, to_x), (2, to_y)):
        for a in (0, 1):
            first[slot, a] = remote(
                own[a].at[mine], xs.at[a, slot, mine], ts.at[slot - 1, a], tr.at[slot - 1, a], dev
            )
    first[1, 0].start()
    first[2, 1].start()
    first[1, 1].start()
    first[2, 0].start()
    diag = [
        remote(xs.at[0, 1, mine], xs.at[0, 3, mine], ts.at[2, 0], tr.at[2, 0], to_y),
        remote(xs.at[1, 2, mine], xs.at[1, 3, mine], ts.at[2, 1], tr.at[2, 1], to_x),
    ]

    def swap(slot, a):
        return remote(
            xs.at[a, slot, mine], xs.at[a, slot, mine], cs.at[slot - 1, a], cr.at[slot - 1, a], to_core
        )

    def swapped(slot, a):
        blk = xs.at[a, slot, theirs]
        remote(blk, blk, cs.at[slot - 1, a], cr.at[slot - 1, a], to_core).wait_recv()

    def unit(u, h, slot, lvl):
        if u == 1 and native:
            total = acc[h, u, slot]
            for b in (0, 1):
                span = pl.ds(pl.multiple_of(lvl * level + b * rows, rows), rows)
                total = total + dot(xs[u, slot, :, span], wd[h, lvl, b], 1, 1)
            acc[h, u, slot] = total
        else:
            span = pl.ds(pl.multiple_of(lvl * level, level), level)
            acc[h, u, slot] += dot(xs[u, slot, :, span], ws[u][h, lvl].reshape(level, cols), 1, 0)

    done = [[-1, -1] for _ in range(parts)]
    ready = [1, 1]

    def grow_slot(u, h, s, slot):
        for lvl in (at - s, at + s):
            @pl.when((lvl >= 0) & (lvl < line))
            def _():
                unit(u, h, slot, lvl)

    def grow(u, h, s):
        done[h][u] = s
        n = ready[u]
        if s == 0:
            def body(slot, _):
                unit(u, h, slot, at)
                return 0

            lax.fori_loop(0, n, body, 0)
            return

        def body(i, _):
            lvl = at + s - 2 * s * lax.rem(i, 2)

            @pl.when((lvl >= 0) & (lvl < line))
            def _():
                unit(u, h, lax.div(i, 2), lvl)
            return 0

        lax.fori_loop(0, 2 * n, body, 0)

    def join(slot, u):
        ready[u] += 1
        for h in range(parts):
            lo, hi = jnp.maximum(at - done[h][u], 0), jnp.minimum(at + done[h][u], line - 1)

            def body(lvl, _):
                unit(u, h, slot, lvl)
                return 0

            lax.fori_loop(lo, hi + 1, body, 0)

    def make_g(h, slot):
        g[h, slot] = (2.0 * jnp.maximum(acc[h, 0, slot], 0.0) * acc[h, 1, slot]).astype(BF16)

    low = at < line - at - 1

    def o_copy(go_up, h, o):
        d = 0 if go_up else 1
        return remote(dw.at[h, o], zin.at[d, h, o], os.at[d, h, o], orr.at[d, h, o], up if go_up else down)

    def make_dw(h, i):
        o = jnp.where(low, line - 1 - i, i)
        span = pl.ds(pl.multiple_of(o * level, level), level)
        lhs = xs[0, :, :, span].reshape(4 * tokens, level)
        value = dot(lhs, g[h].reshape(4 * tokens, cols), 0, 0)
        dw[h, o] = value.astype(BF16).reshape(2, rows, cols)
        if i < line - 1:
            @pl.when(at == 0)
            def _():
                o_copy(True, h, line - 1 - i).start()

            @pl.when(at == line - 1)
            def _():
                o_copy(False, h, i).start()

    own_x.wait()
    own_c.wait()
    for copy in own_w:
        copy.wait()

    def own_level(h):
        for u in (0, 1):
            y_arrival(u, h).wait_recv()
            z_step(h, 0, 2 + u)
        for u in (0, 1):
            grow(u, h, 0)

    own_level(0)

    def got(slot, a):
        def run():
            if slot < 3:
                first[slot, a].wait_recv()
                if (slot, a) == (1, 0):
                    diag[0].start()
                if (slot, a) == (2, 1):
                    diag[1].start()
            else:
                diag[a].wait_recv()
            swap(slot, a).start()
        return run

    def use(slot, a):
        def run():
            swapped(slot, a)
            join(slot, a)
        return run

    def early():
        for h in range(final):
            def body(slot, _):
                make_g(h, slot)
                return 0

            lax.fori_loop(0, 4, body, 0)
            for i in range(line):
                make_dw(h, i)

    if parts == 2:
        hooks = {
            (0, 2, 1): [got(1, 0)],
            (0, 2, 3): [use(1, 0)],
            (1, 1, 1): [got(2, 1)],
            (1, 1, 3): [use(2, 1), got(1, 1)],
            (0, 3, 0): [use(1, 1)],
            (0, 3, 3): [got(2, 0)],
            (1, 2, 0): [use(2, 0)],
            (1, 2, 1): [got(3, 1)],
            (1, 2, 2): [use(3, 1)],
            (1, 3, 1): [got(3, 0)],
            (1, 3, 2): [use(3, 0), early],
        }
        steps = [(0, 1)]
        for s in range(2, line):
            steps += [(0, s), (1, s - 1)]
        steps += [(1, line - 1)]
    else:
        hooks = {
            (0, 1, 2): [got(1, 0)],
            (0, 1, 3): [use(1, 0)],
            (0, 2, 0): [got(2, 1)],
            (0, 2, 1): [got(1, 1), use(2, 1)],
            (0, 2, 2): [use(1, 1)],
            (0, 2, 3): [got(2, 0)],
            (0, 3, 0): [use(2, 0), got(3, 1)],
            (0, 3, 1): [use(3, 1)],
            (0, 3, 2): [got(3, 0)],
            (0, 3, 3): [use(3, 0), early],
        }
        steps = [(0, s) for s in range(1, line)]
    for h, s in steps:
        for j in range(4):
            z_step(h, s, j)
            if j >= 2 and (h, s, j) != (final, line - 1, 3):
                grow(j - 2, h, s)
            for run in hooks.pop((h, s, j), []):
                run()
        if (h, s) == (0, 1):
            for k in range(1, parts):
                z_step(k, 0, 0)
                z_step(k, 0, 1)
                own_level(k)
    for key in list(hooks):
        for run in hooks[key]:
            run()

    def p_copy(slot, k):
        there = lax.rem(c + k, n_tp)
        return remote(
            part_.at[slot, there], tpin.at[k - 1, slot], ps.at[k - 1, slot], pr.at[k - 1, slot], {"tp": there}
        )

    part = tokens // n_tp

    def make_part(slot):
        def body(lvl, _):
            span = pl.ds(pl.multiple_of(lvl * level, level), level)
            value = dot(g[0, slot], wu[0, lvl].reshape(level, cols), 1, 1)
            for h in range(1, parts):
                value = value + dot(g[h, slot], wu[h, lvl].reshape(level, cols), 1, 1)
            part_[slot, :, :, span] = value.astype(BF16).reshape(n_tp, part, level)
            return 0

        lax.fori_loop(0, line, body, 0)
        for k in range(1, n_tp):
            p_copy(slot, k).start()

    def tp_sum(slot):
        for k in range(1, n_tp):
            p_copy(slot, k).wait_recv()
        total = part_[slot, c].astype(F32)
        for k in range(1, n_tp):
            total = total + tpin[k - 1, slot].astype(F32)
        return total

    cut = (width * 3 // 8) // 128 * 128
    left, right = pl.ds(0, cut), pl.ds(cut, width - cut)
    q_copies = {
        "x3": remote(part_.at[3, c, :, left], q1.at[1, :, left], qs.at[0], qr.at[0], to_x),
        "y3": remote(part_.at[3, c, :, right], q1.at[1, :, right], qs.at[1], qr.at[1], to_y),
        "x1": remote(part_.at[1, c, :, left], q1.at[0, :, left], qs.at[2], qr.at[2], to_x),
        "y2": remote(part_.at[2, c, :, right], q1.at[0, :, right], qs.at[3], qr.at[3], to_y),
        "y2r": remote(part_.at[2, c, :, left], q2.at[:, left], qs.at[4], qr.at[4], to_y),
        "x1r": remote(part_.at[1, c, :, right], q2.at[:, right], qs.at[5], qr.at[5], to_x),
    }

    def store_sum(slot):
        part_[slot, c] = tp_sum(slot).astype(BF16)

    def add_in(d, h, o):
        dw[h, o] = (dw[h, o].astype(F32) + zin[d, h, o].astype(F32)).astype(BF16)

    def o_step(h, t):
        for go_up in (True, False):
            d = 0 if go_up else 1
            gap = at if go_up else line - 1 - at
            o = (line - 1 - t + at) if go_up else (t - line + 1 + at)

            @pl.when((gap > 0) & (gap <= t))
            def _():
                o_copy(go_up, h, o).wait_recv()
                if t < line - 1:
                    add_in(d, h, o)
                    o_copy(go_up, h, o).start()

    def dw_at(q, h):
        return dw_out.at[:, pl.ds(pl.multiple_of((q * parts + h) * cols, cols), cols)]

    e_x, e_y, e_own, e_r = [], [], [], []
    for h in range(parts):
        here, across = dw_at(quarter, h), dw_at(2 * r + 1 - p, h)
        e_x.append(remote(fin.at[h, p], here, es.at[0, h], er.at[0, h], to_x))
        e_y.append(remote(fin.at[h, 1 - p], here, es.at[1, h], er.at[1, h], to_y))
        e_own.append(pltpu.make_async_copy(fin.at[h, p], here, el.at[h]))
        e_r.append(remote(across, across, es.at[2, h], er.at[2, h], to_x))

    def finish(h):
        if line == 1:
            fin[h] = dw[h, at]
        for d, there in ((0, has_down), (1, has_up)):
            if line > 1:
                @pl.when(there & jnp.logical_not(has_up & has_down))
                def _():
                    fin[h] = (dw[h, at].astype(F32) + zin[d, h, at].astype(F32)).astype(BF16)

        @pl.when(has_up & has_down)
        def _():
            total = dw[h, at].astype(F32) + zin[0, h, at].astype(F32) + zin[1, h, at].astype(F32)
            fin[h] = total.astype(BF16)

        e_x[h].start()
        e_y[h].start()
        e_own[h].start()

    def relay(h):
        blk = dw_at(2 * r + 1 - p, h)
        remote(blk, blk, es.at[1, h], er.at[1, h], to_y).wait_recv()
        e_r[h].start()

    def in_first():
        q_copies["x3"].wait_recv()
        part_[2, c, :, left] = (part_[2, c, :, left].astype(F32) + q1[1, :, left].astype(F32)).astype(BF16)
        q_copies["y2r"].start()
        q_copies["y3"].wait_recv()
        part_[1, c, :, right] = (part_[1, c, :, right].astype(F32) + q1[1, :, right].astype(F32)).astype(BF16)
        q_copies["x1r"].start()

    out_own = pltpu.make_async_copy(fo, din_out.at[c], dl.at[0])
    out_peers = [
        remote(fo, din_out.at[c], ds.at[k - 1], dr.at[k - 1], {"tp": lax.rem(c + k, n_tp)}) for k in range(1, n_tp)
    ]

    def in_last():
        total = tp_sum(0)
        for name in ("x1", "y2", "y2r", "x1r"):
            q_copies[name].wait_recv()
        fo[...] = (total + q1[0].astype(F32) + q2[...].astype(F32)).astype(BF16)
        out_own.start()
        for copy in out_peers:
            copy.start()

    def last_rows(slot):
        if line > 1:
            grow_slot(1, final, line - 1, slot)
        make_g(final, slot)
        make_part(slot)

    last_rows(3)
    last_rows(1)
    store_sum(3)
    q_copies["x3"].start()
    q_copies["y3"].start()
    if parts > 1:
        o_step(0, 1)
    last_rows(2)
    store_sum(1)
    q_copies["x1"].start()
    store_sum(2)
    q_copies["y2"].start()
    last_rows(0)
    for i in range(line):
        make_dw(final, i)
    if parts == 1 and line > 1:
        o_step(0, 1)
    for t in range(2, line - 1):
        o_step(0, t)
    in_first()
    if line > 2:
        o_step(0, line - 1)
    finish(0)
    for h in range(1, parts):
        for t in range(1, line):
            o_step(h, t)
            if t == 1:
                relay(h - 1)
        if line == 1:
            relay(h - 1)
        finish(h)
    in_last()
    relay(final)

    for k in range(1, n_tp):
        out_peers[k - 1].wait_recv()
    for h in range(parts):
        for q, col in ((2 * (1 - r) + p, 0), (2 * (1 - r) + 1 - p, 2)):
            blk = dw_at(q, h)
            remote(blk, blk, es.at[col, h], er.at[col, h], to_x).wait_recv()
    out_own.wait()
    for copy in e_own:
        copy.wait()
    for copy in out_peers + e_x + e_y + e_r + list(q_copies.values()):
        copy.wait_send()
    for slot in range(4):
        for k in range(1, n_tp):
            p_copy(slot, k).wait_send()
    for h in range(parts):
        for o in range(line):
            @pl.when((at < o) & has_up)
            def _():
                o_copy(True, h, o).wait_send()

            @pl.when((at > o) & has_down)
            def _():
                o_copy(False, h, o).wait_send()
    for slot in (1, 2, 3):
        for a in (0, 1):
            swap(slot, a).wait_send()
    for copy in list(first.values()) + diag + y_copies:
        copy.wait_send()
    for h in range(parts):
        for s in range(line - 1):
            for j in range(4):
                for go_up in (True, False):
                    @pl.when(z_valid(go_up, s))
                    def _():
                        z_copy(go_up, h, s, j).wait_send()


def fused(n_fs, n_tp, n_rep, x, c, w_up, w_down):
    line = n_fs // 2
    tokens, width = x.shape
    rows, block = w_up.shape
    cols = block // (2 * n_rep)
    parts = 2 if cols % 256 == 0 and n_fs > 4 else 1
    cols = cols // parts
    native = rows % 128 == 0
    if not native:
        w_down = w_down.T
    part = tokens // n_tp
    dma = pltpu.SemaphoreType.DMA
    hbm = pl.BlockSpec(memory_space=pl.ANY)
    vmem = lambda *shape: pltpu.VMEM(shape, BF16)
    down_block = (cols, rows) if native else (rows, cols)
    others = max(n_tp - 1, 1)
    return pl.pallas_call(
        functools.partial(kernel, line, n_tp, native, parts),
        out_shape=(
            jax.ShapeDtypeStruct((rows, block), BF16),
            jax.ShapeDtypeStruct((n_tp, part, width), BF16),
        ),
        in_specs=[hbm] * 4,
        out_specs=(hbm,) * 2,
        scratch_shapes=[
            vmem(2, 4, tokens, width),
            vmem(parts, line, 2, rows, cols),
            vmem(parts, line, 2, *down_block),
            pltpu.VMEM((parts, 2, 4, tokens, cols), F32),
            vmem(parts, 4, tokens, cols),
            vmem(parts, line, 2, rows, cols),
            vmem(2, parts, line, 2, rows, cols),
            vmem(parts, 2, rows, cols),
            vmem(4, n_tp, part, width),
            vmem(others, 4, part, width),
            vmem(2, part, width),
            vmem(part, width),
            vmem(part, width),
            dma((2, parts, line, 4)), dma((2, parts, line, 4)), dma((parts, 2)), dma((parts, 2)),
            dma((3, 2)), dma((3, 2)), dma((3, 2)), dma((3, 2)), dma((2 + 2 * parts,)),
            dma((2, parts, line)), dma((2, parts, line)),
            dma((3, parts)), dma((3, parts)), dma((parts,)),
            dma((others, 4)), dma((others, 4)), dma((6,)), dma((6,)),
            dma((others,)), dma((others,)), dma((1,)),
        ],
        compiler_params=pltpu.CompilerParams(
            collective_id=0, has_side_effects=True, vmem_limit_bytes=60 * 2**20
        ),
        name="fused",
    )(x, c, w_up, w_down)


def per_device(inputs, w_up, w_down, cotangent):
    n_rep, n_fs, n_tp = lax.axis_size("rep"), lax.axis_size("fs"), lax.axis_size("tp")
    d_w, d_in = fused(n_fs, n_tp, n_rep, inputs, cotangent, w_up, w_down)
    return d_in.reshape(inputs.shape), d_w.astype(F32)


def solution(mesh):
    in_specs = (P(("rep", "fs"), None), P("fs", "tp"), P("tp", "fs"), P(("rep", "fs"), None))
    out_specs = (P(("rep", "fs"), None), P("fs", "tp"))
    return jax.shard_map(
        per_device, mesh=mesh, in_specs=in_specs, out_specs=out_specs, check_vma=False
    )
```

```python
import functools

import jax
import jax.numpy as jnp
from jax import lax
from jax.experimental import pallas as pl
from jax.experimental.pallas import tpu as pltpu
from jax.sharding import PartitionSpec as P

MESH = pl.DeviceIdType.MESH
F32, BF16 = jnp.float32, jnp.bfloat16


def dot(a, b, da, db):
    return lax.dot_general(a, b, (((da,), (db,)), ((), ())), preferred_element_type=F32)


def kernel(line, n_tp, native, parts, x_in, c_in, up_in, down_in, dw_out, din_out,
           xs, wu, wd, acc, g, dw, zin, fin, part_, tpin, q1, q2, fo,
           zs, zr, ys, yr, ts, tr, cs, cr, ls, os, orr, es, er, el, ps, pr, qs, qr, ds, dr, dl):
    r, f, c = lax.axis_index("rep"), lax.axis_index("fs"), lax.axis_index("tp")
    p, at = lax.rem(f, 2), lax.div(f, 2)
    core = lax.rem(c, 2)
    to_x, to_y = {"rep": 1 - r}, {"fs": f + 1 - 2 * p}
    to_core = {"tp": c + 1 - 2 * core}
    up, down = {"fs": f + 2}, {"fs": f - 2}
    has_up, has_down = at < line - 1, at > 0
    tokens, width = x_in.shape
    rows, cols = wu.shape[3:]
    level = 2 * rows
    final = parts - 1
    quarter = 2 * r + p

    barrier = pltpu.get_barrier_semaphore()
    peers = [{"tp": lax.rem(c + k, n_tp)} for k in range(1, n_tp)]
    for dev in [to_x, to_y] + peers:
        pl.semaphore_signal(barrier, inc=1, device_id=dev, device_id_type=MESH)

    @pl.when(has_up)
    def _():
        pl.semaphore_signal(barrier, inc=1, device_id=up, device_id_type=MESH)

    @pl.when(has_down)
    def _():
        pl.semaphore_signal(barrier, inc=1, device_id=down, device_id_type=MESH)

    def remote(src, dst, send, recv, dev):
        return pltpu.make_async_remote_copy(
            src_ref=src, dst_ref=dst, send_sem=send, recv_sem=recv, device_id=dev, device_id_type=MESH
        )

    half = tokens // 2
    mine = pl.ds(pl.multiple_of(core * half, half), half)
    theirs = pl.ds(pl.multiple_of((1 - core) * half, half), half)
    ws = (wu, wd)

    def own_block(u, q, h):
        span = pl.ds(pl.multiple_of((q * parts + h) * cols, cols), cols)
        if u == 1 and native:
            return down_in.at[span, :]
        return (up_in, down_in)[u].at[:, span]

    own_x = pltpu.make_async_copy(x_in, xs.at[0, 0], ls.at[0])
    own_c = pltpu.make_async_copy(c_in, xs.at[1, 0], ls.at[1])
    own_w = [
        pltpu.make_async_copy(own_block(u, quarter, h), ws[u].at[h, at, p], ls.at[2 + 2 * h + u])
        for h in range(parts) for u in (0, 1)
    ]
    own_x.start()
    own_c.start()
    for copy in own_w:
        copy.start()
    acc[...] = jnp.zeros_like(acc)

    n_near = n_tp + 1
    inner = has_up & has_down

    @pl.when(inner)
    def _():
        pl.semaphore_wait(barrier, n_near + 2)

    @pl.when(jnp.logical_not(inner))
    def _():
        pl.semaphore_wait(barrier, n_near + 1 if line > 1 else n_near)

    y_copies = [
        remote(own_block(u, 2 * r + 1 - p, h), ws[u].at[h, at, p], ys.at[h, u], yr.at[h, u], to_y)
        for h in range(parts) for u in (0, 1)
    ]

    def y_arrival(u, h):
        blk = ws[u].at[h, at, 1 - p]
        return remote(blk, blk, ys.at[h, u], yr.at[h, u], to_y)

    for copy in y_copies:
        copy.start()

    def z_copy(go_up, h, s, j):
        u, own_pair = j % 2, j < 2
        lvl = at - s if go_up else at + s
        blk = ws[u].at[h, lvl, p if own_pair else 1 - p]
        src = own_block(u, quarter, h) if (s == 0 and own_pair) else blk
        d = 0 if go_up else 1
        return remote(src, blk, zs.at[d, h, s, j], zr.at[d, h, s, j], up if go_up else down)

    def z_valid(go_up, s):
        return ((at - s >= 0) & has_up) if go_up else ((at + s < line) & has_down)

    def z_step(h, s, j):
        for go_up in (True, False):
            d = 0 if go_up else 1
            if s > 0:
                lvl = at - s if go_up else at + s

                @pl.when((lvl >= 0) & (lvl < line))
                def _():
                    blk = ws[j % 2].at[h, lvl, p if j < 2 else 1 - p]
                    remote(blk, blk, zs.at[d, h, s - 1, j], zr.at[d, h, s - 1, j], to_x).wait_recv()
            if s < line - 1:
                @pl.when(z_valid(go_up, s))
                def _():
                    z_copy(go_up, h, s, j).start()

    z_step(0, 0, 0)
    z_step(0, 0, 1)

    own = (x_in, c_in)
    first = {}
    for slot, dev in ((1, to_x), (2, to_y)):
        for a in (0, 1):
            first[slot, a] = remote(
                own[a].at[mine], xs.at[a, slot, mine], ts.at[slot - 1, a], tr.at[slot - 1, a], dev
            )
    first[1, 0].start()
    first[2, 1].start()
    first[1, 1].start()
    first[2, 0].start()
    most = half // 48 * 32
    base = pl.multiple_of(core * half, half)
    lead, rest = pl.ds(base, most), pl.ds(base + most, half - most)
    diag = [
        remote(xs.at[0, 1, lead], xs.at[0, 3, lead], ts.at[2, 0], tr.at[2, 0], to_y),
        remote(xs.at[1, 2, mine], xs.at[1, 3, mine], ts.at[2, 1], tr.at[2, 1], to_x),
        remote(xs.at[0, 2, rest], xs.at[0, 3, rest], ts.at[3, 0], tr.at[3, 0], to_x),
    ]

    def swap(slot, a):
        return remote(
            xs.at[a, slot, mine], xs.at[a, slot, mine], cs.at[slot - 1, a], cr.at[slot - 1, a], to_core
        )

    def swapped(slot, a):
        blk = xs.at[a, slot, theirs]
        remote(blk, blk, cs.at[slot - 1, a], cr.at[slot - 1, a], to_core).wait_recv()

    def unit(u, h, slot, lvl):
        if u == 1 and native:
            total = acc[h, u, slot]
            for b in (0, 1):
                span = pl.ds(pl.multiple_of(lvl * level + b * rows, rows), rows)
                total = total + dot(xs[u, slot, :, span], wd[h, lvl, b], 1, 1)
            acc[h, u, slot] = total
        else:
            span = pl.ds(pl.multiple_of(lvl * level, level), level)
            acc[h, u, slot] += dot(xs[u, slot, :, span], ws[u][h, lvl].reshape(level, cols), 1, 0)

    done = [[-1, -1] for _ in range(parts)]
    ready = [1, 1]

    def grow_slot(u, h, s, slot):
        for lvl in (at - s, at + s):
            @pl.when((lvl >= 0) & (lvl < line))
            def _():
                unit(u, h, slot, lvl)

    def grow(u, h, s):
        done[h][u] = s
        n = ready[u]
        if s == 0:
            def body(slot, _):
                unit(u, h, slot, at)
                return 0

            lax.fori_loop(0, n, body, 0)
            return

        def body(i, _):
            lvl = at + s - 2 * s * lax.rem(i, 2)

            @pl.when((lvl >= 0) & (lvl < line))
            def _():
                unit(u, h, lax.div(i, 2), lvl)
            return 0

        lax.fori_loop(0, 2 * n, body, 0)

    def join(slot, u):
        ready[u] += 1
        for h in range(parts):
            lo, hi = jnp.maximum(at - done[h][u], 0), jnp.minimum(at + done[h][u], line - 1)

            def body(lvl, _):
                unit(u, h, slot, lvl)
                return 0

            lax.fori_loop(lo, hi + 1, body, 0)

    def make_g(h, slot):
        g[h, slot] = (2.0 * jnp.maximum(acc[h, 0, slot], 0.0) * acc[h, 1, slot]).astype(BF16)

    low = at < line - at - 1

    def o_copy(go_up, h, o):
        d = 0 if go_up else 1
        return remote(dw.at[h, o], zin.at[d, h, o], os.at[d, h, o], orr.at[d, h, o], up if go_up else down)

    def make_dw(h, i):
        o = jnp.where(low, line - 1 - i, i)
        span = pl.ds(pl.multiple_of(o * level, level), level)
        lhs = xs[0, :, :, span].reshape(4 * tokens, level)
        value = dot(lhs, g[h].reshape(4 * tokens, cols), 0, 0)
        dw[h, o] = value.astype(BF16).reshape(2, rows, cols)
        if i < line - 1:
            @pl.when(at == 0)
            def _():
                o_copy(True, h, line - 1 - i).start()

            @pl.when(at == line - 1)
            def _():
                o_copy(False, h, i).start()

    own_x.wait()
    own_c.wait()
    for copy in own_w:
        copy.wait()

    def own_level(h):
        for u in (0, 1):
            y_arrival(u, h).wait_recv()
            z_step(h, 0, 2 + u)
        for u in (0, 1):
            grow(u, h, 0)

    own_level(0)

    def got(slot, a):
        def run():
            if slot < 3:
                first[slot, a].wait_recv()
                if (slot, a) == (1, 0):
                    diag[0].start()
                if (slot, a) == (2, 1):
                    diag[1].start()
                if (slot, a) == (2, 0):
                    diag[2].start()
            else:
                diag[a].wait_recv()
                if a == 0:
                    diag[2].wait_recv()
            swap(slot, a).start()
        return run

    def use(slot, a):
        def run():
            swapped(slot, a)
            join(slot, a)
        return run

    def early():
        for h in range(final):
            def body(slot, _):
                make_g(h, slot)
                return 0

            lax.fori_loop(0, 4, body, 0)
            for i in range(line):
                make_dw(h, i)

    if parts == 2:
        hooks = {
            (0, 2, 1): [got(1, 0)],
            (0, 2, 3): [use(1, 0)],
            (1, 1, 1): [got(2, 1)],
            (1, 1, 3): [use(2, 1), got(1, 1)],
            (0, 3, 0): [use(1, 1)],
            (0, 3, 3): [got(2, 0)],
            (1, 2, 0): [use(2, 0)],
            (1, 2, 1): [got(3, 1)],
            (1, 2, 2): [use(3, 1)],
            (1, 2, 3): [got(3, 0)],
            (1, 3, 0): [use(3, 0), early],
        }
        steps = [(0, 1)]
        for s in range(2, line):
            steps += [(0, s), (1, s - 1)]
        steps += [(1, line - 1)]
    else:
        hooks = {
            (0, 1, 2): [got(1, 0)],
            (0, 1, 3): [use(1, 0)],
            (0, 2, 0): [got(2, 1)],
            (0, 2, 1): [got(1, 1), use(2, 1)],
            (0, 2, 2): [use(1, 1)],
            (0, 2, 3): [got(2, 0)],
            (0, 3, 0): [use(2, 0), got(3, 1)],
            (0, 3, 1): [use(3, 1)],
            (0, 3, 2): [got(3, 0)],
            (0, 3, 3): [use(3, 0), early],
        }
        steps = [(0, s) for s in range(1, line)]
    for h, s in steps:
        for j in range(4):
            z_step(h, s, j)
            if j >= 2 and (h, s, j) != (final, line - 1, 3):
                grow(j - 2, h, s)
            for run in hooks.pop((h, s, j), []):
                run()
        if (h, s) == (0, 1):
            for k in range(1, parts):
                z_step(k, 0, 0)
                z_step(k, 0, 1)
                own_level(k)
    for key in list(hooks):
        for run in hooks[key]:
            run()

    def p_copy(slot, k):
        there = lax.rem(c + k, n_tp)
        return remote(
            part_.at[slot, there], tpin.at[k - 1, slot], ps.at[k - 1, slot], pr.at[k - 1, slot], {"tp": there}
        )

    part = tokens // n_tp

    def make_part(slot):
        def body(lvl, _):
            span = pl.ds(pl.multiple_of(lvl * level, level), level)
            value = dot(g[0, slot], wu[0, lvl].reshape(level, cols), 1, 1)
            for h in range(1, parts):
                value = value + dot(g[h, slot], wu[h, lvl].reshape(level, cols), 1, 1)
            part_[slot, :, :, span] = value.astype(BF16).reshape(n_tp, part, level)
            return 0

        lax.fori_loop(0, line, body, 0)
        for k in range(1, n_tp):
            p_copy(slot, k).start()

    def tp_sum(slot):
        for k in range(1, n_tp):
            p_copy(slot, k).wait_recv()
        total = part_[slot, c].astype(F32)
        for k in range(1, n_tp):
            total = total + tpin[k - 1, slot].astype(F32)
        return total

    cut = width * 7 // 16 // 128 * 128
    left, right = pl.ds(0, cut), pl.ds(cut, width - cut)
    q_copies = {
        "x3": remote(part_.at[3, c, :, left], q1.at[1, :, left], qs.at[0], qr.at[0], to_x),
        "y3": remote(part_.at[3, c, :, right], q1.at[1, :, right], qs.at[1], qr.at[1], to_y),
        "x1": remote(part_.at[1, c, :, left], q1.at[0, :, left], qs.at[2], qr.at[2], to_x),
        "y2": remote(part_.at[2, c, :, right], q1.at[0, :, right], qs.at[3], qr.at[3], to_y),
        "y2r": remote(part_.at[2, c, :, left], q2.at[:, left], qs.at[4], qr.at[4], to_y),
        "x1r": remote(part_.at[1, c, :, right], q2.at[:, right], qs.at[5], qr.at[5], to_x),
    }

    def store_sum(slot):
        part_[slot, c] = tp_sum(slot).astype(BF16)

    def add_in(d, h, o):
        dw[h, o] = (dw[h, o].astype(F32) + zin[d, h, o].astype(F32)).astype(BF16)

    def o_step(h, t):
        for go_up in (True, False):
            d = 0 if go_up else 1
            gap = at if go_up else line - 1 - at
            o = (line - 1 - t + at) if go_up else (t - line + 1 + at)

            @pl.when((gap > 0) & (gap <= t))
            def _():
                o_copy(go_up, h, o).wait_recv()
                if t < line - 1:
                    add_in(d, h, o)
                    o_copy(go_up, h, o).start()

    def dw_at(q, h):
        return dw_out.at[:, pl.ds(pl.multiple_of((q * parts + h) * cols, cols), cols)]

    e_x, e_y, e_own, e_r = [], [], [], []
    for h in range(parts):
        here, across = dw_at(quarter, h), dw_at(2 * r + 1 - p, h)
        e_x.append(remote(fin.at[h, p], here, es.at[0, h], er.at[0, h], to_x))
        e_y.append(remote(fin.at[h, 1 - p], here, es.at[1, h], er.at[1, h], to_y))
        e_own.append(pltpu.make_async_copy(fin.at[h, p], here, el.at[h]))
        e_r.append(remote(across, across, es.at[2, h], er.at[2, h], to_x))

    def finish(h):
        if line == 1:
            fin[h] = dw[h, at]
        for d, there in ((0, has_down), (1, has_up)):
            if line > 1:
                @pl.when(there & jnp.logical_not(has_up & has_down))
                def _():
                    fin[h] = (dw[h, at].astype(F32) + zin[d, h, at].astype(F32)).astype(BF16)

        @pl.when(has_up & has_down)
        def _():
            total = dw[h, at].astype(F32) + zin[0, h, at].astype(F32) + zin[1, h, at].astype(F32)
            fin[h] = total.astype(BF16)

        e_x[h].start()
        e_y[h].start()
        e_own[h].start()

    def relay(h):
        blk = dw_at(2 * r + 1 - p, h)
        remote(blk, blk, es.at[1, h], er.at[1, h], to_y).wait_recv()
        e_r[h].start()

    def in_x3():
        q_copies["x3"].wait_recv()
        part_[2, c, :, left] = (part_[2, c, :, left].astype(F32) + q1[1, :, left].astype(F32)).astype(BF16)

    def in_y3():
        q_copies["y3"].wait_recv()
        part_[1, c, :, right] = (part_[1, c, :, right].astype(F32) + q1[1, :, right].astype(F32)).astype(BF16)

    out_own = pltpu.make_async_copy(fo, din_out.at[c], dl.at[0])
    out_peers = [
        remote(fo, din_out.at[c], ds.at[k - 1], dr.at[k - 1], {"tp": lax.rem(c + k, n_tp)}) for k in range(1, n_tp)
    ]

    def in_last():
        total = tp_sum(0)
        for name in ("x1", "y2", "y2r", "x1r"):
            q_copies[name].wait_recv()
        fo[...] = (total + q1[0].astype(F32) + q2[...].astype(F32)).astype(BF16)
        out_own.start()
        for copy in out_peers:
            copy.start()

    def last_rows(slot):
        if line > 1:
            grow_slot(1, final, line - 1, slot)
        make_g(final, slot)

    def send(*names):
        for name in names:
            q_copies[name].start()

    def sums(h, lo, hi):
        for t in range(lo, min(hi, line)):
            o_step(h, t)

    def weights(lo, hi):
        for i in range(lo, min(hi, line)):
            make_dw(final, i)

    last_rows(3)
    make_part(3)
    for slot in (1, 2, 0):
        last_rows(slot)
    make_part(1)
    store_sum(3)
    send("x3", "y3")
    if parts > 1:
        sums(0, 1, 2)
    weights(0, 1)
    make_part(2)
    store_sum(1)
    send("x1")
    weights(1, 2)
    store_sum(2)
    send("y2")
    make_part(0)
    weights(2, line)
    if parts == 1:
        sums(0, 1, 2)
    sums(0, 2, line - 1)
    in_x3()
    if line > 2:
        sums(0, line - 1, line)
    finish(0)
    send("y2r")
    in_y3()
    send("x1r")
    for h in range(1, parts):
        sums(h, 1, line - 1)
        relay(h - 1)
        sums(h, max(line - 1, 1), line)
        finish(h)
    in_last()
    relay(final)

    for k in range(1, n_tp):
        out_peers[k - 1].wait_recv()
    for h in range(parts):
        for q, col in ((2 * (1 - r) + p, 0), (2 * (1 - r) + 1 - p, 2)):
            blk = dw_at(q, h)
            remote(blk, blk, es.at[col, h], er.at[col, h], to_x).wait_recv()
    out_own.wait()
    for copy in e_own:
        copy.wait()
    for copy in out_peers + e_x + e_y + e_r + list(q_copies.values()):
        copy.wait_send()
    for slot in range(4):
        for k in range(1, n_tp):
            p_copy(slot, k).wait_send()
    for h in range(parts):
        for o in range(line):
            @pl.when((at < o) & has_up)
            def _():
                o_copy(True, h, o).wait_send()

            @pl.when((at > o) & has_down)
            def _():
                o_copy(False, h, o).wait_send()
    for slot in (1, 2, 3):
        for a in (0, 1):
            swap(slot, a).wait_send()
    for copy in list(first.values()) + diag + y_copies:
        copy.wait_send()
    for h in range(parts):
        for s in range(line - 1):
            for j in range(4):
                for go_up in (True, False):
                    @pl.when(z_valid(go_up, s))
                    def _():
                        z_copy(go_up, h, s, j).wait_send()


def fused(n_fs, n_tp, n_rep, x, c, w_up, w_down):
    line = n_fs // 2
    tokens, width = x.shape
    rows, block = w_up.shape
    cols = block // (2 * n_rep)
    parts = 2 if cols % 256 == 0 and n_fs > 4 else 1
    cols = cols // parts
    native = rows % 128 == 0
    if not native:
        w_down = w_down.T
    part = tokens // n_tp
    dma = pltpu.SemaphoreType.DMA
    hbm = pl.BlockSpec(memory_space=pl.ANY)
    vmem = lambda *shape: pltpu.VMEM(shape, BF16)
    down_block = (cols, rows) if native else (rows, cols)
    others = max(n_tp - 1, 1)
    return pl.pallas_call(
        functools.partial(kernel, line, n_tp, native, parts),
        out_shape=(
            jax.ShapeDtypeStruct((rows, block), BF16),
            jax.ShapeDtypeStruct((n_tp, part, width), BF16),
        ),
        in_specs=[hbm] * 4,
        out_specs=(hbm,) * 2,
        scratch_shapes=[
            vmem(2, 4, tokens, width),
            vmem(parts, line, 2, rows, cols),
            vmem(parts, line, 2, *down_block),
            pltpu.VMEM((parts, 2, 4, tokens, cols), F32),
            vmem(parts, 4, tokens, cols),
            vmem(parts, line, 2, rows, cols),
            vmem(2, parts, line, 2, rows, cols),
            vmem(parts, 2, rows, cols),
            vmem(4, n_tp, part, width),
            vmem(others, 4, part, width),
            vmem(2, part, width),
            vmem(part, width),
            vmem(part, width),
            dma((2, parts, line, 4)), dma((2, parts, line, 4)), dma((parts, 2)), dma((parts, 2)),
            dma((4, 2)), dma((4, 2)), dma((3, 2)), dma((3, 2)), dma((2 + 2 * parts,)),
            dma((2, parts, line)), dma((2, parts, line)),
            dma((3, parts)), dma((3, parts)), dma((parts,)),
            dma((others, 4)), dma((others, 4)), dma((6,)), dma((6,)),
            dma((others,)), dma((others,)), dma((1,)),
        ],
        compiler_params=pltpu.CompilerParams(
            collective_id=0, has_side_effects=True, vmem_limit_bytes=60 * 2**20
        ),
        name="fused",
    )(x, c, w_up, w_down)


def per_device(inputs, w_up, w_down, cotangent):
    n_rep, n_fs, n_tp = lax.axis_size("rep"), lax.axis_size("fs"), lax.axis_size("tp")
    d_w, d_in = fused(n_fs, n_tp, n_rep, inputs, cotangent, w_up, w_down)
    return d_in.reshape(inputs.shape), d_w.astype(F32)


def solution(mesh):
    in_specs = (P(("rep", "fs"), None), P("fs", "tp"), P("tp", "fs"), P(("rep", "fs"), None))
    out_specs = (P(("rep", "fs"), None), P("fs", "tp"))
    return jax.shard_map(
        per_device, mesh=mesh, in_specs=in_specs, out_specs=out_specs, check_vma=False
    )
```

```python
import functools

import jax
import jax.numpy as jnp
from jax import lax
from jax.experimental import pallas as pl
from jax.experimental.pallas import tpu as pltpu
from jax.sharding import PartitionSpec as P

MESH = pl.DeviceIdType.MESH
F32, BF16 = jnp.float32, jnp.bfloat16


def dot(a, b, da, db):
    return lax.dot_general(a, b, (((da,), (db,)), ((), ())), preferred_element_type=F32)


def kernel(line, n_tp, native, parts, x_in, c_in, up_in, down_in, dw_out, din_out,
           xs, wu, wd, acc, g, dw, zin, fin, part_, tpin, q1, q2, fo,
           zs, zr, ys, yr, ts, tr, cs, cr, ls, os, orr, es, er, el, ps, pr, qs, qr, ds, dr, dl):
    r, f, c = lax.axis_index("rep"), lax.axis_index("fs"), lax.axis_index("tp")
    p, at = lax.rem(f, 2), lax.div(f, 2)
    core = lax.rem(c, 2)
    to_x, to_y = {"rep": 1 - r}, {"fs": f + 1 - 2 * p}
    to_core = {"tp": c + 1 - 2 * core}
    up, down = {"fs": f + 2}, {"fs": f - 2}
    has_up, has_down = at < line - 1, at > 0
    tokens, width = x_in.shape
    rows, cols = wu.shape[3:]
    level = 2 * rows
    final = parts - 1
    quarter = 2 * r + p

    barrier = pltpu.get_barrier_semaphore()
    peers = [{"tp": lax.rem(c + k, n_tp)} for k in range(1, n_tp)]
    for dev in [to_x, to_y] + peers:
        pl.semaphore_signal(barrier, inc=1, device_id=dev, device_id_type=MESH)

    @pl.when(has_up)
    def _():
        pl.semaphore_signal(barrier, inc=1, device_id=up, device_id_type=MESH)

    @pl.when(has_down)
    def _():
        pl.semaphore_signal(barrier, inc=1, device_id=down, device_id_type=MESH)

    def remote(src, dst, send, recv, dev):
        return pltpu.make_async_remote_copy(
            src_ref=src, dst_ref=dst, send_sem=send, recv_sem=recv, device_id=dev, device_id_type=MESH
        )

    half = tokens // 2
    mine = pl.ds(pl.multiple_of(core * half, half), half)
    theirs = pl.ds(pl.multiple_of((1 - core) * half, half), half)
    ws = (wu, wd)

    def own_block(u, q, h):
        span = pl.ds(pl.multiple_of((q * parts + h) * cols, cols), cols)
        if u == 1 and native:
            return down_in.at[span, :]
        return (up_in, down_in)[u].at[:, span]

    own_x = pltpu.make_async_copy(x_in, xs.at[0, 0], ls.at[0])
    own_c = pltpu.make_async_copy(c_in, xs.at[1, 0], ls.at[1])
    own_w = [
        pltpu.make_async_copy(own_block(u, quarter, h), ws[u].at[h, at, p], ls.at[2 + 2 * h + u])
        for h in range(parts) for u in (0, 1)
    ]
    own_x.start()
    own_c.start()
    for copy in own_w:
        copy.start()
    acc[...] = jnp.zeros_like(acc)

    n_near = n_tp + 1
    inner = has_up & has_down

    @pl.when(inner)
    def _():
        pl.semaphore_wait(barrier, n_near + 2)

    @pl.when(jnp.logical_not(inner))
    def _():
        pl.semaphore_wait(barrier, n_near + 1 if line > 1 else n_near)

    y_copies = [
        remote(own_block(u, 2 * r + 1 - p, h), ws[u].at[h, at, p], ys.at[h, u], yr.at[h, u], to_y)
        for h in range(parts) for u in (0, 1)
    ]

    def y_arrival(u, h):
        blk = ws[u].at[h, at, 1 - p]
        return remote(blk, blk, ys.at[h, u], yr.at[h, u], to_y)

    for copy in y_copies:
        copy.start()

    def z_copy(go_up, h, s, j):
        u, own_pair = j % 2, j < 2
        lvl = at - s if go_up else at + s
        blk = ws[u].at[h, lvl, p if own_pair else 1 - p]
        src = own_block(u, quarter, h) if (s == 0 and own_pair) else blk
        d = 0 if go_up else 1
        return remote(src, blk, zs.at[d, h, s, j], zr.at[d, h, s, j], up if go_up else down)

    def z_valid(go_up, s):
        return ((at - s >= 0) & has_up) if go_up else ((at + s < line) & has_down)

    def z_step(h, s, j):
        for go_up in (True, False):
            d = 0 if go_up else 1
            if s > 0:
                lvl = at - s if go_up else at + s

                @pl.when((lvl >= 0) & (lvl < line))
                def _():
                    blk = ws[j % 2].at[h, lvl, p if j < 2 else 1 - p]
                    remote(blk, blk, zs.at[d, h, s - 1, j], zr.at[d, h, s - 1, j], to_x).wait_recv()
            if s < line - 1:
                @pl.when(z_valid(go_up, s))
                def _():
                    z_copy(go_up, h, s, j).start()

    z_step(0, 0, 0)
    z_step(0, 0, 1)

    own = (x_in, c_in)
    first = {}
    for slot, dev in ((1, to_x), (2, to_y)):
        for a in (0, 1):
            first[slot, a] = remote(
                own[a].at[mine], xs.at[a, slot, mine], ts.at[slot - 1, a], tr.at[slot - 1, a], dev
            )
    first[1, 0].start()
    first[2, 1].start()
    first[1, 1].start()
    first[2, 0].start()
    most = half // 48 * 32
    base = pl.multiple_of(core * half, half)
    lead, rest = pl.ds(base, most), pl.ds(base + most, half - most)
    diag = [
        remote(xs.at[0, 1, lead], xs.at[0, 3, lead], ts.at[2, 0], tr.at[2, 0], to_y),
        remote(xs.at[1, 2, mine], xs.at[1, 3, mine], ts.at[2, 1], tr.at[2, 1], to_x),
        remote(xs.at[0, 2, rest], xs.at[0, 3, rest], ts.at[3, 0], tr.at[3, 0], to_x),
    ]

    def swap(slot, a):
        return remote(
            xs.at[a, slot, mine], xs.at[a, slot, mine], cs.at[slot - 1, a], cr.at[slot - 1, a], to_core
        )

    def swapped(slot, a):
        blk = xs.at[a, slot, theirs]
        remote(blk, blk, cs.at[slot - 1, a], cr.at[slot - 1, a], to_core).wait_recv()

    def unit(u, h, slot, lvl):
        if u == 1 and native:
            total = acc[h, u, slot]
            for b in (0, 1):
                span = pl.ds(pl.multiple_of(lvl * level + b * rows, rows), rows)
                total = total + dot(xs[u, slot, :, span], wd[h, lvl, b], 1, 1)
            acc[h, u, slot] = total
        else:
            span = pl.ds(pl.multiple_of(lvl * level, level), level)
            acc[h, u, slot] += dot(xs[u, slot, :, span], ws[u][h, lvl].reshape(level, cols), 1, 0)

    done = [[-1, -1] for _ in range(parts)]
    ready = [1, 1]

    def grow_slot(u, h, s, slot):
        for lvl in (at - s, at + s):
            @pl.when((lvl >= 0) & (lvl < line))
            def _():
                unit(u, h, slot, lvl)

    def grow(u, h, s):
        done[h][u] = s
        n = ready[u]
        if s == 0:
            def body(slot, _):
                unit(u, h, slot, at)
                return 0

            lax.fori_loop(0, n, body, 0)
            return

        def body(i, _):
            lvl = at + s - 2 * s * lax.rem(i, 2)

            @pl.when((lvl >= 0) & (lvl < line))
            def _():
                unit(u, h, lax.div(i, 2), lvl)
            return 0

        lax.fori_loop(0, 2 * n, body, 0)

    def join(slot, u, halves):
        for h in halves:
            lo, hi = jnp.maximum(at - done[h][u], 0), jnp.minimum(at + done[h][u], line - 1)

            def body(lvl, _):
                unit(u, h, slot, lvl)
                return 0

            lax.fori_loop(lo, hi + 1, body, 0)

    def make_g(h, slot):
        g[h, slot] = (2.0 * jnp.maximum(acc[h, 0, slot], 0.0) * acc[h, 1, slot]).astype(BF16)

    low = at < line - at - 1

    turns = (1 - p, p)

    def o_copy(go_up, h, o, k):
        d, b = 0 if go_up else 1, turns[k]
        return remote(
            dw.at[h, o, b], zin.at[d, h, o, b], os.at[d, h, o, k], orr.at[d, h, o, k], up if go_up else down
        )

    def make_dw(h, i):
        o = jnp.where(low, line - 1 - i, i)
        span = pl.ds(pl.multiple_of(o * level, level), level)
        lhs = xs[0, :, :, span].reshape(4 * tokens, level)
        value = dot(lhs, g[h].reshape(4 * tokens, cols), 0, 0)
        dw[h, o] = value.astype(BF16).reshape(2, rows, cols)
        if i < line - 1:
            @pl.when(at == 0)
            def _():
                for k in (0, 1):
                    o_copy(True, h, line - 1 - i, k).start()

            @pl.when(at == line - 1)
            def _():
                for k in (0, 1):
                    o_copy(False, h, i, k).start()

    own_x.wait()
    own_c.wait()
    for copy in own_w:
        copy.wait()

    def own_level(h):
        for u in (0, 1):
            y_arrival(u, h).wait_recv()
            z_step(h, 0, 2 + u)
        for u in (0, 1):
            grow(u, h, 0)

    own_level(0)

    def got(slot, a):
        def run():
            if slot < 3:
                first[slot, a].wait_recv()
                if (slot, a) == (1, 0):
                    diag[0].start()
                if (slot, a) == (2, 1):
                    diag[1].start()
                if (slot, a) == (2, 0):
                    diag[2].start()
            else:
                diag[a].wait_recv()
                if a == 0:
                    diag[2].wait_recv()
            swap(slot, a).start()
        return run

    def use(slot, a):
        def run():
            swapped(slot, a)
            ready[a] += 1
            join(slot, a, range(parts))
        return run

    def early():
        swapped(3, 0)
        ready[0] += 1
        for h in range(final):
            join(3, 0, [h])

            def body(slot, _):
                make_g(h, slot)
                return 0

            lax.fori_loop(0, 4, body, 0)
            for i in range(line):
                make_dw(h, i)
        join(3, 0, [final])

    if parts == 2:
        hooks = {
            (0, 2, 1): [got(1, 0)],
            (0, 2, 3): [use(1, 0)],
            (1, 1, 1): [got(2, 1)],
            (1, 1, 3): [use(2, 1), got(1, 1)],
            (0, 3, 0): [use(1, 1)],
            (0, 3, 3): [got(2, 0)],
            (1, 2, 0): [use(2, 0)],
            (1, 2, 1): [got(3, 1)],
            (1, 2, 2): [use(3, 1), got(3, 0)],
            (1, 2, 3): [early],
        }
        steps = [(0, 1)]
        for s in range(2, line):
            steps += [(0, s), (1, s - 1)]
        steps += [(1, line - 1)]
    else:
        hooks = {
            (0, 1, 2): [got(1, 0)],
            (0, 1, 3): [use(1, 0)],
            (0, 2, 0): [got(2, 1)],
            (0, 2, 1): [got(1, 1), use(2, 1)],
            (0, 2, 2): [use(1, 1)],
            (0, 2, 3): [got(2, 0)],
            (0, 3, 0): [use(2, 0), got(3, 1)],
            (0, 3, 1): [use(3, 1)],
            (0, 3, 2): [got(3, 0)],
            (0, 3, 3): [early],
        }
        steps = [(0, s) for s in range(1, line)]
    for h, s in steps:
        for j in range(4):
            z_step(h, s, j)
            if j >= 2 and (h, s, j) != (final, line - 1, 3):
                grow(j - 2, h, s)
            for run in hooks.pop((h, s, j), []):
                run()
        if (h, s) == (0, 1):
            for k in range(1, parts):
                z_step(k, 0, 0)
                z_step(k, 0, 1)
                own_level(k)
    for key in list(hooks):
        for run in hooks[key]:
            run()

    def p_copy(slot, k):
        there = lax.rem(c + k, n_tp)
        return remote(
            part_.at[slot, there], tpin.at[k - 1, slot], ps.at[k - 1, slot], pr.at[k - 1, slot], {"tp": there}
        )

    part = tokens // n_tp

    def make_part(slot):
        def body(lvl, _):
            span = pl.ds(pl.multiple_of(lvl * level, level), level)
            value = dot(g[0, slot], wu[0, lvl].reshape(level, cols), 1, 1)
            for h in range(1, parts):
                value = value + dot(g[h, slot], wu[h, lvl].reshape(level, cols), 1, 1)
            part_[slot, :, :, span] = value.astype(BF16).reshape(n_tp, part, level)
            return 0

        lax.fori_loop(0, line, body, 0)
        for k in range(1, n_tp):
            p_copy(slot, k).start()

    def make_part_rows(slot):
        for k in list(range(1, n_tp)) + [0]:
            there = lax.rem(c + k, n_tp)
            tok = pl.ds(pl.multiple_of(there * part, part), part)

            def body(lvl, _):
                span = pl.ds(pl.multiple_of(lvl * level, level), level)
                value = dot(g[0, slot, tok], wu[0, lvl].reshape(level, cols), 1, 1)
                for h in range(1, parts):
                    value = value + dot(g[h, slot, tok], wu[h, lvl].reshape(level, cols), 1, 1)
                part_[slot, there, :, span] = value.astype(BF16)
                return 0

            lax.fori_loop(0, line, body, 0)
            if k > 0:
                p_copy(slot, k).start()

    def tp_sum(slot):
        for k in range(1, n_tp):
            p_copy(slot, k).wait_recv()
        total = part_[slot, c].astype(F32)
        for k in range(1, n_tp):
            total = total + tpin[k - 1, slot].astype(F32)
        return total

    cut = width * 7 // 16 // 128 * 128
    left, right = pl.ds(0, cut), pl.ds(cut, width - cut)
    q_copies = {
        "x3": remote(part_.at[3, c, :, left], q1.at[1, :, left], qs.at[0], qr.at[0], to_x),
        "y3": remote(part_.at[3, c, :, right], q1.at[1, :, right], qs.at[1], qr.at[1], to_y),
        "x1": remote(part_.at[1, c, :, left], q1.at[0, :, left], qs.at[2], qr.at[2], to_x),
        "y2": remote(part_.at[2, c, :, right], q1.at[0, :, right], qs.at[3], qr.at[3], to_y),
        "y2r": remote(part_.at[2, c, :, left], q2.at[:, left], qs.at[4], qr.at[4], to_y),
        "x1r": remote(part_.at[1, c, :, right], q2.at[:, right], qs.at[5], qr.at[5], to_x),
    }

    def store_sum(slot):
        part_[slot, c] = tp_sum(slot).astype(BF16)

    def o_step(h, t, k):
        b = turns[k]
        for go_up in (True, False):
            d = 0 if go_up else 1
            gap = at if go_up else line - 1 - at
            o = (line - 1 - t + at) if go_up else (t - line + 1 + at)

            @pl.when((gap > 0) & (gap <= t))
            def _():
                o_copy(go_up, h, o, k).wait_recv()
                if t < line - 1:
                    dw[h, o, b] = (dw[h, o, b].astype(F32) + zin[d, h, o, b].astype(F32)).astype(BF16)
                    o_copy(go_up, h, o, k).start()

    half_rows = [pl.ds(i * (rows // 2), rows // 2) for i in (0, 1)]

    def dw_at(q, h, span=slice(None)):
        return dw_out.at[span, pl.ds(pl.multiple_of((q * parts + h) * cols, cols), cols)]

    def e_y(h, i):
        here = dw_at(quarter, h, half_rows[i])
        return remote(fin.at[h, 1 - p, half_rows[i]], here, es.at[1, h, i], er.at[1, h, i], to_y)

    def e_relay(h, i):
        here = dw_at(2 * r + 1 - p, h, half_rows[i])
        return remote(here, here, es.at[2, h, i], er.at[2, h, i], to_x)

    def e_x(h):
        return remote(fin.at[h, p], dw_at(quarter, h), es.at[0, h, 0], er.at[0, h, 0], to_x)

    def e_own(h):
        return pltpu.make_async_copy(fin.at[h, p], dw_at(quarter, h), el.at[h])

    def finish(h, k):
        b = turns[k]
        for d, there in ((0, has_down), (1, has_up)):
            @pl.when(there & jnp.logical_not(has_up & has_down))
            def _():
                fin[h, b] = (dw[h, at, b].astype(F32) + zin[d, h, at, b].astype(F32)).astype(BF16)

        @pl.when(has_up & has_down)
        def _():
            total = dw[h, at, b].astype(F32) + zin[0, h, at, b].astype(F32) + zin[1, h, at, b].astype(F32)
            fin[h, b] = total.astype(BF16)

        if line == 1:
            fin[h, b] = dw[h, at, b]
        if k == 0:
            e_y(h, 0).start()
            e_y(h, 1).start()
        else:
            e_x(h).start()
            e_own(h).start()

    def relay(h):
        for i in (0, 1):
            blk = dw_at(2 * r + 1 - p, h, half_rows[i])
            remote(blk, blk, es.at[1, h, i], er.at[1, h, i], to_y).wait_recv()
            e_relay(h, i).start()

    def in_x3():
        q_copies["x3"].wait_recv()
        part_[2, c, :, left] = (part_[2, c, :, left].astype(F32) + q1[1, :, left].astype(F32)).astype(BF16)

    def in_y3():
        q_copies["y3"].wait_recv()
        part_[1, c, :, right] = (part_[1, c, :, right].astype(F32) + q1[1, :, right].astype(F32)).astype(BF16)

    out_own = pltpu.make_async_copy(fo, din_out.at[c], dl.at[0])
    out_peers = [
        remote(fo, din_out.at[c], ds.at[k - 1], dr.at[k - 1], {"tp": lax.rem(c + k, n_tp)}) for k in range(1, n_tp)
    ]

    def in_last():
        total = tp_sum(0)
        for name in ("x1", "y2", "y2r", "x1r"):
            q_copies[name].wait_recv()
        fo[...] = (total + q1[0].astype(F32) + q2[...].astype(F32)).astype(BF16)
        out_own.start()
        for copy in out_peers:
            copy.start()

    def last_rows(slot):
        if line > 1:
            grow_slot(1, final, line - 1, slot)
        make_g(final, slot)

    def send(*names):
        for name in names:
            q_copies[name].start()

    def sums(h, t, k):
        if 1 <= t < line:
            o_step(h, t, k)

    def weights(lo, hi):
        for i in range(lo, min(hi, line)):
            make_dw(final, i)

    def close(h):
        for k in (0, 1):
            sums(h, line - 1, k)
            finish(h, k)

    split = parts > 1
    last_rows(3)
    make_part_rows(3)
    for slot in (1, 2, 0):
        last_rows(slot)
    store_sum(3)
    send("x3", "y3")
    if split:
        sums(0, 1, 0)
    make_part(1)
    if split:
        sums(0, 1, 1)
    weights(0, 1)
    make_part(2)
    store_sum(1)
    send("x1")
    if split:
        sums(0, 2, 0)
    weights(1, 2)
    make_part(0)
    store_sum(2)
    send("y2")
    if split:
        sums(0, 2, 1)
    weights(2, line)
    for t in range(3 if split else 1, line - 1):
        for k in (0, 1):
            sums(0, t, k)
    close(0)
    in_x3()
    send("y2r")
    in_y3()
    send("x1r")
    for h in range(1, parts):
        for t in range(1, line - 1):
            for k in (0, 1):
                sums(h, t, k)
        relay(h - 1)
        close(h)
    in_last()
    relay(final)

    for k in range(1, n_tp):
        out_peers[k - 1].wait_recv()
    for h in range(parts):
        blk = dw_at(2 * (1 - r) + p, h)
        remote(blk, blk, es.at[0, h, 0], er.at[0, h, 0], to_x).wait_recv()
        for i in (0, 1):
            blk = dw_at(2 * (1 - r) + 1 - p, h, half_rows[i])
            remote(blk, blk, es.at[2, h, i], er.at[2, h, i], to_x).wait_recv()
    out_own.wait()
    for copy in out_peers + list(q_copies.values()):
        copy.wait_send()
    for h in range(parts):
        e_own(h).wait()
        e_x(h).wait_send()
        for i in (0, 1):
            e_y(h, i).wait_send()
            e_relay(h, i).wait_send()
    for slot in range(4):
        for k in range(1, n_tp):
            p_copy(slot, k).wait_send()
    for h in range(parts):
        for o in range(line):
            @pl.when((at < o) & has_up)
            def _():
                for k in (0, 1):
                    o_copy(True, h, o, k).wait_send()

            @pl.when((at > o) & has_down)
            def _():
                for k in (0, 1):
                    o_copy(False, h, o, k).wait_send()
    for slot in (1, 2, 3):
        for a in (0, 1):
            swap(slot, a).wait_send()
    for copy in list(first.values()) + diag + y_copies:
        copy.wait_send()
    for h in range(parts):
        for s in range(line - 1):
            for j in range(4):
                for go_up in (True, False):
                    @pl.when(z_valid(go_up, s))
                    def _():
                        z_copy(go_up, h, s, j).wait_send()


def fused(n_fs, n_tp, n_rep, x, c, w_up, w_down):
    line = n_fs // 2
    tokens, width = x.shape
    rows, block = w_up.shape
    cols = block // (2 * n_rep)
    parts = 2 if cols % 256 == 0 and n_fs > 4 else 1
    cols = cols // parts
    native = rows % 128 == 0
    if not native:
        w_down = w_down.T
    part = tokens // n_tp
    dma = pltpu.SemaphoreType.DMA
    hbm = pl.BlockSpec(memory_space=pl.ANY)
    vmem = lambda *shape: pltpu.VMEM(shape, BF16)
    down_block = (cols, rows) if native else (rows, cols)
    others = max(n_tp - 1, 1)
    return pl.pallas_call(
        functools.partial(kernel, line, n_tp, native, parts),
        out_shape=(
            jax.ShapeDtypeStruct((rows, block), BF16),
            jax.ShapeDtypeStruct((n_tp, part, width), BF16),
        ),
        in_specs=[hbm] * 4,
        out_specs=(hbm,) * 2,
        scratch_shapes=[
            vmem(2, 4, tokens, width),
            vmem(parts, line, 2, rows, cols),
            vmem(parts, line, 2, *down_block),
            pltpu.VMEM((parts, 2, 4, tokens, cols), F32),
            vmem(parts, 4, tokens, cols),
            vmem(parts, line, 2, rows, cols),
            vmem(2, parts, line, 2, rows, cols),
            vmem(parts, 2, rows, cols),
            vmem(4, n_tp, part, width),
            vmem(others, 4, part, width),
            vmem(2, part, width),
            vmem(part, width),
            vmem(part, width),
            dma((2, parts, line, 4)), dma((2, parts, line, 4)), dma((parts, 2)), dma((parts, 2)),
            dma((4, 2)), dma((4, 2)), dma((3, 2)), dma((3, 2)), dma((2 + 2 * parts,)),
            dma((2, parts, line, 2)), dma((2, parts, line, 2)),
            dma((4, parts, 2)), dma((4, parts, 2)), dma((parts,)),
            dma((others, 4)), dma((others, 4)), dma((6,)), dma((6,)),
            dma((others,)), dma((others,)), dma((1,)),
        ],
        compiler_params=pltpu.CompilerParams(
            collective_id=0, has_side_effects=True, vmem_limit_bytes=60 * 2**20
        ),
        name="fused",
    )(x, c, w_up, w_down)


def per_device(inputs, w_up, w_down, cotangent):
    n_rep, n_fs, n_tp = lax.axis_size("rep"), lax.axis_size("fs"), lax.axis_size("tp")
    d_w, d_in = fused(n_fs, n_tp, n_rep, inputs, cotangent, w_up, w_down)
    return d_in.reshape(inputs.shape), d_w.astype(F32)


def solution(mesh):
    in_specs = (P(("rep", "fs"), None), P("fs", "tp"), P("tp", "fs"), P(("rep", "fs"), None))
    out_specs = (P(("rep", "fs"), None), P("fs", "tp"))
    return jax.shard_map(
        per_device, mesh=mesh, in_specs=in_specs, out_specs=out_specs, check_vma=False
    )
```

```python
import functools

import jax
import jax.numpy as jnp
from jax import lax
from jax.experimental import pallas as pl
from jax.experimental.pallas import tpu as pltpu
from jax.sharding import PartitionSpec as P

MESH = pl.DeviceIdType.MESH
F32, BF16 = jnp.float32, jnp.bfloat16


def dot(a, b, da, db):
    return lax.dot_general(a, b, (((da,), (db,)), ((), ())), preferred_element_type=F32)


def kernel(line, n_tp, native, parts, x_in, c_in, up_in, down_in, dw_out, din_out,
           xs, wu, wd, acc, g, dw, zin, fin, part_, tpin, q1, q2, fo, ahead,
           zs, zr, ys, yr, ts, tr, cs, cr, ls, os, orr, es, er, el, ps, pr, qs, qr, ds, dr, dl):
    r, f, c = lax.axis_index("rep"), lax.axis_index("fs"), lax.axis_index("tp")
    p, at = lax.rem(f, 2), lax.div(f, 2)
    core = lax.rem(c, 2)
    to_x, to_y = {"rep": 1 - r}, {"fs": f + 1 - 2 * p}
    to_core = {"tp": c + 1 - 2 * core}
    up, down = {"fs": f + 2}, {"fs": f - 2}
    has_up, has_down = at < line - 1, at > 0
    tokens, width = x_in.shape
    rows, cols = wu.shape[3:]
    level = 2 * rows
    final = parts - 1
    quarter = 2 * r + p

    barrier = pltpu.get_barrier_semaphore()
    peers = [{"tp": lax.rem(c + k, n_tp)} for k in range(1, n_tp)]
    for dev in [to_x, to_y] + peers:
        pl.semaphore_signal(barrier, inc=1, device_id=dev, device_id_type=MESH)

    @pl.when(has_up)
    def _():
        pl.semaphore_signal(barrier, inc=1, device_id=up, device_id_type=MESH)

    @pl.when(has_down)
    def _():
        pl.semaphore_signal(barrier, inc=1, device_id=down, device_id_type=MESH)

    def remote(src, dst, send, recv, dev):
        return pltpu.make_async_remote_copy(
            src_ref=src, dst_ref=dst, send_sem=send, recv_sem=recv, device_id=dev, device_id_type=MESH
        )

    half = tokens // 2
    mine = pl.ds(pl.multiple_of(core * half, half), half)
    theirs = pl.ds(pl.multiple_of((1 - core) * half, half), half)
    ws = (wu, wd)

    def own_block(u, q, h):
        span = pl.ds(pl.multiple_of((q * parts + h) * cols, cols), cols)
        if u == 1 and native:
            return down_in.at[span, :]
        return (up_in, down_in)[u].at[:, span]

    own_x = pltpu.make_async_copy(x_in, xs.at[0, 0], ls.at[0])
    own_c = pltpu.make_async_copy(c_in, xs.at[1, 0], ls.at[1])
    own_w = [
        pltpu.make_async_copy(own_block(u, quarter, h), ws[u].at[h, at, p], ls.at[2 + 2 * h + u])
        for h in range(parts) for u in (0, 1)
    ]
    own_x.start()
    own_c.start()
    for copy in own_w:
        copy.start()
    acc[...] = jnp.zeros_like(acc)

    n_near = n_tp + 1
    inner = has_up & has_down

    @pl.when(inner)
    def _():
        pl.semaphore_wait(barrier, n_near + 2)

    @pl.when(jnp.logical_not(inner))
    def _():
        pl.semaphore_wait(barrier, n_near + 1 if line > 1 else n_near)

    y_copies = [
        remote(own_block(u, 2 * r + 1 - p, h), ws[u].at[h, at, p], ys.at[h, u], yr.at[h, u], to_y)
        for h in range(parts) for u in (0, 1)
    ]

    def y_arrival(u, h):
        blk = ws[u].at[h, at, 1 - p]
        return remote(blk, blk, ys.at[h, u], yr.at[h, u], to_y)

    for copy in y_copies:
        copy.start()

    def z_copy(go_up, h, s, j):
        u, own_pair = j % 2, j < 2
        lvl = at - s if go_up else at + s
        blk = ws[u].at[h, lvl, p if own_pair else 1 - p]
        src = own_block(u, quarter, h) if (s == 0 and own_pair) else blk
        d = 0 if go_up else 1
        return remote(src, blk, zs.at[d, h, s, j], zr.at[d, h, s, j], up if go_up else down)

    def z_valid(go_up, s):
        return ((at - s >= 0) & has_up) if go_up else ((at + s < line) & has_down)

    def z_step(h, s, j):
        for go_up in (True, False):
            d = 0 if go_up else 1
            if s > 0:
                lvl = at - s if go_up else at + s

                @pl.when((lvl >= 0) & (lvl < line))
                def _():
                    blk = ws[j % 2].at[h, lvl, p if j < 2 else 1 - p]
                    remote(blk, blk, zs.at[d, h, s - 1, j], zr.at[d, h, s - 1, j], to_x).wait_recv()
            if s < line - 1:
                @pl.when(z_valid(go_up, s))
                def _():
                    z_copy(go_up, h, s, j).start()

    z_step(0, 0, 0)
    z_step(0, 0, 1)

    own = (x_in, c_in)
    first = {}
    for slot, dev in ((1, to_x), (2, to_y)):
        for a in (0, 1):
            first[slot, a] = remote(
                own[a].at[mine], xs.at[a, slot, mine], ts.at[slot - 1, a], tr.at[slot - 1, a], dev
            )
    first[1, 0].start()
    first[2, 1].start()
    first[1, 1].start()
    first[2, 0].start()
    most = half // 48 * 32
    base = pl.multiple_of(core * half, half)
    lead, rest = pl.ds(base, most), pl.ds(base + most, half - most)
    diag = [
        remote(xs.at[0, 1, lead], xs.at[0, 3, lead], ts.at[2, 0], tr.at[2, 0], to_y),
        remote(xs.at[1, 2, mine], xs.at[1, 3, mine], ts.at[2, 1], tr.at[2, 1], to_x),
        remote(xs.at[0, 2, rest], xs.at[0, 3, rest], ts.at[3, 0], tr.at[3, 0], to_x),
    ]

    def swap(slot, a):
        return remote(
            xs.at[a, slot, mine], xs.at[a, slot, mine], cs.at[slot - 1, a], cr.at[slot - 1, a], to_core
        )

    def swapped(slot, a):
        blk = xs.at[a, slot, theirs]
        remote(blk, blk, cs.at[slot - 1, a], cr.at[slot - 1, a], to_core).wait_recv()

    def unit(u, h, slot, lvl):
        if u == 1 and native:
            total = acc[h, u, slot]
            for b in (0, 1):
                span = pl.ds(pl.multiple_of(lvl * level + b * rows, rows), rows)
                total = total + dot(xs[u, slot, :, span], wd[h, lvl, b], 1, 1)
            acc[h, u, slot] = total
        else:
            span = pl.ds(pl.multiple_of(lvl * level, level), level)
            acc[h, u, slot] += dot(xs[u, slot, :, span], ws[u][h, lvl].reshape(level, cols), 1, 0)

    done = [[-1, -1] for _ in range(parts)]
    ready = [1, 1]

    def grow_slot(u, h, s, slot):
        for lvl in (at - s, at + s):
            @pl.when((lvl >= 0) & (lvl < line))
            def _():
                unit(u, h, slot, lvl)

    def grow(u, h, s):
        done[h][u] = s
        n = ready[u]
        if s == 0:
            def body(slot, _):
                unit(u, h, slot, at)
                return 0

            lax.fori_loop(0, n, body, 0)
            return

        def body(i, _):
            lvl = at + s - 2 * s * lax.rem(i, 2)

            @pl.when((lvl >= 0) & (lvl < line))
            def _():
                unit(u, h, lax.div(i, 2), lvl)
            return 0

        lax.fori_loop(0, 2 * n, body, 0)

    def join(slot, u, halves):
        for h in halves:
            lo, hi = jnp.maximum(at - done[h][u], 0), jnp.minimum(at + done[h][u], line - 1)

            def body(lvl, _):
                unit(u, h, slot, lvl)
                return 0

            lax.fori_loop(lo, hi + 1, body, 0)

    def make_g(h, slot):
        g[h, slot] = (2.0 * jnp.maximum(acc[h, 0, slot], 0.0) * acc[h, 1, slot]).astype(BF16)

    low = at < line - at - 1

    turns = (1 - p, p)

    def o_copy(go_up, h, o, k):
        d, b = 0 if go_up else 1, turns[k]
        return remote(
            dw.at[h, o, b], zin.at[d, h, o, b], os.at[d, h, o, k], orr.at[d, h, o, k], up if go_up else down
        )

    def make_dw(h, i):
        o = jnp.where(low, line - 1 - i, i)
        span = pl.ds(pl.multiple_of(o * level, level), level)
        lhs = xs[0, :, :, span].reshape(4 * tokens, level)
        value = dot(lhs, g[h].reshape(4 * tokens, cols), 0, 0)
        dw[h, o] = value.astype(BF16).reshape(2, rows, cols)
        if i < line - 1:
            @pl.when(at == 0)
            def _():
                for k in (0, 1):
                    o_copy(True, h, line - 1 - i, k).start()

            @pl.when(at == line - 1)
            def _():
                for k in (0, 1):
                    o_copy(False, h, i, k).start()

    part = tokens // n_tp

    def start_part(slot):
        def body(lvl, _):
            span = pl.ds(pl.multiple_of(lvl * level, level), level)
            value = dot(g[0, slot], wu[0, lvl].reshape(level, cols), 1, 1)
            ahead[:, :, span] = value.reshape(n_tp, part, level)
            return 0

        lax.fori_loop(0, line, body, 0)

    own_x.wait()
    own_c.wait()
    for copy in own_w:
        copy.wait()

    def own_level(h):
        for u in (0, 1):
            y_arrival(u, h).wait_recv()
            z_step(h, 0, 2 + u)
        for u in (0, 1):
            grow(u, h, 0)

    own_level(0)

    def got(slot, a):
        def run():
            if slot < 3:
                first[slot, a].wait_recv()
                if (slot, a) == (1, 0):
                    diag[0].start()
                if (slot, a) == (2, 1):
                    diag[1].start()
                if (slot, a) == (2, 0):
                    diag[2].start()
            else:
                diag[a].wait_recv()
                if a == 0:
                    diag[2].wait_recv()
            swap(slot, a).start()
        return run

    def use(slot, a):
        def run():
            swapped(slot, a)
            ready[a] += 1
            join(slot, a, range(parts))
        return run

    def early():
        swapped(3, 0)
        ready[0] += 1
        for h in range(final):
            join(3, 0, [h])

            def body(slot, _):
                make_g(h, slot)
                return 0

            lax.fori_loop(0, 4, body, 0)
            for i in range(line):
                make_dw(h, i)
        join(3, 0, [final])
        if parts > 1:
            start_part(3)

    if parts == 2:
        hooks = {
            (0, 2, 1): [got(1, 0)],
            (0, 2, 3): [use(1, 0)],
            (1, 1, 1): [got(2, 1)],
            (1, 1, 3): [use(2, 1), got(1, 1)],
            (0, 3, 0): [use(1, 1)],
            (0, 3, 3): [got(2, 0)],
            (1, 2, 0): [use(2, 0)],
            (1, 2, 1): [got(3, 1)],
            (1, 2, 2): [use(3, 1), got(3, 0)],
            (1, 2, 3): [early],
        }
        steps = [(0, 1)]
        for s in range(2, line):
            steps += [(0, s), (1, s - 1)]
        steps += [(1, line - 1)]
    else:
        hooks = {
            (0, 1, 2): [got(1, 0)],
            (0, 1, 3): [use(1, 0)],
            (0, 2, 0): [got(2, 1)],
            (0, 2, 1): [got(1, 1), use(2, 1)],
            (0, 2, 2): [use(1, 1)],
            (0, 2, 3): [got(2, 0)],
            (0, 3, 0): [use(2, 0), got(3, 1)],
            (0, 3, 1): [use(3, 1)],
            (0, 3, 2): [got(3, 0)],
            (0, 3, 3): [early],
        }
        steps = [(0, s) for s in range(1, line)]
    for h, s in steps:
        for j in range(4):
            z_step(h, s, j)
            if j >= 2 and (h, s, j) != (final, line - 1, 3):
                grow(j - 2, h, s)
            for run in hooks.pop((h, s, j), []):
                run()
        if (h, s) == (0, 1):
            for k in range(1, parts):
                z_step(k, 0, 0)
                z_step(k, 0, 1)
                own_level(k)
    for key in list(hooks):
        for run in hooks[key]:
            run()

    def p_copy(slot, k):
        there = lax.rem(c + k, n_tp)
        return remote(
            part_.at[slot, there], tpin.at[k - 1, slot], ps.at[k - 1, slot], pr.at[k - 1, slot], {"tp": there}
        )

    def make_part(slot):
        def body(lvl, _):
            span = pl.ds(pl.multiple_of(lvl * level, level), level)
            value = dot(g[0, slot], wu[0, lvl].reshape(level, cols), 1, 1)
            for h in range(1, parts):
                value = value + dot(g[h, slot], wu[h, lvl].reshape(level, cols), 1, 1)
            part_[slot, :, :, span] = value.astype(BF16).reshape(n_tp, part, level)
            return 0

        lax.fori_loop(0, line, body, 0)
        for k in range(1, n_tp):
            p_copy(slot, k).start()

    def end_part(slot):
        for k in list(range(1, n_tp)) + [0]:
            there = lax.rem(c + k, n_tp)
            tok = pl.ds(pl.multiple_of(there * part, part), part)

            def body(lvl, _):
                span = pl.ds(pl.multiple_of(lvl * level, level), level)
                value = ahead[there, :, span] + dot(g[1, slot, tok], wu[1, lvl].reshape(level, cols), 1, 1)
                part_[slot, there, :, span] = value.astype(BF16)
                return 0

            lax.fori_loop(0, line, body, 0)
            if k > 0:
                p_copy(slot, k).start()

    def tp_sum(slot):
        for k in range(1, n_tp):
            p_copy(slot, k).wait_recv()
        total = part_[slot, c].astype(F32)
        for k in range(1, n_tp):
            total = total + tpin[k - 1, slot].astype(F32)
        return total

    cut = width * 3 // 8 // 128 * 128
    early_cut = cut // 256 * 128
    left, right = pl.ds(0, cut), pl.ds(cut, width - cut)
    left_a, left_b = pl.ds(0, early_cut), pl.ds(early_cut, cut - early_cut)
    q_copies = {
        "x3": remote(part_.at[3, c, :, left], q1.at[1, :, left], qs.at[0], qr.at[0], to_x),
        "y3": remote(part_.at[3, c, :, right], q1.at[1, :, right], qs.at[1], qr.at[1], to_y),
        "x1": remote(part_.at[1, c, :, left], q1.at[0, :, left], qs.at[2], qr.at[2], to_x),
        "y2": remote(part_.at[2, c, :, right], q1.at[0, :, right], qs.at[3], qr.at[3], to_y),
        "y2a": remote(part_.at[2, c, :, left_a], q2.at[:, left_a], qs.at[4], qr.at[4], to_y),
        "y2b": remote(part_.at[2, c, :, left_b], q2.at[:, left_b], qs.at[6], qr.at[6], to_y),
        "x1r": remote(part_.at[1, c, :, right], q2.at[:, right], qs.at[5], qr.at[5], to_x),
    }

    def store_sum(slot):
        part_[slot, c] = tp_sum(slot).astype(BF16)

    def o_step(h, t, k):
        b = turns[k]
        for go_up in (True, False):
            d = 0 if go_up else 1
            gap = at if go_up else line - 1 - at
            o = (line - 1 - t + at) if go_up else (t - line + 1 + at)

            @pl.when((gap > 0) & (gap <= t))
            def _():
                o_copy(go_up, h, o, k).wait_recv()
                if t < line - 1:
                    dw[h, o, b] = (dw[h, o, b].astype(F32) + zin[d, h, o, b].astype(F32)).astype(BF16)
                    o_copy(go_up, h, o, k).start()

    half_rows = [pl.ds(i * (rows // 2), rows // 2) for i in (0, 1)]

    def dw_at(q, h, span=slice(None)):
        return dw_out.at[span, pl.ds(pl.multiple_of((q * parts + h) * cols, cols), cols)]

    def e_y(h, i):
        here = dw_at(quarter, h, half_rows[i])
        return remote(fin.at[h, 1 - p, half_rows[i]], here, es.at[1, h, i], er.at[1, h, i], to_y)

    def e_relay(h, i):
        here = dw_at(2 * r + 1 - p, h, half_rows[i])
        return remote(here, here, es.at[2, h, i], er.at[2, h, i], to_x)

    def e_x(h):
        return remote(fin.at[h, p], dw_at(quarter, h), es.at[0, h, 0], er.at[0, h, 0], to_x)

    def e_own(h):
        return pltpu.make_async_copy(fin.at[h, p], dw_at(quarter, h), el.at[h])

    def finish(h, k):
        b = turns[k]
        for d, there in ((0, has_down), (1, has_up)):
            @pl.when(there & jnp.logical_not(has_up & has_down))
            def _():
                fin[h, b] = (dw[h, at, b].astype(F32) + zin[d, h, at, b].astype(F32)).astype(BF16)

        @pl.when(has_up & has_down)
        def _():
            total = dw[h, at, b].astype(F32) + zin[0, h, at, b].astype(F32) + zin[1, h, at, b].astype(F32)
            fin[h, b] = total.astype(BF16)

        if line == 1:
            fin[h, b] = dw[h, at, b]
        if k == 0:
            e_y(h, 0).start()
            e_y(h, 1).start()
        else:
            e_x(h).start()
            e_own(h).start()

    def relay(h):
        for i in (0, 1):
            blk = dw_at(2 * r + 1 - p, h, half_rows[i])
            remote(blk, blk, es.at[1, h, i], er.at[1, h, i], to_y).wait_recv()
            e_relay(h, i).start()

    def in_x3():
        q_copies["x3"].wait_recv()
        part_[2, c, :, left] = (part_[2, c, :, left].astype(F32) + q1[1, :, left].astype(F32)).astype(BF16)

    def in_y3():
        q_copies["y3"].wait_recv()
        part_[1, c, :, right] = (part_[1, c, :, right].astype(F32) + q1[1, :, right].astype(F32)).astype(BF16)

    segments = ((right, ("y2", "x1r")), (left_a, ("x1", "y2a")), (left_b, ("y2b",)))

    def out_own(i):
        span = segments[i][0]
        return pltpu.make_async_copy(fo.at[:, span], din_out.at[c, :, span], dl.at[i])

    def out_peer(i, k):
        span = segments[i][0]
        return remote(
            fo.at[:, span], din_out.at[c, :, span], ds.at[k - 1, i], dr.at[k - 1, i], {"tp": lax.rem(c + k, n_tp)}
        )

    def in_last(i):
        span, names = segments[i]
        for name in names:
            q_copies[name].wait_recv()
        total = part_[0, c, :, span].astype(F32)
        for k in range(1, n_tp):
            total = total + tpin[k - 1, 0, :, span].astype(F32)
        fo[:, span] = (total + q1[0, :, span].astype(F32) + q2[:, span].astype(F32)).astype(BF16)
        out_own(i).start()
        for k in range(1, n_tp):
            out_peer(i, k).start()

    def last_rows(slot):
        if line > 1:
            grow_slot(1, final, line - 1, slot)
        make_g(final, slot)

    def send(*names):
        for name in names:
            q_copies[name].start()

    def sums(h, t, k):
        if 1 <= t < line:
            o_step(h, t, k)

    def weights(lo, hi):
        for i in range(lo, min(hi, line)):
            make_dw(final, i)

    def close(h):
        for k in (0, 1):
            sums(h, line - 1, k)
            finish(h, k)
            if (h, k) == (final, 0):
                send("y2b")

    split = parts > 1
    last_rows(3)
    if split:
        end_part(3)
    else:
        make_part(3)
    for slot in (1, 2, 0):
        last_rows(slot)
    store_sum(3)
    send("x3", "y3")
    if split:
        sums(0, 1, 0)
    make_part(1)
    if split:
        sums(0, 1, 1)
    weights(0, 1)
    make_part(2)
    store_sum(1)
    send("x1")
    if split:
        sums(0, 2, 0)
    weights(1, 2)
    make_part(0)
    store_sum(2)
    send("y2")
    if split:
        sums(0, 2, 1)
    weights(2, line)
    for t in range(3 if split else 1, line - 1):
        for k in (0, 1):
            sums(0, t, k)
    if split:
        close(0)
    in_x3()
    send("y2a")
    in_y3()
    send("x1r")
    if not split:
        close(0)
    for h in range(1, parts):
        for t in range(1, line - 1):
            for k in (0, 1):
                sums(h, t, k)
        relay(h - 1)
        close(h)
    for k in range(1, n_tp):
        p_copy(0, k).wait_recv()
    in_last(0)
    in_last(1)
    relay(final)
    in_last(2)

    for i in range(3):
        out_own(i).wait()
        for k in range(1, n_tp):
            out_peer(i, k).wait_recv()
            out_peer(i, k).wait_send()
    for h in range(parts):
        blk = dw_at(2 * (1 - r) + p, h)
        remote(blk, blk, es.at[0, h, 0], er.at[0, h, 0], to_x).wait_recv()
        for i in (0, 1):
            blk = dw_at(2 * (1 - r) + 1 - p, h, half_rows[i])
            remote(blk, blk, es.at[2, h, i], er.at[2, h, i], to_x).wait_recv()
    for copy in q_copies.values():
        copy.wait_send()
    for h in range(parts):
        e_own(h).wait()
        e_x(h).wait_send()
        for i in (0, 1):
            e_y(h, i).wait_send()
            e_relay(h, i).wait_send()
    for slot in range(4):
        for k in range(1, n_tp):
            p_copy(slot, k).wait_send()
    for h in range(parts):
        for o in range(line):
            @pl.when((at < o) & has_up)
            def _():
                for k in (0, 1):
                    o_copy(True, h, o, k).wait_send()

            @pl.when((at > o) & has_down)
            def _():
                for k in (0, 1):
                    o_copy(False, h, o, k).wait_send()
    for slot in (1, 2, 3):
        for a in (0, 1):
            swap(slot, a).wait_send()
    for copy in list(first.values()) + diag + y_copies:
        copy.wait_send()
    for h in range(parts):
        for s in range(line - 1):
            for j in range(4):
                for go_up in (True, False):
                    @pl.when(z_valid(go_up, s))
                    def _():
                        z_copy(go_up, h, s, j).wait_send()


def fused(n_fs, n_tp, n_rep, x, c, w_up, w_down):
    line = n_fs // 2
    tokens, width = x.shape
    rows, block = w_up.shape
    cols = block // (2 * n_rep)
    parts = 2 if cols % 256 == 0 and n_fs > 4 else 1
    cols = cols // parts
    native = rows % 128 == 0
    if not native:
        w_down = w_down.T
    part = tokens // n_tp
    dma = pltpu.SemaphoreType.DMA
    hbm = pl.BlockSpec(memory_space=pl.ANY)
    vmem = lambda *shape: pltpu.VMEM(shape, BF16)
    down_block = (cols, rows) if native else (rows, cols)
    others = max(n_tp - 1, 1)
    return pl.pallas_call(
        functools.partial(kernel, line, n_tp, native, parts),
        out_shape=(
            jax.ShapeDtypeStruct((rows, block), BF16),
            jax.ShapeDtypeStruct((n_tp, part, width), BF16),
        ),
        in_specs=[hbm] * 4,
        out_specs=(hbm,) * 2,
        scratch_shapes=[
            vmem(2, 4, tokens, width),
            vmem(parts, line, 2, rows, cols),
            vmem(parts, line, 2, *down_block),
            pltpu.VMEM((parts, 2, 4, tokens, cols), F32),
            vmem(parts, 4, tokens, cols),
            vmem(parts, line, 2, rows, cols),
            vmem(2, parts, line, 2, rows, cols),
            vmem(parts, 2, rows, cols),
            vmem(4, n_tp, part, width),
            vmem(others, 4, part, width),
            vmem(2, part, width),
            vmem(part, width),
            vmem(part, width),
            pltpu.VMEM((n_tp, part, width) if parts > 1 else (1, 8, 128), F32),
            dma((2, parts, line, 4)), dma((2, parts, line, 4)), dma((parts, 2)), dma((parts, 2)),
            dma((4, 2)), dma((4, 2)), dma((3, 2)), dma((3, 2)), dma((2 + 2 * parts,)),
            dma((2, parts, line, 2)), dma((2, parts, line, 2)),
            dma((4, parts, 2)), dma((4, parts, 2)), dma((parts,)),
            dma((others, 4)), dma((others, 4)), dma((7,)), dma((7,)),
            dma((others, 3)), dma((others, 3)), dma((3,)),
        ],
        compiler_params=pltpu.CompilerParams(
            collective_id=0, has_side_effects=True, vmem_limit_bytes=52 * 2**20
        ),
        name="fused",
    )(x, c, w_up, w_down)


def per_device(inputs, w_up, w_down, cotangent):
    n_rep, n_fs, n_tp = lax.axis_size("rep"), lax.axis_size("fs"), lax.axis_size("tp")
    d_w, d_in = fused(n_fs, n_tp, n_rep, inputs, cotangent, w_up, w_down)
    return d_in.reshape(inputs.shape), d_w.astype(F32)


def solution(mesh):
    in_specs = (P(("rep", "fs"), None), P("fs", "tp"), P("tp", "fs"), P(("rep", "fs"), None))
    out_specs = (P(("rep", "fs"), None), P("fs", "tp"))
    return jax.shard_map(
        per_device, mesh=mesh, in_specs=in_specs, out_specs=out_specs, check_vma=False
    )
```

```python
import functools

import jax
import jax.numpy as jnp
from jax import lax
from jax.experimental import pallas as pl
from jax.experimental.pallas import tpu as pltpu
from jax.sharding import PartitionSpec as P

MESH = pl.DeviceIdType.MESH
F32, BF16 = jnp.float32, jnp.bfloat16


def dot(a, b, da, db):
    return lax.dot_general(a, b, (((da,), (db,)), ((), ())), preferred_element_type=F32)


def kernel(line, n_tp, native, parts, x_in, c_in, up_in, down_in, dw_out, din_out,
           xs, wu, wd, acc, g, dw, zin, fin, part_, tpin, q1, q2, fo, ahead,
           zs, zr, ys, yr, ts, tr, cs, cr, ls, os, orr, es, er, el, ps, pr, qs, qr, ds, dr, dl):
    r, f, c = lax.axis_index("rep"), lax.axis_index("fs"), lax.axis_index("tp")
    p, at = lax.rem(f, 2), lax.div(f, 2)
    core = lax.rem(c, 2)
    to_x, to_y = {"rep": 1 - r}, {"fs": f + 1 - 2 * p}
    to_core = {"tp": c + 1 - 2 * core}
    up, down = {"fs": f + 2}, {"fs": f - 2}
    has_up, has_down = at < line - 1, at > 0
    tokens, width = x_in.shape
    rows, cols = wu.shape[3:]
    level = 2 * rows
    final = parts - 1
    quarter = 2 * r + p

    barrier = pltpu.get_barrier_semaphore()
    peers = [{"tp": lax.rem(c + k, n_tp)} for k in range(1, n_tp)]
    for dev in [to_x, to_y] + peers:
        pl.semaphore_signal(barrier, inc=1, device_id=dev, device_id_type=MESH)

    @pl.when(has_up)
    def _():
        pl.semaphore_signal(barrier, inc=1, device_id=up, device_id_type=MESH)

    @pl.when(has_down)
    def _():
        pl.semaphore_signal(barrier, inc=1, device_id=down, device_id_type=MESH)

    def remote(src, dst, send, recv, dev):
        return pltpu.make_async_remote_copy(
            src_ref=src, dst_ref=dst, send_sem=send, recv_sem=recv, device_id=dev, device_id_type=MESH
        )

    half = tokens // 2
    mine = pl.ds(pl.multiple_of(core * half, half), half)
    theirs = pl.ds(pl.multiple_of((1 - core) * half, half), half)
    ws = (wu, wd)

    def own_block(u, q, h):
        span = pl.ds(pl.multiple_of((q * parts + h) * cols, cols), cols)
        if u == 1 and native:
            return down_in.at[span, :]
        return (up_in, down_in)[u].at[:, span]

    own_x = pltpu.make_async_copy(x_in, xs.at[0, 0], ls.at[0])
    own_c = pltpu.make_async_copy(c_in, xs.at[1, 0], ls.at[0])
    own_w = [
        pltpu.make_async_copy(own_block(u, quarter, h), ws[u].at[h, at, p], ls.at[1])
        for h in range(parts) for u in (0, 1)
    ]
    own_x.start()
    own_c.start()
    for copy in own_w:
        copy.start()
    acc[...] = jnp.zeros_like(acc)

    n_near = n_tp + 1
    inner = has_up & has_down

    @pl.when(inner)
    def _():
        pl.semaphore_wait(barrier, n_near + 2)

    @pl.when(jnp.logical_not(inner))
    def _():
        pl.semaphore_wait(barrier, n_near + 1 if line > 1 else n_near)

    y_copies = [
        remote(own_block(u, 2 * r + 1 - p, h), ws[u].at[h, at, p], ys.at[0], yr.at[h, u], to_y)
        for h in range(parts) for u in (0, 1)
    ]

    def y_arrival(u, h):
        blk = ws[u].at[h, at, 1 - p]
        return remote(blk, blk, ys.at[0], yr.at[h, u], to_y)

    for copy in y_copies:
        copy.start()

    def z_copy(go_up, h, s, j):
        u, own_pair = j % 2, j < 2
        lvl = at - s if go_up else at + s
        blk = ws[u].at[h, lvl, p if own_pair else 1 - p]
        src = own_block(u, quarter, h) if (s == 0 and own_pair) else blk
        d = 0 if go_up else 1
        return remote(src, blk, zs.at[d, u], zr.at[h, lvl, j], up if go_up else down)

    def z_valid(go_up, s):
        return ((at - s >= 0) & has_up) if go_up else ((at + s < line) & has_down)

    def z_step(h, s, j):
        for go_up in (True, False):
            d = 0 if go_up else 1
            if s > 0:
                lvl = at - s if go_up else at + s

                @pl.when((lvl >= 0) & (lvl < line))
                def _():
                    blk = ws[j % 2].at[h, lvl, p if j < 2 else 1 - p]
                    remote(blk, blk, zs.at[d, j % 2], zr.at[h, lvl, j], to_x).wait_recv()
            if s < line - 1:
                @pl.when(z_valid(go_up, s))
                def _():
                    z_copy(go_up, h, s, j).start()

    z_step(0, 0, 0)
    z_step(0, 0, 1)

    own = (x_in, c_in)
    first = {}
    for slot, dev in ((1, to_x), (2, to_y)):
        for a in (0, 1):
            first[slot, a] = remote(
                own[a].at[mine], xs.at[a, slot, mine], ts.at[0], tr.at[slot - 1, a], dev
            )
    first[1, 0].start()
    first[2, 1].start()
    first[1, 1].start()
    first[2, 0].start()
    most = half // 48 * 32
    base = pl.multiple_of(core * half, half)
    lead, rest = pl.ds(base, most), pl.ds(base + most, half - most)
    diag = [
        remote(xs.at[0, 1, lead], xs.at[0, 3, lead], ts.at[0], tr.at[2, 0], to_y),
        remote(xs.at[1, 2, mine], xs.at[1, 3, mine], ts.at[0], tr.at[2, 1], to_x),
        remote(xs.at[0, 2, rest], xs.at[0, 3, rest], ts.at[0], tr.at[3, 0], to_x),
    ]

    def swap(slot, a):
        return remote(
            xs.at[a, slot, mine], xs.at[a, slot, mine], cs.at[0], cr.at[slot - 1, a], to_core
        )

    def swapped(slot, a):
        blk = xs.at[a, slot, theirs]
        remote(blk, blk, cs.at[0], cr.at[slot - 1, a], to_core).wait_recv()

    def unit(u, h, slot, lvl):
        if u == 1 and native:
            total = acc[h, u, slot]
            for b in (0, 1):
                span = pl.ds(pl.multiple_of(lvl * level + b * rows, rows), rows)
                total = total + dot(xs[u, slot, :, span], wd[h, lvl, b], 1, 1)
            acc[h, u, slot] = total
        else:
            span = pl.ds(pl.multiple_of(lvl * level, level), level)
            acc[h, u, slot] += dot(xs[u, slot, :, span], ws[u][h, lvl].reshape(level, cols), 1, 0)

    done = [[-1, -1] for _ in range(parts)]
    ready = [1, 1]

    def grow_slot(u, h, s, slot):
        for lvl in (at - s, at + s):
            @pl.when((lvl >= 0) & (lvl < line))
            def _():
                unit(u, h, slot, lvl)

    def grow(u, h, s):
        done[h][u] = s
        n = ready[u]
        if s == 0:
            def body(slot, _):
                unit(u, h, slot, at)
                return 0

            lax.fori_loop(0, n, body, 0)
            return

        def body(i, _):
            lvl = at + s - 2 * s * lax.rem(i, 2)

            @pl.when((lvl >= 0) & (lvl < line))
            def _():
                unit(u, h, lax.div(i, 2), lvl)
            return 0

        lax.fori_loop(0, 2 * n, body, 0)

    def join(slot, u, halves):
        for h in halves:
            lo, hi = jnp.maximum(at - done[h][u], 0), jnp.minimum(at + done[h][u], line - 1)

            def body(lvl, _):
                unit(u, h, slot, lvl)
                return 0

            lax.fori_loop(lo, hi + 1, body, 0)

    def make_g(h, slot):
        g[h, slot] = (2.0 * jnp.maximum(acc[h, 0, slot], 0.0) * acc[h, 1, slot]).astype(BF16)

    low = at < line - at - 1

    turns = (1 - p, p)

    def o_copy(go_up, h, o, k, here=None):
        def o_last(o):
            return jnp.where(o == (at - 1 if here is None else at), line, o)

        d, b = 0 if go_up else 1, turns[k]
        return remote(
            dw.at[h, o, b], zin.at[d, h, o, b], os.at[d], orr.at[h, o, k] if go_up else orr.at[h, o_last(o), k],
            up if go_up else down,
        )

    def make_dw(h, i):
        o = jnp.where(low, line - 1 - i, i)
        span = pl.ds(pl.multiple_of(o * level, level), level)
        lhs = xs[0, :, :, span].reshape(4 * tokens, level)
        value = dot(lhs, g[h].reshape(4 * tokens, cols), 0, 0)
        dw[h, o] = value.astype(BF16).reshape(2, rows, cols)
        if i < line - 1:
            @pl.when(at == 0)
            def _():
                for k in (0, 1):
                    o_copy(True, h, line - 1 - i, k).start()

            @pl.when(at == line - 1)
            def _():
                for k in (0, 1):
                    o_copy(False, h, i, k).start()

    part = tokens // n_tp

    def start_part(slot):
        def body(lvl, _):
            span = pl.ds(pl.multiple_of(lvl * level, level), level)
            value = dot(g[0, slot], wu[0, lvl].reshape(level, cols), 1, 1)
            ahead[:, :, span] = value.reshape(n_tp, part, level)
            return 0

        lax.fori_loop(0, line, body, 0)

    both = xs.at[:, 0]
    pltpu.make_async_copy(both, both, ls.at[0]).wait()
    pltpu.make_async_copy(fin, fin, ls.at[1]).wait()

    def own_level(h):
        for u in (0, 1):
            y_arrival(u, h).wait_recv()
            z_step(h, 0, 2 + u)
        for u in (0, 1):
            grow(u, h, 0)

    own_level(0)

    def got(slot, a):
        def run():
            if slot < 3:
                first[slot, a].wait_recv()
                if (slot, a) == (1, 0):
                    diag[0].start()
                if (slot, a) == (2, 1):
                    diag[1].start()
                if (slot, a) == (2, 0):
                    diag[2].start()
            else:
                diag[a].wait_recv()
                if a == 0:
                    diag[2].wait_recv()
            swap(slot, a).start()
        return run

    def use(slot, a):
        def run():
            swapped(slot, a)
            ready[a] += 1
            join(slot, a, range(parts))
        return run

    def early():
        swapped(3, 0)
        ready[0] += 1
        for h in range(final):
            join(3, 0, [h])

            def body(slot, _):
                make_g(h, slot)
                return 0

            lax.fori_loop(0, 4, body, 0)
            for i in range(line):
                make_dw(h, i)
        join(3, 0, [final])
        if parts > 1:
            start_part(3)

    if parts == 2:
        hooks = {
            (0, 2, 1): [got(1, 0)],
            (0, 2, 3): [use(1, 0)],
            (1, 1, 1): [got(2, 1)],
            (1, 1, 3): [use(2, 1), got(1, 1)],
            (0, 3, 0): [use(1, 1)],
            (0, 3, 3): [got(2, 0)],
            (1, 2, 0): [use(2, 0)],
            (1, 2, 1): [got(3, 1)],
            (1, 2, 2): [use(3, 1), got(3, 0)],
            (1, 2, 3): [early],
        }
        steps = [(0, 1)]
        for s in range(2, line):
            steps += [(0, s), (1, s - 1)]
        steps += [(1, line - 1)]
    else:
        hooks = {
            (0, 1, 2): [got(1, 0)],
            (0, 1, 3): [use(1, 0)],
            (0, 2, 0): [got(2, 1)],
            (0, 2, 1): [got(1, 1), use(2, 1)],
            (0, 2, 2): [use(1, 1)],
            (0, 2, 3): [got(2, 0)],
            (0, 3, 0): [use(2, 0), got(3, 1)],
            (0, 3, 1): [use(3, 1)],
            (0, 3, 2): [got(3, 0)],
            (0, 3, 3): [early],
        }
        steps = [(0, s) for s in range(1, line)]
    for h, s in steps:
        for j in range(4):
            z_step(h, s, j)
            if j >= 2 and (h, s, j) != (final, line - 1, 3):
                grow(j - 2, h, s)
            for run in hooks.pop((h, s, j), []):
                run()
        if (h, s) == (0, 1):
            for k in range(1, parts):
                z_step(k, 0, 0)
                z_step(k, 0, 1)
                own_level(k)
    for key in list(hooks):
        for run in hooks[key]:
            run()

    def p_copy(slot, k):
        there = lax.rem(c + k, n_tp)
        return remote(
            part_.at[slot, there], tpin.at[k - 1, slot], ps.at[0], pr.at[k - 1, slot], {"tp": there}
        )

    def make_part(slot):
        def body(lvl, _):
            span = pl.ds(pl.multiple_of(lvl * level, level), level)
            value = dot(g[0, slot], wu[0, lvl].reshape(level, cols), 1, 1)
            for h in range(1, parts):
                value = value + dot(g[h, slot], wu[h, lvl].reshape(level, cols), 1, 1)
            part_[slot, :, :, span] = value.astype(BF16).reshape(n_tp, part, level)
            return 0

        lax.fori_loop(0, line, body, 0)
        for k in range(1, n_tp):
            p_copy(slot, k).start()

    wide = line // 2 * level

    def e_part(slot, k, i):
        there = lax.rem(c + k, n_tp)
        span = (pl.ds(0, wide), pl.ds(wide, width - wide))[i]
        return remote(
            part_.at[slot, there, :, span], tpin.at[k - 1, slot, :, span],
            ps.at[0], pr.at[k - 1, 4 * i + slot], {"tp": there},
        )

    def end_part(slot):
        for i, (lo, hi) in enumerate(((0, line // 2), (line // 2, line))):
            def body(lvl, _):
                span = pl.ds(pl.multiple_of(lvl * level, level), level)
                value = dot(g[1, slot], wu[1, lvl].reshape(level, cols), 1, 1)
                part_[slot, :, :, span] = (ahead[:, :, span] + value.reshape(n_tp, part, level)).astype(BF16)
                return 0

            lax.fori_loop(lo, hi, body, 0)
            for k in range(1, n_tp):
                e_part(slot, k, i).start()

    def end_sum(slot, i):
        span = (pl.ds(0, wide), pl.ds(wide, width - wide))[i]
        total = part_[slot, c, :, span].astype(F32)
        for k in range(1, n_tp):
            e_part(slot, k, i).wait_recv()
            total = total + tpin[k - 1, slot, :, span].astype(F32)
        part_[slot, c, :, span] = total.astype(BF16)

    def tp_sum(slot):
        for k in range(1, n_tp):
            p_copy(slot, k).wait_recv()
        total = part_[slot, c].astype(F32)
        for k in range(1, n_tp):
            total = total + tpin[k - 1, slot].astype(F32)
        return total

    cut = width * 3 // 8 // 128 * 128
    early_cut = cut // 256 * 128
    left, right = pl.ds(0, cut), pl.ds(cut, width - cut)
    left_a, left_b = pl.ds(0, early_cut), pl.ds(early_cut, cut - early_cut)
    q_copies = {
        "x3": remote(part_.at[3, c, :, left], q1.at[1, :, left], qs.at[0], qr.at[0], to_x),
        "y3": remote(part_.at[3, c, :, right], q1.at[1, :, right], qs.at[0], qr.at[1], to_y),
        "x1": remote(part_.at[1, c, :, left], q1.at[0, :, left], qs.at[0], qr.at[2], to_x),
        "y2": remote(part_.at[2, c, :, right], q1.at[0, :, right], qs.at[0], qr.at[3], to_y),
        "y2a": remote(part_.at[2, c, :, left_a], q2.at[:, left_a], qs.at[0], qr.at[4], to_y),
        "y2b": remote(part_.at[2, c, :, left_b], q2.at[:, left_b], qs.at[0], qr.at[6], to_y),
        "x1r": remote(part_.at[1, c, :, right], q2.at[:, right], qs.at[0], qr.at[5], to_x),
    }

    def store_sum(slot):
        part_[slot, c] = tp_sum(slot).astype(BF16)

    def o_step(h, t, k):
        b = turns[k]
        for go_up in (True, False):
            d = 0 if go_up else 1
            gap = at if go_up else line - 1 - at
            o = (line - 1 - t + at) if go_up else (t - line + 1 + at)

            @pl.when((gap > 0) & (gap <= t))
            def _():
                o_copy(go_up, h, o, k, True).wait_recv()
                if t < line - 1:
                    dw[h, o, b] = (dw[h, o, b].astype(F32) + zin[d, h, o, b].astype(F32)).astype(BF16)
                    o_copy(go_up, h, o, k).start()

    half_rows = [pl.ds(i * (rows // 2), rows // 2) for i in (0, 1)]

    def dw_at(q, h, span=slice(None)):
        return dw_out.at[span, pl.ds(pl.multiple_of((q * parts + h) * cols, cols), cols)]

    def e_y(h, i):
        here = dw_at(quarter, h, half_rows[i])
        return remote(fin.at[h, 1 - p, half_rows[i]], here, es.at[1], er.at[1 + i, h], to_y)

    def e_relay(h, i):
        here = dw_at(2 * r + 1 - p, h, half_rows[i])
        return remote(here, here, es.at[2], er.at[3 + i, h], to_x)

    def e_x(h):
        return remote(fin.at[h, p], dw_at(quarter, h), es.at[0], er.at[0, h], to_x)

    def e_own(h):
        return pltpu.make_async_copy(fin.at[h, p], dw_at(quarter, h), el.at[0])

    def finish(h, k):
        b = turns[k]
        for d, there in ((0, has_down), (1, has_up)):
            @pl.when(there & jnp.logical_not(has_up & has_down))
            def _():
                fin[h, b] = (dw[h, at, b].astype(F32) + zin[d, h, at, b].astype(F32)).astype(BF16)

        @pl.when(has_up & has_down)
        def _():
            total = dw[h, at, b].astype(F32) + zin[0, h, at, b].astype(F32) + zin[1, h, at, b].astype(F32)
            fin[h, b] = total.astype(BF16)

        if line == 1:
            fin[h, b] = dw[h, at, b]
        if k == 0:
            e_y(h, 0).start()
            e_y(h, 1).start()
        else:
            e_x(h).start()
            e_own(h).start()

    def relay(h):
        for i in (0, 1):
            blk = dw_at(2 * r + 1 - p, h, half_rows[i])
            remote(blk, blk, es.at[1], er.at[1 + i, h], to_y).wait_recv()
            e_relay(h, i).start()

    def in_x3():
        q_copies["x3"].wait_recv()
        part_[2, c, :, left] = (part_[2, c, :, left].astype(F32) + q1[1, :, left].astype(F32)).astype(BF16)

    def in_y3():
        q_copies["y3"].wait_recv()
        part_[1, c, :, right] = (part_[1, c, :, right].astype(F32) + q1[1, :, right].astype(F32)).astype(BF16)

    segments = ((right, ("y2", "x1r")), (left_a, ("x1", "y2a")), (left_b, ("y2b",)))

    def out_own(i):
        span = segments[i][0]
        return pltpu.make_async_copy(fo.at[:, span], din_out.at[c, :, span], dl.at[0])

    def out_peer(i, k):
        span = segments[i][0]
        return remote(
            fo.at[:, span], din_out.at[c, :, span], ds.at[0], dr.at[k - 1, i], {"tp": lax.rem(c + k, n_tp)}
        )

    def in_last(i):
        span, names = segments[i]
        for name in names:
            q_copies[name].wait_recv()
        total = part_[0, c, :, span].astype(F32)
        for k in range(1, n_tp):
            total = total + tpin[k - 1, 0, :, span].astype(F32)
        fo[:, span] = (total + q1[0, :, span].astype(F32) + q2[:, span].astype(F32)).astype(BF16)
        out_own(i).start()
        for k in range(1, n_tp):
            out_peer(i, k).start()

    def last_rows(slot):
        if line > 1:
            grow_slot(1, final, line - 1, slot)
        make_g(final, slot)

    def send(*names):
        for name in names:
            q_copies[name].start()

    def sums(h, t, k):
        if 1 <= t < line:
            o_step(h, t, k)

    def weights(lo, hi):
        for i in range(lo, min(hi, line)):
            make_dw(final, i)

    def close(h):
        for k in (0, 1):
            sums(h, line - 1, k)
            finish(h, k)
            if (h, k) == (final, 0):
                send("y2b")

    split = parts > 1
    last_rows(3)
    if split:
        end_part(3)
    else:
        make_part(3)
    for slot in (1, 2, 0):
        last_rows(slot)
    if split:
        end_sum(3, 0)
        send("x3")
        end_sum(3, 1)
        send("y3")
    else:
        store_sum(3)
        send("x3", "y3")
    if split:
        sums(0, 1, 0)
    make_part(1)
    if split:
        sums(0, 1, 1)
    weights(0, 1)
    make_part(2)
    store_sum(1)
    send("x1")
    if split:
        sums(0, 2, 0)
    weights(1, 2)
    make_part(0)
    store_sum(2)
    send("y2")
    if split:
        sums(0, 2, 1)
    weights(2, line)
    for t in range(3 if split else 1, line - 1):
        for k in (0, 1):
            sums(0, t, k)
    if split:
        close(0)
    in_x3()
    send("y2a")
    in_y3()
    send("x1r")
    if not split:
        close(0)
    for h in range(1, parts):
        for t in range(1, line - 1):
            for k in (0, 1):
                sums(h, t, k)
        relay(h - 1)
        close(h)
    for k in range(1, n_tp):
        p_copy(0, k).wait_recv()
    in_last(0)
    in_last(1)
    relay(final)
    in_last(2)

    for i in range(3):
        for k in range(1, n_tp):
            out_peer(i, k).wait_recv()
    for h in range(parts):
        blk = dw_at(2 * (1 - r) + p, h)
        remote(blk, blk, es.at[0], er.at[0, h], to_x).wait_recv()
        for i in (0, 1):
            blk = dw_at(2 * (1 - r) + 1 - p, h, half_rows[i])
            remote(blk, blk, es.at[2], er.at[3 + i, h], to_x).wait_recv()

    def sent(ref, sem):
        pltpu.make_async_copy(ref, ref, sem).wait()

    sent(fo, dl.at[0])
    sent(fin.at[:, 0], el.at[0])
    for i in range(3):
        sent(fin.at[:, 0], es.at[i])
    sent(part_.at[pl.ds(0, 3), 0], qs.at[0])
    if n_tp > 1:
        sent(tpin, ps.at[0])
        sent(tpin.at[:, 0], ds.at[0])
    sent(xs.at[0, pl.ds(0, 3)], ts.at[0])
    sent(xs.at[0, pl.ds(0, 3)], cs.at[0])
    sent(fin, ys.at[0])
    for k in range(line):
        @pl.when((at == k) & has_up)
        def _():
            sent(dw.at[:, pl.ds(0, max(line - 1 - k, 1))], os.at[0])
            for u in (0, 1):
                sent(ws[u].at[:, pl.ds(0, k + 1)], zs.at[0, u])

        @pl.when((at == k) & has_down)
        def _():
            sent(dw.at[:, pl.ds(0, max(k, 1))], os.at[1])
            for u in (0, 1):
                sent(ws[u].at[:, pl.ds(0, line - k)], zs.at[1, u])


def fused(n_fs, n_tp, n_rep, x, c, w_up, w_down):
    line = n_fs // 2
    tokens, width = x.shape
    rows, block = w_up.shape
    cols = block // (2 * n_rep)
    parts = 2 if cols % 256 == 0 and n_fs > 4 else 1
    cols = cols // parts
    native = rows % 128 == 0
    if not native:
        w_down = w_down.T
    part = tokens // n_tp
    dma = pltpu.SemaphoreType.DMA
    hbm = pl.BlockSpec(memory_space=pl.ANY)
    vmem = lambda *shape: pltpu.VMEM(shape, BF16)
    down_block = (cols, rows) if native else (rows, cols)
    others = max(n_tp - 1, 1)
    return pl.pallas_call(
        functools.partial(kernel, line, n_tp, native, parts),
        out_shape=(
            jax.ShapeDtypeStruct((rows, block), BF16),
            jax.ShapeDtypeStruct((n_tp, part, width), BF16),
        ),
        in_specs=[hbm] * 4,
        out_specs=(hbm,) * 2,
        scratch_shapes=[
            vmem(2, 4, tokens, width),
            vmem(parts, line, 2, rows, cols),
            vmem(parts, line, 2, *down_block),
            pltpu.VMEM((parts, 2, 4, tokens, cols), F32),
            vmem(parts, 4, tokens, cols),
            vmem(parts, line, 2, rows, cols),
            vmem(2, parts, line, 2, rows, cols),
            vmem(parts, 2, rows, cols),
            vmem(4, n_tp, part, width),
            vmem(others, 4, part, width),
            vmem(2, part, width),
            vmem(part, width),
            vmem(part, width),
            pltpu.VMEM((n_tp, part, width) if parts > 1 else (1, 8, 128), F32),
            dma((2, 2)), dma((parts, line, 4)), dma((1,)), dma((parts, 2)),
            dma((1,)), dma((4, 2)), dma((1,)), dma((3, 2)), dma((2,)),
            dma((2,)), dma((parts, line + 1, 2)),
            dma((3,)), dma((5, parts)), dma((1,)),
            dma((1,)), dma((others, 8)), dma((1,)), dma((7,)),
            dma((1,)), dma((others, 3)), dma((1,)),
        ],
        compiler_params=pltpu.CompilerParams(
            collective_id=0, has_side_effects=True, vmem_limit_bytes=52 * 2**20
        ),
        name="fused",
    )(x, c, w_up, w_down)


def per_device(inputs, w_up, w_down, cotangent):
    n_rep, n_fs, n_tp = lax.axis_size("rep"), lax.axis_size("fs"), lax.axis_size("tp")
    d_w, d_in = fused(n_fs, n_tp, n_rep, inputs, cotangent, w_up, w_down)
    return d_in.reshape(inputs.shape), d_w.astype(F32)


def solution(mesh):
    in_specs = (P(("rep", "fs"), None), P("fs", "tp"), P("tp", "fs"), P(("rep", "fs"), None))
    out_specs = (P(("rep", "fs"), None), P("fs", "tp"))
    return jax.shard_map(
        per_device, mesh=mesh, in_specs=in_specs, out_specs=out_specs, check_vma=False
    )
```

```python
import functools

import jax
import jax.numpy as jnp
from jax import lax
from jax.experimental import pallas as pl
from jax.experimental.pallas import tpu as pltpu
from jax.sharding import PartitionSpec as P

MESH = pl.DeviceIdType.MESH
F32, BF16 = jnp.float32, jnp.bfloat16


def dot(a, b, da, db):
    return lax.dot_general(a, b, (((da,), (db,)), ((), ())), preferred_element_type=F32)


def kernel(line, n_tp, native, parts, x_in, c_in, up_in, down_in, dw_out, din_out,
           xs, wu, wd, acc, g, dw, zin, fin, part_, tpin, q1, q2, fo, ahead,
           zs, zr, ys, yr, ts, tr, cs, cr, ls, os, orr, es, er, el, ps, pr, qs, qr, ds, dr, dl):
    r, f, c = lax.axis_index("rep"), lax.axis_index("fs"), lax.axis_index("tp")
    p, at = lax.rem(f, 2), lax.div(f, 2)
    core = lax.rem(c, 2)
    to_x, to_y = {"rep": 1 - r}, {"fs": f + 1 - 2 * p}
    to_core = {"tp": c + 1 - 2 * core}
    up, down = {"fs": f + 2}, {"fs": f - 2}
    has_up, has_down = at < line - 1, at > 0
    tokens, width = x_in.shape
    rows, cols = wu.shape[3:]
    level = 2 * rows
    final = parts - 1
    quarter = 2 * r + p

    barrier = pltpu.get_barrier_semaphore()
    peers = [{"tp": lax.rem(c + k, n_tp)} for k in range(1, n_tp)]
    for dev in [to_x, to_y] + peers:
        pl.semaphore_signal(barrier, inc=1, device_id=dev, device_id_type=MESH)

    @pl.when(has_up)
    def _():
        pl.semaphore_signal(barrier, inc=1, device_id=up, device_id_type=MESH)

    @pl.when(has_down)
    def _():
        pl.semaphore_signal(barrier, inc=1, device_id=down, device_id_type=MESH)

    def remote(src, dst, send, recv, dev):
        return pltpu.make_async_remote_copy(
            src_ref=src, dst_ref=dst, send_sem=send, recv_sem=recv, device_id=dev, device_id_type=MESH
        )

    half = tokens // 2
    mine = pl.ds(pl.multiple_of(core * half, half), half)
    theirs = pl.ds(pl.multiple_of((1 - core) * half, half), half)
    ws = (wu, wd)

    def own_block(u, q, h):
        span = pl.ds(pl.multiple_of((q * parts + h) * cols, cols), cols)
        if u == 1 and native:
            return down_in.at[span, :]
        return (up_in, down_in)[u].at[:, span]

    own_x = pltpu.make_async_copy(x_in, xs.at[0, 0], ls.at[0])
    own_c = pltpu.make_async_copy(c_in, xs.at[1, 0], ls.at[0])
    own_w = [
        pltpu.make_async_copy(own_block(u, quarter, h), ws[u].at[h, at, p], ls.at[1])
        for h in range(parts) for u in (0, 1)
    ]
    own_x.start()
    own_c.start()
    for copy in own_w:
        copy.start()
    acc[...] = jnp.zeros_like(acc)

    n_near = n_tp + 1
    inner = has_up & has_down

    @pl.when(inner)
    def _():
        pl.semaphore_wait(barrier, n_near + 2)

    @pl.when(jnp.logical_not(inner))
    def _():
        pl.semaphore_wait(barrier, n_near + 1 if line > 1 else n_near)

    y_copies = [
        remote(own_block(u, 2 * r + 1 - p, h), ws[u].at[h, at, p], ys.at[0], yr.at[h, u], to_y)
        for h in range(parts) for u in (0, 1)
    ]

    def y_arrival(u, h):
        blk = ws[u].at[h, at, 1 - p]
        return remote(blk, blk, ys.at[0], yr.at[h, u], to_y)

    for copy in y_copies:
        copy.start()

    def z_copy(go_up, h, s, j):
        u, own_pair = j % 2, j < 2
        lvl = at - s if go_up else at + s
        blk = ws[u].at[h, lvl, p if own_pair else 1 - p]
        src = own_block(u, quarter, h) if (s == 0 and own_pair) else blk
        d = 0 if go_up else 1
        return remote(src, blk, zs.at[d, u], zr.at[h, lvl, j], up if go_up else down)

    def z_valid(go_up, s):
        return ((at - s >= 0) & has_up) if go_up else ((at + s < line) & has_down)

    def z_step(h, s, j):
        for go_up in (True, False):
            d = 0 if go_up else 1
            if s > 0:
                lvl = at - s if go_up else at + s

                @pl.when((lvl >= 0) & (lvl < line))
                def _():
                    blk = ws[j % 2].at[h, lvl, p if j < 2 else 1 - p]
                    remote(blk, blk, zs.at[d, j % 2], zr.at[h, lvl, j], to_x).wait_recv()
            if s < line - 1:
                @pl.when(z_valid(go_up, s))
                def _():
                    z_copy(go_up, h, s, j).start()

    z_step(0, 0, 0)
    z_step(0, 0, 1)

    own = (x_in, c_in)
    first = {}
    for slot, dev in ((1, to_x), (2, to_y)):
        for a in (0, 1):
            first[slot, a] = remote(
                own[a].at[mine], xs.at[a, slot, mine], ts.at[0], tr.at[slot - 1, a], dev
            )
    first[1, 0].start()
    first[2, 1].start()
    first[1, 1].start()
    first[2, 0].start()
    most = half // 48 * 32
    base = pl.multiple_of(core * half, half)
    lead, rest = pl.ds(base, most), pl.ds(base + most, half - most)
    diag = [
        remote(xs.at[0, 1, lead], xs.at[0, 3, lead], ts.at[0], tr.at[2, 0], to_y),
        remote(xs.at[1, 2, mine], xs.at[1, 3, mine], ts.at[0], tr.at[2, 1], to_x),
        remote(xs.at[0, 2, rest], xs.at[0, 3, rest], ts.at[0], tr.at[3, 0], to_x),
    ]

    def swap(slot, a):
        return remote(
            xs.at[a, slot, mine], xs.at[a, slot, mine], cs.at[0], cr.at[slot - 1, a], to_core
        )

    def swapped(slot, a):
        blk = xs.at[a, slot, theirs]
        remote(blk, blk, cs.at[0], cr.at[slot - 1, a], to_core).wait_recv()

    def unit(u, h, slot, lvl):
        if u == 1 and native:
            total = acc[h, u, slot]
            for b in (0, 1):
                span = pl.ds(pl.multiple_of(lvl * level + b * rows, rows), rows)
                total = total + dot(xs[u, slot, :, span], wd[h, lvl, b], 1, 1)
            acc[h, u, slot] = total
        else:
            span = pl.ds(pl.multiple_of(lvl * level, level), level)
            acc[h, u, slot] += dot(xs[u, slot, :, span], ws[u][h, lvl].reshape(level, cols), 1, 0)

    done = [[-1, -1] for _ in range(parts)]
    ready = [1, 1]

    def grow_slot(u, h, s, slot):
        for lvl in (at - s, at + s):
            @pl.when((lvl >= 0) & (lvl < line))
            def _():
                unit(u, h, slot, lvl)

    def grow(u, h, s):
        done[h][u] = s
        n = ready[u]
        if s == 0:
            def body(slot, _):
                unit(u, h, slot, at)
                return 0

            lax.fori_loop(0, n, body, 0)
            return

        def body(i, _):
            lvl = at + s - 2 * s * lax.rem(i, 2)

            @pl.when((lvl >= 0) & (lvl < line))
            def _():
                unit(u, h, lax.div(i, 2), lvl)
            return 0

        lax.fori_loop(0, 2 * n, body, 0)

    def join(slot, u, halves):
        for h in halves:
            lo, hi = jnp.maximum(at - done[h][u], 0), jnp.minimum(at + done[h][u], line - 1)

            def body(lvl, _):
                unit(u, h, slot, lvl)
                return 0

            lax.fori_loop(lo, hi + 1, body, 0)

    def make_g(h, slot):
        g[h, slot] = (2.0 * jnp.maximum(acc[h, 0, slot], 0.0) * acc[h, 1, slot]).astype(BF16)

    low = at < line - at - 1

    turns = (1 - p, p)

    def o_copy(go_up, h, o, k, here=None):
        def o_last(o):
            return jnp.where(o == (at - 1 if here is None else at), line, o)

        d, b = 0 if go_up else 1, turns[k]
        return remote(
            dw.at[h, o, b], zin.at[d, h, o, b], os.at[d], orr.at[h, o, k] if go_up else orr.at[h, o_last(o), k],
            up if go_up else down,
        )

    def make_dw(h, i):
        o = jnp.where(low, line - 1 - i, i)
        span = pl.ds(pl.multiple_of(o * level, level), level)
        lhs = xs[0, :, :, span].reshape(4 * tokens, level)
        value = dot(lhs, g[h].reshape(4 * tokens, cols), 0, 0)
        dw[h, o] = value.astype(BF16).reshape(2, rows, cols)
        if i < line - 1:
            @pl.when(at == 0)
            def _():
                for k in (0, 1):
                    o_copy(True, h, line - 1 - i, k).start()

            @pl.when(at == line - 1)
            def _():
                for k in (0, 1):
                    o_copy(False, h, i, k).start()

    part = tokens // n_tp

    def start_part(slot):
        def body(lvl, _):
            span = pl.ds(pl.multiple_of(lvl * level, level), level)
            value = dot(g[0, slot], wu[0, lvl].reshape(level, cols), 1, 1)
            ahead[:, :, span] = value.reshape(n_tp, part, level)
            return 0

        lax.fori_loop(0, line, body, 0)

    both = xs.at[:, 0]
    pltpu.make_async_copy(both, both, ls.at[0]).wait()
    pltpu.make_async_copy(fin, fin, ls.at[1]).wait()

    def own_level(h):
        for u in (0, 1):
            y_arrival(u, h).wait_recv()
            z_step(h, 0, 2 + u)
        for u in (0, 1):
            grow(u, h, 0)

    own_level(0)

    def got(slot, a):
        def run():
            if slot < 3:
                first[slot, a].wait_recv()
                if (slot, a) == (1, 0):
                    diag[0].start()
                if (slot, a) == (2, 1):
                    diag[1].start()
                if (slot, a) == (2, 0):
                    diag[2].start()
            else:
                diag[a].wait_recv()
                if a == 0:
                    diag[2].wait_recv()
            swap(slot, a).start()
        return run

    def use(slot, a):
        def run():
            swapped(slot, a)
            ready[a] += 1
            join(slot, a, range(parts))
        return run

    def early():
        swapped(3, 0)
        ready[0] += 1
        for h in range(final):
            join(3, 0, [h])

            def body(slot, _):
                make_g(h, slot)
                return 0

            lax.fori_loop(0, 4, body, 0)
            for i in range(line):
                make_dw(h, i)
        join(3, 0, [final])
        if parts > 1:
            start_part(3)

    if parts == 2:
        hooks = {
            (0, 2, 1): [got(1, 0)],
            (0, 2, 3): [use(1, 0)],
            (1, 1, 1): [got(2, 1)],
            (1, 1, 3): [use(2, 1), got(1, 1)],
            (0, 3, 0): [use(1, 1)],
            (0, 3, 3): [got(2, 0)],
            (1, 2, 0): [use(2, 0)],
            (1, 2, 1): [got(3, 1)],
            (1, 2, 2): [use(3, 1), got(3, 0)],
            (1, 2, 3): [early],
        }
        steps = [(0, 1)]
        for s in range(2, line):
            steps += [(0, s), (1, s - 1)]
        steps += [(1, line - 1)]
    else:
        hooks = {
            (0, 1, 2): [got(1, 0)],
            (0, 1, 3): [use(1, 0)],
            (0, 2, 0): [got(2, 1)],
            (0, 2, 1): [got(1, 1), use(2, 1)],
            (0, 2, 2): [use(1, 1)],
            (0, 2, 3): [got(2, 0)],
            (0, 3, 0): [use(2, 0), got(3, 1)],
            (0, 3, 1): [use(3, 1)],
            (0, 3, 2): [got(3, 0)],
            (0, 3, 3): [early],
        }
        steps = [(0, s) for s in range(1, line)]
    for h, s in steps:
        for j in range(4):
            z_step(h, s, j)
            if j >= 2 and (h, s, j) != (final, line - 1, 3):
                grow(j - 2, h, s)
            for run in hooks.pop((h, s, j), []):
                run()
        if (h, s) == (0, 1):
            for k in range(1, parts):
                z_step(k, 0, 0)
                z_step(k, 0, 1)
                own_level(k)
    for key in list(hooks):
        for run in hooks[key]:
            run()

    def p_copy(slot, k):
        there = lax.rem(c + k, n_tp)
        return remote(
            part_.at[slot, there], tpin.at[k - 1, slot], ps.at[0], pr.at[k - 1, slot], {"tp": there}
        )

    def make_part(slot):
        def body(lvl, _):
            span = pl.ds(pl.multiple_of(lvl * level, level), level)
            value = dot(g[0, slot], wu[0, lvl].reshape(level, cols), 1, 1)
            for h in range(1, parts):
                value = value + dot(g[h, slot], wu[h, lvl].reshape(level, cols), 1, 1)
            part_[slot, :, :, span] = value.astype(BF16).reshape(n_tp, part, level)
            return 0

        lax.fori_loop(0, line, body, 0)
        for k in range(1, n_tp):
            p_copy(slot, k).start()

    marks = [i * line // 4 for i in range(5)]
    turn = (2, 0, 1, 3)

    def group(i):
        return pl.ds(marks[i] * level, (marks[i + 1] - marks[i]) * level)

    def e_part(slot, k, i):
        there = lax.rem(c + k, n_tp)
        return remote(
            part_.at[slot, there, :, group(i)], tpin.at[k - 1, slot, :, group(i)],
            ps.at[0], pr.at[k - 1, 4 * i + slot], {"tp": there},
        )

    def end_part(slot):
        for i in turn:
            def body(lvl, _):
                span = pl.ds(pl.multiple_of(lvl * level, level), level)
                value = dot(g[1, slot], wu[1, lvl].reshape(level, cols), 1, 1)
                part_[slot, :, :, span] = (ahead[:, :, span] + value.reshape(n_tp, part, level)).astype(BF16)
                return 0

            lax.fori_loop(marks[i], marks[i + 1], body, 0)
            for k in range(1, n_tp):
                e_part(slot, k, i).start()

    def end_sum(slot, i):
        total = part_[slot, c, :, group(i)].astype(F32)
        for k in range(1, n_tp):
            e_part(slot, k, i).wait_recv()
            total = total + tpin[k - 1, slot, :, group(i)].astype(F32)
        part_[slot, c, :, group(i)] = total.astype(BF16)
        for copy in third[i]:
            copy.start()

    def tp_sum(slot):
        for k in range(1, n_tp):
            p_copy(slot, k).wait_recv()
        total = part_[slot, c].astype(F32)
        for k in range(1, n_tp):
            total = total + tpin[k - 1, slot].astype(F32)
        return total

    cut = width * 3 // 8 // 128 * 128
    early_cut = cut * 2 // 384 * 128
    left, right = pl.ds(0, cut), pl.ds(cut, width - cut)
    left_a, left_b = pl.ds(0, early_cut), pl.ds(early_cut, cut - early_cut)
    third = []
    for i in range(4):
        lo, hi = marks[i] * level, marks[i + 1] * level
        mid = min(max(cut, lo), hi)
        third.append([])
        for k, (start, stop, dev) in enumerate(((lo, mid, to_x), (mid, hi, to_y))):
            if stop > start:
                span = pl.ds(start, stop - start)
                third[i].append(
                    remote(part_.at[3, c, :, span], q1.at[1, :, span], qs.at[0], qr.at[8 + 2 * i + k], dev)
                )
    toward_x = [third[i][0] for i in range(4) if marks[i] * level < cut]
    toward_y = [third[i][-1] for i in range(4) if marks[i + 1] * level > cut]
    q_copies = {
        "x1": remote(part_.at[1, c, :, left], q1.at[0, :, left], qs.at[0], qr.at[2], to_x),
        "y2": remote(part_.at[2, c, :, right], q1.at[0, :, right], qs.at[0], qr.at[3], to_y),
        "y2a": remote(part_.at[2, c, :, left_a], q2.at[:, left_a], qs.at[0], qr.at[4], to_y),
        "y2b": remote(part_.at[2, c, :, left_b], q2.at[:, left_b], qs.at[0], qr.at[6], to_y),
        "x1r": remote(part_.at[1, c, :, right], q2.at[:, right], qs.at[0], qr.at[5], to_x),
    }

    def store_sum(slot):
        part_[slot, c] = tp_sum(slot).astype(BF16)

    def o_step(h, t, k):
        b = turns[k]
        for go_up in (True, False):
            d = 0 if go_up else 1
            gap = at if go_up else line - 1 - at
            o = (line - 1 - t + at) if go_up else (t - line + 1 + at)

            @pl.when((gap > 0) & (gap <= t))
            def _():
                o_copy(go_up, h, o, k, True).wait_recv()
                if t < line - 1:
                    dw[h, o, b] = (dw[h, o, b].astype(F32) + zin[d, h, o, b].astype(F32)).astype(BF16)
                    o_copy(go_up, h, o, k).start()

    half_rows = [pl.ds(i * (rows // 2), rows // 2) for i in (0, 1)]

    def dw_at(q, h, span=slice(None)):
        return dw_out.at[span, pl.ds(pl.multiple_of((q * parts + h) * cols, cols), cols)]

    def e_y(h, i):
        here = dw_at(quarter, h, half_rows[i])
        return remote(fin.at[h, 1 - p, half_rows[i]], here, es.at[1], er.at[1 + i, h], to_y)

    def e_relay(h, i):
        here = dw_at(2 * r + 1 - p, h, half_rows[i])
        return remote(here, here, es.at[2], er.at[3 + i, h], to_x)

    def e_x(h):
        return remote(fin.at[h, p], dw_at(quarter, h), es.at[0], er.at[0, h], to_x)

    def e_own(h):
        return pltpu.make_async_copy(fin.at[h, p], dw_at(quarter, h), el.at[0])

    def finish(h, k):
        b = turns[k]
        for d, there in ((0, has_down), (1, has_up)):
            @pl.when(there & jnp.logical_not(has_up & has_down))
            def _():
                fin[h, b] = (dw[h, at, b].astype(F32) + zin[d, h, at, b].astype(F32)).astype(BF16)

        @pl.when(has_up & has_down)
        def _():
            total = dw[h, at, b].astype(F32) + zin[0, h, at, b].astype(F32) + zin[1, h, at, b].astype(F32)
            fin[h, b] = total.astype(BF16)

        if line == 1:
            fin[h, b] = dw[h, at, b]
        if k == 0:
            e_y(h, 0).start()
            e_y(h, 1).start()
        else:
            e_x(h).start()
            e_own(h).start()

    def relay(h):
        for i in (0, 1):
            blk = dw_at(2 * r + 1 - p, h, half_rows[i])
            remote(blk, blk, es.at[1], er.at[1 + i, h], to_y).wait_recv()
            e_relay(h, i).start()

    def in_x3():
        for copy in toward_x:
            copy.wait_recv()
        part_[2, c, :, left] = (part_[2, c, :, left].astype(F32) + q1[1, :, left].astype(F32)).astype(BF16)

    def in_y3():
        for copy in toward_y:
            copy.wait_recv()
        part_[1, c, :, right] = (part_[1, c, :, right].astype(F32) + q1[1, :, right].astype(F32)).astype(BF16)

    segments = ((right, ("y2", "x1r")), (left_a, ("x1", "y2a")), (left_b, ("y2b",)))

    def out_own(i):
        span = segments[i][0]
        return pltpu.make_async_copy(fo.at[:, span], din_out.at[c, :, span], dl.at[0])

    def out_peer(i, k):
        span = segments[i][0]
        return remote(
            fo.at[:, span], din_out.at[c, :, span], ds.at[0], dr.at[k - 1, i], {"tp": lax.rem(c + k, n_tp)}
        )

    def in_last(i):
        span, names = segments[i]
        for name in names:
            q_copies[name].wait_recv()
        total = part_[0, c, :, span].astype(F32)
        for k in range(1, n_tp):
            total = total + tpin[k - 1, 0, :, span].astype(F32)
        fo[:, span] = (total + q1[0, :, span].astype(F32) + q2[:, span].astype(F32)).astype(BF16)
        out_own(i).start()
        for k in range(1, n_tp):
            out_peer(i, k).start()

    def last_rows(slot):
        if line > 1:
            grow_slot(1, final, line - 1, slot)
        make_g(final, slot)

    def send(*names):
        for name in names:
            q_copies[name].start()

    def sums(h, t, k):
        if 1 <= t < line:
            o_step(h, t, k)

    def weights(lo, hi):
        for i in range(lo, min(hi, line)):
            make_dw(final, i)

    def close(h, k):
        sums(h, line - 1, k)
        finish(h, k)

    split = parts > 1
    last_rows(3)
    if split:
        end_part(3)
    else:
        make_part(3)
    last_rows(1)
    if split:
        end_sum(3, 2)
        end_sum(3, 0)
    last_rows(2)
    if split:
        end_sum(3, 1)
        end_sum(3, 3)
    last_rows(0)
    if not split:
        store_sum(3)
        for copies in third:
            for copy in copies:
                copy.start()
    if split:
        sums(0, 1, 0)
    make_part(1)
    if split:
        sums(0, 1, 1)
    weights(0, 1)
    make_part(2)
    store_sum(1)
    send("x1")
    if split:
        sums(0, 2, 0)
    weights(1, 2)
    make_part(0)
    store_sum(2)
    send("y2")
    if split:
        sums(0, 2, 1)
    weights(2, line)
    for t in range(3 if split else 1, line - 1):
        for k in (0, 1):
            sums(0, t, k)
    if split:
        close(0, 0)
        close(0, 1)
    in_x3()
    in_y3()
    send("x1r")
    for h in range(1, parts):
        for t in range(1, line - 1):
            for k in (0, 1):
                sums(h, t, k)
    close(final, 0)
    send("y2a", "y2b")
    if split:
        relay(0)
    close(final, 1)
    for k in range(1, n_tp):
        p_copy(0, k).wait_recv()
    in_last(0)
    relay(final)
    in_last(1)
    in_last(2)

    for i in range(3):
        for k in range(1, n_tp):
            out_peer(i, k).wait_recv()
    for h in range(parts):
        blk = dw_at(2 * (1 - r) + p, h)
        remote(blk, blk, es.at[0], er.at[0, h], to_x).wait_recv()
        for i in (0, 1):
            blk = dw_at(2 * (1 - r) + 1 - p, h, half_rows[i])
            remote(blk, blk, es.at[2], er.at[3 + i, h], to_x).wait_recv()

    def sent(ref, sem):
        pltpu.make_async_copy(ref, ref, sem).wait()

    sent(fo, dl.at[0])
    sent(fin.at[:, 0], el.at[0])
    for i in range(3):
        sent(fin.at[:, 0], es.at[i])
    sent(part_.at[pl.ds(0, 3), 0], qs.at[0])
    if n_tp > 1:
        sent(tpin, ps.at[0])
        sent(tpin.at[:, 0], ds.at[0])
    sent(xs.at[0, pl.ds(0, 3)], ts.at[0])
    sent(xs.at[0, pl.ds(0, 3)], cs.at[0])
    sent(fin, ys.at[0])
    for k in range(line):
        @pl.when((at == k) & has_up)
        def _():
            sent(dw.at[:, pl.ds(0, max(line - 1 - k, 1))], os.at[0])
            for u in (0, 1):
                sent(ws[u].at[:, pl.ds(0, k + 1)], zs.at[0, u])

        @pl.when((at == k) & has_down)
        def _():
            sent(dw.at[:, pl.ds(0, max(k, 1))], os.at[1])
            for u in (0, 1):
                sent(ws[u].at[:, pl.ds(0, line - k)], zs.at[1, u])


def fused(n_fs, n_tp, n_rep, x, c, w_up, w_down):
    line = n_fs // 2
    tokens, width = x.shape
    rows, block = w_up.shape
    cols = block // (2 * n_rep)
    parts = 2 if cols % 256 == 0 and n_fs >= 8 else 1
    cols = cols // parts
    native = rows % 128 == 0
    if not native:
        w_down = w_down.T
    part = tokens // n_tp
    dma = pltpu.SemaphoreType.DMA
    hbm = pl.BlockSpec(memory_space=pl.ANY)
    vmem = lambda *shape: pltpu.VMEM(shape, BF16)
    down_block = (cols, rows) if native else (rows, cols)
    others = max(n_tp - 1, 1)
    return pl.pallas_call(
        functools.partial(kernel, line, n_tp, native, parts),
        out_shape=(
            jax.ShapeDtypeStruct((rows, block), BF16),
            jax.ShapeDtypeStruct((n_tp, part, width), BF16),
        ),
        in_specs=[hbm] * 4,
        out_specs=(hbm,) * 2,
        scratch_shapes=[
            vmem(2, 4, tokens, width),
            vmem(parts, line, 2, rows, cols),
            vmem(parts, line, 2, *down_block),
            pltpu.VMEM((parts, 2, 4, tokens, cols), F32),
            vmem(parts, 4, tokens, cols),
            vmem(parts, line, 2, rows, cols),
            vmem(2, parts, line, 2, rows, cols),
            vmem(parts, 2, rows, cols),
            vmem(4, n_tp, part, width),
            vmem(others, 4, part, width),
            vmem(2, part, width),
            vmem(part, width),
            vmem(part, width),
            pltpu.VMEM((n_tp, part, width) if parts > 1 else (1, 8, 128), F32),
            dma((2, 2)), dma((parts, line, 4)), dma((1,)), dma((parts, 2)),
            dma((1,)), dma((4, 2)), dma((1,)), dma((3, 2)), dma((2,)),
            dma((2,)), dma((parts, line + 1, 2)),
            dma((3,)), dma((5, parts)), dma((1,)),
            dma((1,)), dma((others, 16)), dma((1,)), dma((16,)),
            dma((1,)), dma((others, 3)), dma((1,)),
        ],
        compiler_params=pltpu.CompilerParams(
            collective_id=0, has_side_effects=True, vmem_limit_bytes=52 * 2**20
        ),
        name="fused",
    )(x, c, w_up, w_down)


def per_device(inputs, w_up, w_down, cotangent):
    n_rep, n_fs, n_tp = lax.axis_size("rep"), lax.axis_size("fs"), lax.axis_size("tp")
    d_w, d_in = fused(n_fs, n_tp, n_rep, inputs, cotangent, w_up, w_down)
    return d_in.reshape(inputs.shape), d_w.astype(F32)


def solution(mesh):
    in_specs = (P(("rep", "fs"), None), P("fs", "tp"), P("tp", "fs"), P(("rep", "fs"), None))
    out_specs = (P(("rep", "fs"), None), P("fs", "tp"))
    return jax.shard_map(
        per_device, mesh=mesh, in_specs=in_specs, out_specs=out_specs, check_vma=False
    )
```

```python
import functools

import jax
import jax.numpy as jnp
from jax import lax
from jax.experimental import pallas as pl
from jax.experimental.pallas import tpu as pltpu
from jax.sharding import PartitionSpec as P

MESH = pl.DeviceIdType.MESH
F32, BF16 = jnp.float32, jnp.bfloat16


def dot(a, b, da, db):
    return lax.dot_general(a, b, (((da,), (db,)), ((), ())), preferred_element_type=F32)


def kernel(line, n_tp, native, parts, x_in, c_in, up_in, down_in, dw_out, din_out,
           xs, wu, wd, acc, g, dw, zin, fin, part_, tpin, q1, q2, fo, ahead,
           zs, zr, ys, yr, ts, tr, cs, cr, ls, os, orr, es, er, el, ps, pr, qs, qr, ds, dr, dl):
    r, f, c = lax.axis_index("rep"), lax.axis_index("fs"), lax.axis_index("tp")
    p, at = lax.rem(f, 2), lax.div(f, 2)
    core = lax.rem(c, 2)
    to_x, to_y = {"rep": 1 - r}, {"fs": f + 1 - 2 * p}
    to_core = {"tp": c + 1 - 2 * core}
    up, down = {"fs": f + 2}, {"fs": f - 2}
    has_up, has_down = at < line - 1, at > 0
    tokens, width = x_in.shape
    rows, cols = wu.shape[3:]
    level = 2 * rows
    final = parts - 1
    quarter = 2 * r + p

    barrier = pltpu.get_barrier_semaphore()
    peers = [{"tp": lax.rem(c + k, n_tp)} for k in range(1, n_tp)]
    for dev in [to_x, to_y] + peers:
        pl.semaphore_signal(barrier, inc=1, device_id=dev, device_id_type=MESH)

    @pl.when(has_up)
    def _():
        pl.semaphore_signal(barrier, inc=1, device_id=up, device_id_type=MESH)

    @pl.when(has_down)
    def _():
        pl.semaphore_signal(barrier, inc=1, device_id=down, device_id_type=MESH)

    def remote(src, dst, send, recv, dev):
        return pltpu.make_async_remote_copy(
            src_ref=src, dst_ref=dst, send_sem=send, recv_sem=recv, device_id=dev, device_id_type=MESH
        )

    half = tokens // 2
    mine = pl.ds(pl.multiple_of(core * half, half), half)
    theirs = pl.ds(pl.multiple_of((1 - core) * half, half), half)
    ws = (wu, wd)

    def own_block(u, q, h):
        span = pl.ds(pl.multiple_of((q * parts + h) * cols, cols), cols)
        if u == 1 and native:
            return down_in.at[span, :]
        return (up_in, down_in)[u].at[:, span]

    own_x = pltpu.make_async_copy(x_in, xs.at[0, 0], ls.at[0])
    own_c = pltpu.make_async_copy(c_in, xs.at[1, 0], ls.at[0])
    own_w = [
        pltpu.make_async_copy(own_block(u, quarter, h), ws[u].at[h, at, p], ls.at[1])
        for h in range(parts) for u in (0, 1)
    ]
    own_x.start()
    own_c.start()
    for copy in own_w:
        copy.start()
    acc[...] = jnp.zeros_like(acc)

    n_near = n_tp + 1
    inner = has_up & has_down

    @pl.when(inner)
    def _():
        pl.semaphore_wait(barrier, n_near + 2)

    @pl.when(jnp.logical_not(inner))
    def _():
        pl.semaphore_wait(barrier, n_near + 1 if line > 1 else n_near)

    y_copies = [
        remote(own_block(u, 2 * r + 1 - p, h), ws[u].at[h, at, p], ys.at[0], yr.at[h, u], to_y)
        for h in range(parts) for u in (0, 1)
    ]

    def y_arrival(u, h):
        blk = ws[u].at[h, at, 1 - p]
        return remote(blk, blk, ys.at[0], yr.at[h, u], to_y)

    for copy in y_copies:
        copy.start()

    def z_copy(go_up, h, s, j):
        u, own_pair = j % 2, j < 2
        lvl = at - s if go_up else at + s
        blk = ws[u].at[h, lvl, p if own_pair else 1 - p]
        src = own_block(u, quarter, h) if (s == 0 and own_pair) else blk
        d = 0 if go_up else 1
        return remote(src, blk, zs.at[d, u], zr.at[h, lvl, j], up if go_up else down)

    def z_valid(go_up, s):
        return ((at - s >= 0) & has_up) if go_up else ((at + s < line) & has_down)

    def z_step(h, s, j):
        for go_up in (True, False):
            d = 0 if go_up else 1
            if s > 0:
                lvl = at - s if go_up else at + s

                @pl.when((lvl >= 0) & (lvl < line))
                def _():
                    blk = ws[j % 2].at[h, lvl, p if j < 2 else 1 - p]
                    remote(blk, blk, zs.at[d, j % 2], zr.at[h, lvl, j], to_x).wait_recv()
            if s < line - 1:
                @pl.when(z_valid(go_up, s))
                def _():
                    z_copy(go_up, h, s, j).start()

    z_step(0, 0, 0)
    z_step(0, 0, 1)

    own = (x_in, c_in)
    first = {}
    for slot, dev in ((1, to_x), (2, to_y)):
        for a in (0, 1):
            first[slot, a] = remote(
                own[a].at[mine], xs.at[a, slot, mine], ts.at[0], tr.at[slot - 1, a], dev
            )
    first[1, 0].start()
    first[2, 1].start()
    first[1, 1].start()
    first[2, 0].start()
    most = half // 48 * 32
    base = pl.multiple_of(core * half, half)
    lead, rest = pl.ds(base, most), pl.ds(base + most, half - most)
    diag = [
        remote(xs.at[0, 1, lead], xs.at[0, 3, lead], ts.at[0], tr.at[2, 0], to_y),
        remote(xs.at[1, 2, mine], xs.at[1, 3, mine], ts.at[0], tr.at[2, 1], to_x),
        remote(xs.at[0, 2, rest], xs.at[0, 3, rest], ts.at[0], tr.at[3, 0], to_x),
    ]

    def swap(slot, a):
        return remote(
            xs.at[a, slot, mine], xs.at[a, slot, mine], cs.at[0], cr.at[slot - 1, a], to_core
        )

    def swapped(slot, a):
        blk = xs.at[a, slot, theirs]
        remote(blk, blk, cs.at[0], cr.at[slot - 1, a], to_core).wait_recv()

    def unit(u, h, slot, lvl):
        if u == 1 and native:
            total = acc[h, u, slot]
            for b in (0, 1):
                span = pl.ds(pl.multiple_of(lvl * level + b * rows, rows), rows)
                total = total + dot(xs[u, slot, :, span], wd[h, lvl, b], 1, 1)
            acc[h, u, slot] = total
        else:
            span = pl.ds(pl.multiple_of(lvl * level, level), level)
            acc[h, u, slot] += dot(xs[u, slot, :, span], ws[u][h, lvl].reshape(level, cols), 1, 0)

    done = [[-1, -1] for _ in range(parts)]
    ready = [1, 1]

    def grow_slot(u, h, s, slot):
        for lvl in (at - s, at + s):
            @pl.when((lvl >= 0) & (lvl < line))
            def _():
                unit(u, h, slot, lvl)

    def grow(u, h, s):
        done[h][u] = s
        n = ready[u]
        if s == 0:
            def body(slot, _):
                unit(u, h, slot, at)
                return 0

            lax.fori_loop(0, n, body, 0)
            return

        def body(i, _):
            lvl = at + s - 2 * s * lax.rem(i, 2)

            @pl.when((lvl >= 0) & (lvl < line))
            def _():
                unit(u, h, lax.div(i, 2), lvl)
            return 0

        lax.fori_loop(0, 2 * n, body, 0)

    def join(slot, u, halves):
        for h in halves:
            lo, hi = jnp.maximum(at - done[h][u], 0), jnp.minimum(at + done[h][u], line - 1)

            def body(lvl, _):
                unit(u, h, slot, lvl)
                return 0

            lax.fori_loop(lo, hi + 1, body, 0)

    def make_g(h, slot):
        g[h, slot] = (2.0 * jnp.maximum(acc[h, 0, slot], 0.0) * acc[h, 1, slot]).astype(BF16)

    low = at < line - at - 1

    turns = (1 - p, p)

    def o_copy(go_up, h, o, k, here=None):
        def o_last(o):
            return jnp.where(o == (at - 1 if here is None else at), line, o)

        d, b = 0 if go_up else 1, turns[k]
        return remote(
            dw.at[h, o, b], zin.at[d, h, o, b], os.at[d], orr.at[h, o, k] if go_up else orr.at[h, o_last(o), k],
            up if go_up else down,
        )

    def make_dw(h, i):
        o = jnp.where(low, line - 1 - i, i)
        span = pl.ds(pl.multiple_of(o * level, level), level)
        lhs = xs[0, :, :, span].reshape(4 * tokens, level)
        value = dot(lhs, g[h].reshape(4 * tokens, cols), 0, 0)
        dw[h, o] = value.astype(BF16).reshape(2, rows, cols)
        if i < line - 1:
            @pl.when(at == 0)
            def _():
                for k in (0, 1):
                    o_copy(True, h, line - 1 - i, k).start()

            @pl.when(at == line - 1)
            def _():
                for k in (0, 1):
                    o_copy(False, h, i, k).start()

    part = tokens // n_tp

    def start_part(slot):
        def body(lvl, _):
            span = pl.ds(pl.multiple_of(lvl * level, level), level)
            value = dot(g[0, slot], wu[0, lvl].reshape(level, cols), 1, 1)
            ahead[:, :, span] = value.reshape(n_tp, part, level)
            return 0

        lax.fori_loop(0, line, body, 0)

    both = xs.at[:, 0]
    pltpu.make_async_copy(both, both, ls.at[0]).wait()
    pltpu.make_async_copy(fin, fin, ls.at[1]).wait()

    def own_level(h):
        for u in (0, 1):
            y_arrival(u, h).wait_recv()
            z_step(h, 0, 2 + u)
        for u in (0, 1):
            grow(u, h, 0)

    own_level(0)

    def got(slot, a):
        def run():
            if slot < 3:
                first[slot, a].wait_recv()
                if (slot, a) == (1, 0):
                    diag[0].start()
                if (slot, a) == (2, 1):
                    diag[1].start()
                if (slot, a) == (2, 0):
                    diag[2].start()
            else:
                diag[a].wait_recv()
                if a == 0:
                    diag[2].wait_recv()
            swap(slot, a).start()
        return run

    def use(slot, a):
        def run():
            swapped(slot, a)
            ready[a] += 1
            join(slot, a, range(parts))
        return run

    def early():
        swapped(3, 0)
        ready[0] += 1
        for h in range(final):
            join(3, 0, [h])

            def body(slot, _):
                make_g(h, slot)
                return 0

            lax.fori_loop(0, 4, body, 0)
            for i in range(line):
                make_dw(h, i)
        join(3, 0, [final])
        if parts > 1:
            start_part(3)

    if parts == 2:
        hooks = {
            (0, 2, 1): [got(1, 0)],
            (0, 2, 3): [use(1, 0)],
            (1, 1, 1): [got(2, 1)],
            (1, 1, 3): [use(2, 1), got(1, 1)],
            (0, 3, 0): [use(1, 1)],
            (0, 3, 3): [got(2, 0)],
            (1, 2, 0): [use(2, 0)],
            (1, 2, 1): [got(3, 1)],
            (1, 2, 2): [use(3, 1), got(3, 0)],
            (1, 2, 3): [early],
        }
        steps = [(0, 1)]
        for s in range(2, line):
            steps += [(0, s), (1, s - 1)]
        steps += [(1, line - 1)]
    else:
        hooks = {
            (0, 1, 2): [got(1, 0)],
            (0, 1, 3): [use(1, 0)],
            (0, 2, 0): [got(2, 1)],
            (0, 2, 1): [got(1, 1), use(2, 1)],
            (0, 2, 2): [use(1, 1)],
            (0, 2, 3): [got(2, 0)],
            (0, 3, 0): [use(2, 0), got(3, 1)],
            (0, 3, 1): [use(3, 1)],
            (0, 3, 2): [got(3, 0)],
            (0, 3, 3): [early],
        }
        steps = [(0, s) for s in range(1, line)]
    for h, s in steps:
        for j in range(4):
            z_step(h, s, j)
            if j >= 2 and (h, s, j) != (final, line - 1, 3):
                grow(j - 2, h, s)
            for run in hooks.pop((h, s, j), []):
                run()
        if (h, s) == (0, 1):
            for k in range(1, parts):
                z_step(k, 0, 0)
                z_step(k, 0, 1)
                own_level(k)
    for key in list(hooks):
        for run in hooks[key]:
            run()

    def p_copy(slot, k):
        there = lax.rem(c + k, n_tp)
        return remote(
            part_.at[slot, there], tpin.at[k - 1, slot], ps.at[0], pr.at[k - 1, slot], {"tp": there}
        )

    def make_part(slot):
        def body(lvl, _):
            span = pl.ds(pl.multiple_of(lvl * level, level), level)
            value = dot(g[0, slot], wu[0, lvl].reshape(level, cols), 1, 1)
            for h in range(1, parts):
                value = value + dot(g[h, slot], wu[h, lvl].reshape(level, cols), 1, 1)
            part_[slot, :, :, span] = value.astype(BF16).reshape(n_tp, part, level)
            return 0

        lax.fori_loop(0, line, body, 0)
        for k in range(1, n_tp):
            p_copy(slot, k).start()

    marks = [i * line // 4 for i in range(5)]
    turn = (2, 0, 1, 3)

    def group(i):
        return pl.ds(marks[i] * level, (marks[i + 1] - marks[i]) * level)

    def e_part(slot, k, i):
        there = lax.rem(c + k, n_tp)
        return remote(
            part_.at[slot, there, :, group(i)], tpin.at[k - 1, slot, :, group(i)],
            ps.at[0], pr.at[k - 1, 3 + i], {"tp": there},
        )

    def end_part(slot):
        for i in turn:
            def body(lvl, _):
                span = pl.ds(pl.multiple_of(lvl * level, level), level)
                value = dot(g[1, slot], wu[1, lvl].reshape(level, cols), 1, 1)
                part_[slot, :, :, span] = (ahead[:, :, span] + value.reshape(n_tp, part, level)).astype(BF16)
                return 0

            lax.fori_loop(marks[i], marks[i + 1], body, 0)
            for k in range(1, n_tp):
                e_part(slot, k, i).start()

    def end_sum(slot, i):
        total = part_[slot, c, :, group(i)].astype(F32)
        for k in range(1, n_tp):
            e_part(slot, k, i).wait_recv()
            total = total + tpin[k - 1, slot, :, group(i)].astype(F32)
        part_[slot, c, :, group(i)] = total.astype(BF16)
        for copy in third[i]:
            copy.start()

    def tp_sum(slot):
        for k in range(1, n_tp):
            p_copy(slot, k).wait_recv()
        total = part_[slot, c].astype(F32)
        for k in range(1, n_tp):
            total = total + tpin[k - 1, slot].astype(F32)
        return total

    cut = width * 3 // 8 // 128 * 128
    early_cut = cut * 2 // 384 * 128
    left, right = pl.ds(0, cut), pl.ds(cut, width - cut)
    left_a, left_b = pl.ds(0, early_cut), pl.ds(early_cut, cut - early_cut)
    third = []
    for i in range(4):
        lo, hi = marks[i] * level, marks[i + 1] * level
        mid = min(max(cut, lo), hi)
        third.append([])
        for k, (start, stop, dev) in enumerate(((lo, mid, to_x), (mid, hi, to_y))):
            if stop > start:
                span = pl.ds(start, stop - start)
                third[i].append(
                    remote(part_.at[3, c, :, span], q1.at[1, :, span], qs.at[0], qr.at[7 + i if k == 0 else 11 + i], dev)
                )
    toward_x = [third[i][0] for i in range(4) if marks[i] * level < cut]
    toward_y = [third[i][-1] for i in range(4) if marks[i + 1] * level > cut]
    q_copies = {
        "x1": remote(part_.at[1, c, :, left], q1.at[0, :, left], qs.at[0], qr.at[2], to_x),
        "y2": remote(part_.at[2, c, :, right], q1.at[0, :, right], qs.at[0], qr.at[3], to_y),
        "y2a": remote(part_.at[2, c, :, left_a], q2.at[:, left_a], qs.at[0], qr.at[4], to_y),
        "y2b": remote(part_.at[2, c, :, left_b], q2.at[:, left_b], qs.at[0], qr.at[6], to_y),
        "x1r": remote(part_.at[1, c, :, right], q2.at[:, right], qs.at[0], qr.at[5], to_x),
    }

    def store_sum(slot):
        part_[slot, c] = tp_sum(slot).astype(BF16)

    def o_step(h, t, k):
        b = turns[k]
        for go_up in (True, False):
            d = 0 if go_up else 1
            gap = at if go_up else line - 1 - at
            o = (line - 1 - t + at) if go_up else (t - line + 1 + at)

            @pl.when((gap > 0) & (gap <= t))
            def _():
                o_copy(go_up, h, o, k, True).wait_recv()
                if t < line - 1:
                    dw[h, o, b] = (dw[h, o, b].astype(F32) + zin[d, h, o, b].astype(F32)).astype(BF16)
                    o_copy(go_up, h, o, k).start()

    half_rows = [pl.ds(i * (rows // 2), rows // 2) for i in (0, 1)]

    def dw_at(q, h, span=slice(None)):
        return dw_out.at[span, pl.ds(pl.multiple_of((q * parts + h) * cols, cols), cols)]

    def e_y(h, i):
        here = dw_at(quarter, h, half_rows[i])
        return remote(fin.at[h, 1 - p, half_rows[i]], here, es.at[1], er.at[1 + i, h], to_y)

    def e_relay(h, i):
        here = dw_at(2 * r + 1 - p, h, half_rows[i])
        return remote(here, here, es.at[2], er.at[3 + i, h], to_x)

    def e_x(h):
        return remote(fin.at[h, p], dw_at(quarter, h), es.at[0], er.at[0, h], to_x)

    def e_own(h):
        return pltpu.make_async_copy(fin.at[h, p], dw_at(quarter, h), el.at[0])

    def finish(h, k):
        b = turns[k]
        for d, there in ((0, has_down), (1, has_up)):
            @pl.when(there & jnp.logical_not(has_up & has_down))
            def _():
                fin[h, b] = (dw[h, at, b].astype(F32) + zin[d, h, at, b].astype(F32)).astype(BF16)

        @pl.when(has_up & has_down)
        def _():
            total = dw[h, at, b].astype(F32) + zin[0, h, at, b].astype(F32) + zin[1, h, at, b].astype(F32)
            fin[h, b] = total.astype(BF16)

        if line == 1:
            fin[h, b] = dw[h, at, b]
        if k == 0:
            e_y(h, 0).start()
            e_y(h, 1).start()
        else:
            e_x(h).start()
            e_own(h).start()

    def relay(h):
        for i in (0, 1):
            blk = dw_at(2 * r + 1 - p, h, half_rows[i])
            remote(blk, blk, es.at[1], er.at[1 + i, h], to_y).wait_recv()
            e_relay(h, i).start()

    def in_x3():
        for copy in toward_x:
            copy.wait_recv()
        part_[2, c, :, left] = (part_[2, c, :, left].astype(F32) + q1[1, :, left].astype(F32)).astype(BF16)

    def in_y3():
        for copy in toward_y:
            copy.wait_recv()
        part_[1, c, :, right] = (part_[1, c, :, right].astype(F32) + q1[1, :, right].astype(F32)).astype(BF16)

    segments = ((right, ("y2", "x1r")), (left_a, ("x1", "y2a")), (left_b, ("y2b",)))

    def out_own(i):
        span = segments[i][0]
        return pltpu.make_async_copy(fo.at[:, span], din_out.at[c, :, span], dl.at[0])

    def out_peer(i, k):
        span = segments[i][0]
        return remote(
            fo.at[:, span], din_out.at[c, :, span], ds.at[0], dr.at[k - 1, i], {"tp": lax.rem(c + k, n_tp)}
        )

    def in_last(i):
        span, names = segments[i]
        for name in names:
            q_copies[name].wait_recv()
        total = part_[0, c, :, span].astype(F32)
        for k in range(1, n_tp):
            total = total + tpin[k - 1, 0, :, span].astype(F32)
        fo[:, span] = (total + q1[0, :, span].astype(F32) + q2[:, span].astype(F32)).astype(BF16)
        out_own(i).start()
        for k in range(1, n_tp):
            out_peer(i, k).start()

    def last_rows(slot):
        if line > 1:
            grow_slot(1, final, line - 1, slot)
        make_g(final, slot)

    def send(*names):
        for name in names:
            q_copies[name].start()

    def sums(h, t, k):
        if 1 <= t < line:
            o_step(h, t, k)

    def weights(lo, hi):
        for i in range(lo, min(hi, line)):
            make_dw(final, i)

    def close(h, k):
        sums(h, line - 1, k)
        finish(h, k)

    split = parts > 1
    last_rows(3)
    if split:
        end_part(3)
    else:
        make_part(3)
    if split:
        end_sum(3, 2)
        end_sum(3, 0)
    last_rows(1)
    last_rows(2)
    if split:
        end_sum(3, 1)
        end_sum(3, 3)
    last_rows(0)
    if not split:
        store_sum(3)
        for copies in third:
            for copy in copies:
                copy.start()
    if split:
        sums(0, 1, 0)
    make_part(1)
    if split:
        sums(0, 1, 1)
    weights(0, 1)
    make_part(2)
    store_sum(1)
    send("x1")
    if split:
        sums(0, 2, 0)
    weights(1, 2)
    make_part(0)
    store_sum(2)
    send("y2")
    if split:
        sums(0, 2, 1)
    weights(2, line)
    for t in range(3 if split else 1, line - 1):
        for k in (0, 1):
            sums(0, t, k)
    if split:
        close(0, 0)
        close(0, 1)
    in_x3()
    in_y3()
    send("x1r")
    for h in range(1, parts):
        for t in range(1, line - 1):
            for k in (0, 1):
                sums(h, t, k)
    close(final, 0)
    send("y2a", "y2b")
    if split:
        relay(0)
    close(final, 1)
    for k in range(1, n_tp):
        p_copy(0, k).wait_recv()
    in_last(0)
    relay(final)
    in_last(1)
    in_last(2)

    for i in range(3):
        for k in range(1, n_tp):
            out_peer(i, k).wait_recv()
    for h in range(parts):
        blk = dw_at(2 * (1 - r) + p, h)
        remote(blk, blk, es.at[0], er.at[0, h], to_x).wait_recv()
        for i in (0, 1):
            blk = dw_at(2 * (1 - r) + 1 - p, h, half_rows[i])
            remote(blk, blk, es.at[2], er.at[3 + i, h], to_x).wait_recv()

    def sent(ref, sem):
        pltpu.make_async_copy(ref, ref, sem).wait()

    sent(fo, dl.at[0])
    sent(fin.at[:, 0], el.at[0])
    for i in range(3):
        sent(fin.at[:, 0], es.at[i])
    sent(part_.at[pl.ds(0, 3), 0], qs.at[0])
    if n_tp > 1:
        sent(tpin, ps.at[0])
        sent(tpin.at[:, 0], ds.at[0])
    sent(xs.at[0, pl.ds(0, 3)], ts.at[0])
    sent(xs.at[0, pl.ds(0, 3)], cs.at[0])
    sent(fin, ys.at[0])
    for k in range(line):
        @pl.when((at == k) & has_up)
        def _():
            sent(dw.at[:, pl.ds(0, max(line - 1 - k, 1))], os.at[0])
            for u in (0, 1):
                sent(ws[u].at[:, pl.ds(0, k + 1)], zs.at[0, u])

        @pl.when((at == k) & has_down)
        def _():
            sent(dw.at[:, pl.ds(0, max(k, 1))], os.at[1])
            for u in (0, 1):
                sent(ws[u].at[:, pl.ds(0, line - k)], zs.at[1, u])


def fused(n_fs, n_tp, n_rep, x, c, w_up, w_down):
    line = n_fs // 2
    tokens, width = x.shape
    rows, block = w_up.shape
    cols = block // (2 * n_rep)
    parts = 2 if cols % 256 == 0 and n_fs >= 8 else 1
    cols = cols // parts
    native = rows % 128 == 0
    if not native:
        w_down = w_down.T
    part = tokens // n_tp
    dma = pltpu.SemaphoreType.DMA
    hbm = pl.BlockSpec(memory_space=pl.ANY)
    vmem = lambda *shape: pltpu.VMEM(shape, BF16)
    down_block = (cols, rows) if native else (rows, cols)
    others = max(n_tp - 1, 1)
    return pl.pallas_call(
        functools.partial(kernel, line, n_tp, native, parts),
        out_shape=(
            jax.ShapeDtypeStruct((rows, block), BF16),
            jax.ShapeDtypeStruct((n_tp, part, width), BF16),
        ),
        in_specs=[hbm] * 4,
        out_specs=(hbm,) * 2,
        scratch_shapes=[
            vmem(2, 4, tokens, width),
            vmem(parts, line, 2, rows, cols),
            vmem(parts, line, 2, *down_block),
            pltpu.VMEM((parts, 2, 4, tokens, cols), F32),
            vmem(parts, 4, tokens, cols),
            vmem(parts, line, 2, rows, cols),
            vmem(2, parts, line, 2, rows, cols),
            vmem(parts, 2, rows, cols),
            vmem(4, n_tp, part, width),
            vmem(others, 4, part, width),
            vmem(2, part, width),
            vmem(part, width),
            vmem(part, width),
            pltpu.VMEM((n_tp, part, width) if parts > 1 else (1, 8, 128), F32),
            dma((2, 2)), dma((parts, line, 4)), dma((1,)), dma((parts, 2)),
            dma((1,)), dma((4, 2)), dma((1,)), dma((3, 2)), dma((2,)),
            dma((2,)), dma((parts, line + 1, 2)),
            dma((3,)), dma((5, parts)), dma((1,)),
            dma((1,)), dma((others, 7)), dma((1,)), dma((16,)),
            dma((1,)), dma((others, 3)), dma((1,)),
        ],
        compiler_params=pltpu.CompilerParams(
            collective_id=0, has_side_effects=True, vmem_limit_bytes=52 * 2**20
        ),
        name="fused",
    )(x, c, w_up, w_down)


def per_device(inputs, w_up, w_down, cotangent):
    n_rep, n_fs, n_tp = lax.axis_size("rep"), lax.axis_size("fs"), lax.axis_size("tp")
    d_w, d_in = fused(n_fs, n_tp, n_rep, inputs, cotangent, w_up, w_down)
    return d_in.reshape(inputs.shape), d_w.astype(F32)


def solution(mesh):
    in_specs = (P(("rep", "fs"), None), P("fs", "tp"), P("tp", "fs"), P(("rep", "fs"), None))
    out_specs = (P(("rep", "fs"), None), P("fs", "tp"))
    return jax.shard_map(
        per_device, mesh=mesh, in_specs=in_specs, out_specs=out_specs, check_vma=False
    )
```

```python
import functools

import jax
import jax.numpy as jnp
from jax import lax
from jax.experimental import pallas as pl
from jax.experimental.pallas import tpu as pltpu
from jax.sharding import PartitionSpec as P

MESH = pl.DeviceIdType.MESH
F32, BF16 = jnp.float32, jnp.bfloat16


def dot(a, b, da, db):
    return lax.dot_general(a, b, (((da,), (db,)), ((), ())), preferred_element_type=F32)


def kernel(line, n_tp, native, parts, x_in, c_in, up_in, down_in, dw_out, din_out,
           xs, wu, wd, acc, g, dw, zin, fin, part_, tpin, q1, q2, fo, ahead,
           zs, zr, ys, yr, ts, tr, cs, cr, ls, os, orr, es, er, el, ps, pr, qs, qr, ds, dr, dl):
    r, f, c = lax.axis_index("rep"), lax.axis_index("fs"), lax.axis_index("tp")
    p, at = lax.rem(f, 2), lax.div(f, 2)
    core = lax.rem(c, 2)
    to_x, to_y = {"rep": 1 - r}, {"fs": f + 1 - 2 * p}
    to_core = {"tp": c + 1 - 2 * core}
    up, down = {"fs": f + 2}, {"fs": f - 2}
    has_up, has_down = at < line - 1, at > 0
    tokens, width = x_in.shape
    rows, cols = wu.shape[3:]
    level = 2 * rows
    final = parts - 1
    quarter = 2 * r + p

    barrier = pltpu.get_barrier_semaphore()
    peers = [{"tp": lax.rem(c + k, n_tp)} for k in range(1, n_tp)]
    for dev in [to_x, to_y] + peers:
        pl.semaphore_signal(barrier, inc=1, device_id=dev, device_id_type=MESH)

    @pl.when(has_up)
    def _():
        pl.semaphore_signal(barrier, inc=1, device_id=up, device_id_type=MESH)

    @pl.when(has_down)
    def _():
        pl.semaphore_signal(barrier, inc=1, device_id=down, device_id_type=MESH)

    def remote(src, dst, send, recv, dev):
        return pltpu.make_async_remote_copy(
            src_ref=src, dst_ref=dst, send_sem=send, recv_sem=recv, device_id=dev, device_id_type=MESH
        )

    half = tokens // 2
    mine = pl.ds(pl.multiple_of(core * half, half), half)
    theirs = pl.ds(pl.multiple_of((1 - core) * half, half), half)
    ws = (wu, wd)

    def own_block(u, q, h):
        span = pl.ds(pl.multiple_of((q * parts + h) * cols, cols), cols)
        if u == 1 and native:
            return down_in.at[span, :]
        return (up_in, down_in)[u].at[:, span]

    own_x = pltpu.make_async_copy(x_in, xs.at[0, 0], ls.at[0])
    own_c = pltpu.make_async_copy(c_in, xs.at[1, 0], ls.at[0])
    own_w = [
        pltpu.make_async_copy(own_block(u, quarter, h), ws[u].at[h, at, p], ls.at[1])
        for h in range(parts) for u in (0, 1)
    ]
    own_x.start()
    own_c.start()
    for copy in own_w:
        copy.start()
    acc[...] = jnp.zeros_like(acc)

    n_near = n_tp + 1
    inner = has_up & has_down

    @pl.when(inner)
    def _():
        pl.semaphore_wait(barrier, n_near + 2)

    @pl.when(jnp.logical_not(inner))
    def _():
        pl.semaphore_wait(barrier, n_near + 1 if line > 1 else n_near)

    y_copies = [
        remote(own_block(u, 2 * r + 1 - p, h), ws[u].at[h, at, p], ys.at[0], yr.at[h, u], to_y)
        for h in range(parts) for u in (0, 1)
    ]

    def y_arrival(u, h):
        blk = ws[u].at[h, at, 1 - p]
        return remote(blk, blk, ys.at[0], yr.at[h, u], to_y)

    for copy in y_copies:
        copy.start()

    def z_copy(go_up, h, s, j):
        u, own_pair = j % 2, j < 2
        lvl = at - s if go_up else at + s
        blk = ws[u].at[h, lvl, p if own_pair else 1 - p]
        src = own_block(u, quarter, h) if (s == 0 and own_pair) else blk
        d = 0 if go_up else 1
        return remote(src, blk, zs.at[d, u], zr.at[h, lvl, j], up if go_up else down)

    def z_valid(go_up, s):
        return ((at - s >= 0) & has_up) if go_up else ((at + s < line) & has_down)

    def z_step(h, s, j):
        for go_up in (True, False):
            d = 0 if go_up else 1
            if s > 0:
                lvl = at - s if go_up else at + s

                @pl.when((lvl >= 0) & (lvl < line))
                def _():
                    blk = ws[j % 2].at[h, lvl, p if j < 2 else 1 - p]
                    remote(blk, blk, zs.at[d, j % 2], zr.at[h, lvl, j], to_x).wait_recv()
            if s < line - 1:
                @pl.when(z_valid(go_up, s))
                def _():
                    z_copy(go_up, h, s, j).start()

    z_step(0, 0, 0)
    z_step(0, 0, 1)

    own = (x_in, c_in)
    first = {}
    for slot, dev in ((1, to_x), (2, to_y)):
        for a in (0, 1):
            first[slot, a] = remote(
                own[a].at[mine], xs.at[a, slot, mine], ts.at[0], tr.at[slot - 1, a], dev
            )
    first[1, 0].start()
    first[2, 1].start()
    first[1, 1].start()
    first[2, 0].start()
    most = half // 48 * 32
    base = pl.multiple_of(core * half, half)
    lead, rest = pl.ds(base, most), pl.ds(base + most, half - most)
    diag = [
        remote(xs.at[0, 1, lead], xs.at[0, 3, lead], ts.at[0], tr.at[2, 0], to_y),
        remote(xs.at[1, 2, mine], xs.at[1, 3, mine], ts.at[0], tr.at[2, 1], to_x),
        remote(xs.at[0, 2, rest], xs.at[0, 3, rest], ts.at[0], tr.at[3, 0], to_x),
    ]

    def swap(slot, a):
        return remote(
            xs.at[a, slot, mine], xs.at[a, slot, mine], cs.at[0], cr.at[slot - 1, a], to_core
        )

    def swapped(slot, a):
        blk = xs.at[a, slot, theirs]
        remote(blk, blk, cs.at[0], cr.at[slot - 1, a], to_core).wait_recv()

    def unit(u, h, slot, lvl):
        if u == 1 and native:
            total = acc[h, u, slot]
            for b in (0, 1):
                span = pl.ds(pl.multiple_of(lvl * level + b * rows, rows), rows)
                total = total + dot(xs[u, slot, :, span], wd[h, lvl, b], 1, 1)
            acc[h, u, slot] = total
        else:
            span = pl.ds(pl.multiple_of(lvl * level, level), level)
            acc[h, u, slot] += dot(xs[u, slot, :, span], ws[u][h, lvl].reshape(level, cols), 1, 0)

    done = [[-1, -1] for _ in range(parts)]
    ready = [1, 1]

    def grow_slot(u, h, s, slot):
        for lvl in (at - s, at + s):
            @pl.when((lvl >= 0) & (lvl < line))
            def _():
                unit(u, h, slot, lvl)

    def grow(u, h, s):
        done[h][u] = s
        n = ready[u]
        if s == 0:
            def body(slot, _):
                unit(u, h, slot, at)
                return 0

            lax.fori_loop(0, n, body, 0)
            return

        def body(i, _):
            lvl = at + s - 2 * s * lax.rem(i, 2)

            @pl.when((lvl >= 0) & (lvl < line))
            def _():
                unit(u, h, lax.div(i, 2), lvl)
            return 0

        lax.fori_loop(0, 2 * n, body, 0)

    def join(slot, u, halves):
        for h in halves:
            lo, hi = jnp.maximum(at - done[h][u], 0), jnp.minimum(at + done[h][u], line - 1)

            def body(lvl, _):
                unit(u, h, slot, lvl)
                return 0

            lax.fori_loop(lo, hi + 1, body, 0)

    def make_g(h, slot):
        g[h, slot] = (2.0 * jnp.maximum(acc[h, 0, slot], 0.0) * acc[h, 1, slot]).astype(BF16)

    low = at < line - at - 1

    turns = (1 - p, p)

    def o_copy(go_up, h, o, k, here=None):
        def o_last(o):
            return jnp.where(o == (at - 1 if here is None else at), line, o)

        d, b = 0 if go_up else 1, turns[k]
        return remote(
            dw.at[h, o, b], zin.at[d, h, o, b], os.at[d], orr.at[h, o, k] if go_up else orr.at[h, o_last(o), k],
            up if go_up else down,
        )

    def make_dw(h, i):
        o = jnp.where(low, line - 1 - i, i)
        span = pl.ds(pl.multiple_of(o * level, level), level)
        lhs = xs[0, :, :, span].reshape(4 * tokens, level)
        value = dot(lhs, g[h].reshape(4 * tokens, cols), 0, 0)
        dw[h, o] = value.astype(BF16).reshape(2, rows, cols)
        if i < line - 1:
            @pl.when(at == 0)
            def _():
                for k in (0, 1):
                    o_copy(True, h, line - 1 - i, k).start()

            @pl.when(at == line - 1)
            def _():
                for k in (0, 1):
                    o_copy(False, h, i, k).start()

    part = tokens // n_tp

    def start_part(slot):
        def body(lvl, _):
            span = pl.ds(pl.multiple_of(lvl * level, level), level)
            value = dot(g[0, slot], wu[0, lvl].reshape(level, cols), 1, 1)
            ahead[:, :, span] = value.reshape(n_tp, part, level)
            return 0

        lax.fori_loop(0, line, body, 0)

    both = xs.at[:, 0]
    pltpu.make_async_copy(both, both, ls.at[0]).wait()
    pltpu.make_async_copy(fin, fin, ls.at[1]).wait()

    def own_level(h):
        for u in (0, 1):
            y_arrival(u, h).wait_recv()
            z_step(h, 0, 2 + u)
        for u in (0, 1):
            grow(u, h, 0)

    own_level(0)

    def got(slot, a):
        def run():
            if slot < 3:
                first[slot, a].wait_recv()
                if (slot, a) == (1, 0):
                    diag[0].start()
                if (slot, a) == (2, 1):
                    diag[1].start()
                if (slot, a) == (2, 0):
                    diag[2].start()
            else:
                diag[a].wait_recv()
                if a == 0:
                    diag[2].wait_recv()
            swap(slot, a).start()
        return run

    def use(slot, a):
        def run():
            swapped(slot, a)
            ready[a] += 1
            join(slot, a, range(parts))
        return run

    def early():
        swapped(3, 0)
        ready[0] += 1
        for h in range(final):
            join(3, 0, [h])

            def body(slot, _):
                make_g(h, slot)
                return 0

            lax.fori_loop(0, 4, body, 0)
            for i in range(line):
                make_dw(h, i)
        join(3, 0, [final])
        if parts > 1:
            start_part(3)

    if parts == 2:
        hooks = {
            (0, 2, 1): [got(1, 0)],
            (0, 2, 3): [use(1, 0)],
            (1, 1, 1): [got(2, 1)],
            (1, 1, 3): [use(2, 1), got(1, 1)],
            (0, 3, 0): [use(1, 1)],
            (0, 3, 3): [got(2, 0)],
            (1, 2, 0): [use(2, 0)],
            (1, 2, 1): [got(3, 1)],
            (1, 2, 2): [use(3, 1), got(3, 0)],
            (1, 2, 3): [early],
        }
        steps = [(0, 1)]
        for s in range(2, line):
            steps += [(0, s), (1, s - 1)]
        steps += [(1, line - 1)]
    else:
        hooks = {
            (0, 1, 2): [got(1, 0)],
            (0, 1, 3): [use(1, 0)],
            (0, 2, 0): [got(2, 1)],
            (0, 2, 1): [got(1, 1), use(2, 1)],
            (0, 2, 2): [use(1, 1)],
            (0, 2, 3): [got(2, 0)],
            (0, 3, 0): [use(2, 0), got(3, 1)],
            (0, 3, 1): [use(3, 1)],
            (0, 3, 2): [got(3, 0)],
            (0, 3, 3): [early],
        }
        steps = [(0, s) for s in range(1, line)]
    for h, s in steps:
        for j in range(4):
            z_step(h, s, j)
            if j >= 2 and (h, s, j) != (final, line - 1, 3):
                grow(j - 2, h, s)
            for run in hooks.pop((h, s, j), []):
                run()
        if (h, s) == (0, 1):
            for k in range(1, parts):
                z_step(k, 0, 0)
                z_step(k, 0, 1)
                own_level(k)
    for key in list(hooks):
        for run in hooks[key]:
            run()

    def p_copy(slot, k):
        there = lax.rem(c + k, n_tp)
        return remote(
            part_.at[slot, there], tpin.at[k - 1, slot], ps.at[0], pr.at[k - 1, slot], {"tp": there}
        )

    def make_part(slot):
        def body(lvl, _):
            span = pl.ds(pl.multiple_of(lvl * level, level), level)
            value = dot(g[0, slot], wu[0, lvl].reshape(level, cols), 1, 1)
            for h in range(1, parts):
                value = value + dot(g[h, slot], wu[h, lvl].reshape(level, cols), 1, 1)
            part_[slot, :, :, span] = value.astype(BF16).reshape(n_tp, part, level)
            return 0

        lax.fori_loop(0, line, body, 0)
        for k in range(1, n_tp):
            p_copy(slot, k).start()

    marks = [i * line // 4 for i in range(5)]
    turn = (2, 0, 1, 3)

    def group(i):
        return pl.ds(marks[i] * level, (marks[i + 1] - marks[i]) * level)

    def e_part(slot, k, i):
        there = lax.rem(c + k, n_tp)
        return remote(
            part_.at[slot, there, :, group(i)], tpin.at[k - 1, slot, :, group(i)],
            ps.at[0], pr.at[k - 1, 3 + i], {"tp": there},
        )

    def end_part(slot):
        for i in turn:
            def body(lvl, _):
                span = pl.ds(pl.multiple_of(lvl * level, level), level)
                value = dot(g[1, slot], wu[1, lvl].reshape(level, cols), 1, 1)
                part_[slot, :, :, span] = (ahead[:, :, span] + value.reshape(n_tp, part, level)).astype(BF16)
                return 0

            lax.fori_loop(marks[i], marks[i + 1], body, 0)
            for k in range(1, n_tp):
                e_part(slot, k, i).start()

    def end_sum(slot, i):
        total = part_[slot, c, :, group(i)].astype(F32)
        for k in range(1, n_tp):
            e_part(slot, k, i).wait_recv()
            total = total + tpin[k - 1, slot, :, group(i)].astype(F32)
        part_[slot, c, :, group(i)] = total.astype(BF16)
        for copy in third[i]:
            copy.start()

    def tp_sum(slot):
        for k in range(1, n_tp):
            p_copy(slot, k).wait_recv()
        total = part_[slot, c].astype(F32)
        for k in range(1, n_tp):
            total = total + tpin[k - 1, slot].astype(F32)
        return total

    cut = width * 3 // 8 // 128 * 128
    early_cut = max(cut - 128, 128)
    left, right = pl.ds(0, cut), pl.ds(cut, width - cut)
    left_a, left_b = pl.ds(0, early_cut), pl.ds(early_cut, cut - early_cut)
    third = []
    for i in range(4):
        lo, hi = marks[i] * level, marks[i + 1] * level
        mid = min(max(cut, lo), hi)
        third.append([])
        for k, (start, stop, dev) in enumerate(((lo, mid, to_x), (mid, hi, to_y))):
            if stop > start:
                span = pl.ds(start, stop - start)
                third[i].append(
                    remote(part_.at[3, c, :, span], q1.at[1, :, span], qs.at[0], qr.at[7 + i if k == 0 else 11 + i], dev)
                )
    toward_x = [third[i][0] for i in range(4) if marks[i] * level < cut]
    toward_y = [third[i][-1] for i in range(4) if marks[i + 1] * level > cut]
    q_copies = {
        "x1": remote(part_.at[1, c, :, left], q1.at[0, :, left], qs.at[0], qr.at[2], to_x),
        "y2": remote(part_.at[2, c, :, right], q1.at[0, :, right], qs.at[0], qr.at[3], to_y),
        "y2a": remote(part_.at[2, c, :, left_a], q2.at[:, left_a], qs.at[0], qr.at[4], to_y),
        "y2b": remote(part_.at[2, c, :, left_b], q2.at[:, left_b], qs.at[0], qr.at[6], to_y),
        "x1r": remote(part_.at[1, c, :, right], q2.at[:, right], qs.at[0], qr.at[5], to_x),
    }

    def store_sum(slot):
        part_[slot, c] = tp_sum(slot).astype(BF16)

    def o_step(h, t, k):
        b = turns[k]
        for go_up in (True, False):
            d = 0 if go_up else 1
            gap = at if go_up else line - 1 - at
            o = (line - 1 - t + at) if go_up else (t - line + 1 + at)

            @pl.when((gap > 0) & (gap <= t))
            def _():
                o_copy(go_up, h, o, k, True).wait_recv()
                if t < line - 1:
                    dw[h, o, b] = (dw[h, o, b].astype(F32) + zin[d, h, o, b].astype(F32)).astype(BF16)
                    o_copy(go_up, h, o, k).start()

    half_rows = [pl.ds(i * (rows // 2), rows // 2) for i in (0, 1)]

    def dw_at(q, h, span=slice(None)):
        return dw_out.at[span, pl.ds(pl.multiple_of((q * parts + h) * cols, cols), cols)]

    def e_y(h, i):
        here = dw_at(quarter, h, half_rows[i])
        return remote(fin.at[h, 1 - p, half_rows[i]], here, es.at[1], er.at[1 + i, h], to_y)

    def e_relay(h, i):
        here = dw_at(2 * r + 1 - p, h, half_rows[i])
        return remote(here, here, es.at[2], er.at[3 + i, h], to_x)

    def e_x(h):
        return remote(fin.at[h, p], dw_at(quarter, h), es.at[0], er.at[0, h], to_x)

    def e_own(h):
        return pltpu.make_async_copy(fin.at[h, p], dw_at(quarter, h), el.at[0])

    def finish(h, k):
        b = turns[k]
        for d, there in ((0, has_down), (1, has_up)):
            @pl.when(there & jnp.logical_not(has_up & has_down))
            def _():
                fin[h, b] = (dw[h, at, b].astype(F32) + zin[d, h, at, b].astype(F32)).astype(BF16)

        @pl.when(has_up & has_down)
        def _():
            total = dw[h, at, b].astype(F32) + zin[0, h, at, b].astype(F32) + zin[1, h, at, b].astype(F32)
            fin[h, b] = total.astype(BF16)

        if line == 1:
            fin[h, b] = dw[h, at, b]
        if k == 0:
            e_y(h, 0).start()
            e_y(h, 1).start()
        else:
            e_x(h).start()
            e_own(h).start()

    def relay(h):
        for i in (0, 1):
            blk = dw_at(2 * r + 1 - p, h, half_rows[i])
            remote(blk, blk, es.at[1], er.at[1 + i, h], to_y).wait_recv()
            e_relay(h, i).start()

    def in_x3():
        for copy in toward_x:
            copy.wait_recv()
        part_[2, c, :, left] = (part_[2, c, :, left].astype(F32) + q1[1, :, left].astype(F32)).astype(BF16)

    def in_y3():
        for copy in toward_y:
            copy.wait_recv()
        part_[1, c, :, right] = (part_[1, c, :, right].astype(F32) + q1[1, :, right].astype(F32)).astype(BF16)

    segments = ((right, ("y2", "x1r")), (left_a, ("x1", "y2a")), (left_b, ("y2b",)))

    def out_own(i):
        span = segments[i][0]
        return pltpu.make_async_copy(fo.at[:, span], din_out.at[c, :, span], dl.at[0])

    def out_peer(i, k):
        span = segments[i][0]
        return remote(
            fo.at[:, span], din_out.at[c, :, span], ds.at[0], dr.at[k - 1, i], {"tp": lax.rem(c + k, n_tp)}
        )

    def in_last(i):
        span, names = segments[i]
        for name in names:
            q_copies[name].wait_recv()
        total = part_[0, c, :, span].astype(F32)
        for k in range(1, n_tp):
            total = total + tpin[k - 1, 0, :, span].astype(F32)
        fo[:, span] = (total + q1[0, :, span].astype(F32) + q2[:, span].astype(F32)).astype(BF16)
        out_own(i).start()
        for k in range(1, n_tp):
            out_peer(i, k).start()

    def last_rows(slot):
        if line > 1:
            grow_slot(1, final, line - 1, slot)
        make_g(final, slot)

    def send(*names):
        for name in names:
            q_copies[name].start()

    def sums(h, t, k):
        if 1 <= t < line:
            o_step(h, t, k)

    def weights(lo, hi):
        for i in range(lo, min(hi, line)):
            make_dw(final, i)

    def close(h, k):
        sums(h, line - 1, k)
        finish(h, k)

    split = parts > 1
    last_rows(3)
    if split:
        end_part(3)
    else:
        make_part(3)
    if split:
        end_sum(3, 2)
        end_sum(3, 0)
    last_rows(1)
    last_rows(2)
    if split:
        end_sum(3, 1)
        end_sum(3, 3)
    last_rows(0)
    if not split:
        store_sum(3)
        for copies in third:
            for copy in copies:
                copy.start()
    if split:
        sums(0, 1, 0)
    make_part(1)
    if split:
        sums(0, 1, 1)
    weights(0, 1)
    make_part(2)
    store_sum(1)
    send("x1")
    if split:
        sums(0, 2, 0)
    weights(1, 2)
    make_part(0)
    store_sum(2)
    send("y2")
    if split:
        sums(0, 2, 1)
    weights(2, line)
    for t in range(3 if split else 1, line - 1):
        for k in (0, 1):
            sums(0, t, k)
    if split:
        close(0, 0)
        close(0, 1)
    in_x3()
    in_y3()
    send("x1r")
    for h in range(1, parts):
        for t in range(1, line - 1):
            for k in (0, 1):
                sums(h, t, k)
    close(final, 0)
    send("y2a", "y2b")
    if split:
        relay(0)
    close(final, 1)
    for k in range(1, n_tp):
        p_copy(0, k).wait_recv()
    in_last(0)
    relay(final)

    def sent(ref, sem):
        pltpu.make_async_copy(ref, ref, sem).wait()

    if n_tp > 1:
        sent(tpin, ps.at[0])
    sent(xs.at[0, pl.ds(0, 3)], ts.at[0])
    sent(xs.at[0, pl.ds(0, 3)], cs.at[0])
    sent(fin, ys.at[0])
    for k in range(line):
        @pl.when((at == k) & has_up)
        def _():
            sent(dw.at[:, pl.ds(0, max(line - 1 - k, 1))], os.at[0])
            for u in (0, 1):
                sent(ws[u].at[:, pl.ds(0, k + 1)], zs.at[0, u])

        @pl.when((at == k) & has_down)
        def _():
            sent(dw.at[:, pl.ds(0, max(k, 1))], os.at[1])
            for u in (0, 1):
                sent(ws[u].at[:, pl.ds(0, line - k)], zs.at[1, u])

    in_last(1)
    in_last(2)

    for i in range(3):
        for k in range(1, n_tp):
            out_peer(i, k).wait_recv()
    for h in range(parts):
        blk = dw_at(2 * (1 - r) + p, h)
        remote(blk, blk, es.at[0], er.at[0, h], to_x).wait_recv()
        for i in (0, 1):
            blk = dw_at(2 * (1 - r) + 1 - p, h, half_rows[i])
            remote(blk, blk, es.at[2], er.at[3 + i, h], to_x).wait_recv()

    sent(fo, dl.at[0])
    sent(fin.at[:, 0], el.at[0])
    for i in range(3):
        sent(fin.at[:, 0], es.at[i])
    sent(part_.at[pl.ds(0, 3), 0], qs.at[0])
    if n_tp > 1:
        sent(tpin.at[:, 0], ds.at[0])


def fused(n_fs, n_tp, n_rep, x, c, w_up, w_down):
    line = n_fs // 2
    tokens, width = x.shape
    rows, block = w_up.shape
    cols = block // (2 * n_rep)
    parts = 2 if cols % 256 == 0 and n_fs >= 8 else 1
    cols = cols // parts
    native = rows % 128 == 0
    if not native:
        w_down = w_down.T
    part = tokens // n_tp
    dma = pltpu.SemaphoreType.DMA
    hbm = pl.BlockSpec(memory_space=pl.ANY)
    vmem = lambda *shape: pltpu.VMEM(shape, BF16)
    down_block = (cols, rows) if native else (rows, cols)
    others = max(n_tp - 1, 1)
    return pl.pallas_call(
        functools.partial(kernel, line, n_tp, native, parts),
        out_shape=(
            jax.ShapeDtypeStruct((rows, block), BF16),
            jax.ShapeDtypeStruct((n_tp, part, width), BF16),
        ),
        in_specs=[hbm] * 4,
        out_specs=(hbm,) * 2,
        scratch_shapes=[
            vmem(2, 4, tokens, width),
            vmem(parts, line, 2, rows, cols),
            vmem(parts, line, 2, *down_block),
            pltpu.VMEM((parts, 2, 4, tokens, cols), F32),
            vmem(parts, 4, tokens, cols),
            vmem(parts, line, 2, rows, cols),
            vmem(2, parts, line, 2, rows, cols),
            vmem(parts, 2, rows, cols),
            vmem(4, n_tp, part, width),
            vmem(others, 4, part, width),
            vmem(2, part, width),
            vmem(part, width),
            vmem(part, width),
            pltpu.VMEM((n_tp, part, width) if parts > 1 else (1, 8, 128), F32),
            dma((2, 2)), dma((parts, line, 4)), dma((1,)), dma((parts, 2)),
            dma((1,)), dma((4, 2)), dma((1,)), dma((3, 2)), dma((2,)),
            dma((2,)), dma((parts, line + 1, 2)),
            dma((3,)), dma((5, parts)), dma((1,)),
            dma((1,)), dma((others, 7)), dma((1,)), dma((16,)),
            dma((1,)), dma((others, 3)), dma((1,)),
        ],
        compiler_params=pltpu.CompilerParams(
            collective_id=0, has_side_effects=True, vmem_limit_bytes=52 * 2**20
        ),
        name="fused",
    )(x, c, w_up, w_down)


def per_device(inputs, w_up, w_down, cotangent):
    n_rep, n_fs, n_tp = lax.axis_size("rep"), lax.axis_size("fs"), lax.axis_size("tp")
    d_w, d_in = fused(n_fs, n_tp, n_rep, inputs, cotangent, w_up, w_down)
    return d_in.reshape(inputs.shape), d_w.astype(F32)


def solution(mesh):
    in_specs = (P(("rep", "fs"), None), P("fs", "tp"), P("tp", "fs"), P(("rep", "fs"), None))
    out_specs = (P(("rep", "fs"), None), P("fs", "tp"))
    return jax.shard_map(
        per_device, mesh=mesh, in_specs=in_specs, out_specs=out_specs, check_vma=False
    )
```
